256 devices in a mesh: sp: 64 (over z, x, core), tp: 4 (over y).
Axes of the slice: x: 4, y: 4, z: 8, core: 2. Of those that a mesh axis runs over, the one named last changes fastest.
Arguments:
- queries: bfloat16 [20480, 1024], P('sp', 'tp'), may hold values from -6.6 to 6.6
- key_matrix: bfloat16 [20480, 256], P('sp', 'tp'), may hold values from -6.6 to 6.6
- values: bfloat16 [20480, 256], P('sp', 'tp'), may hold values from -6 to 6
- query_gain: float32 [64], replicated, may hold values from 0.19 to 8
- key_norm_gain: float32 [64], replicated, may hold values from 0.19 to 8
- head_gain: float32 [1024], P('tp'), may hold values from 0.1 to 1.9
- out_proj: bfloat16 [1024, 2048], replicated, may hold values from -0.1875 to 0.1875
- residual: bfloat16 [20480, 2048], P('sp'), may hold values from -6 to 6
- ffn_gain: float32 [2048], replicated, may hold values from 0.1 to 1.9
- routes: int32 [20480, 4], P('sp'), may hold values from 0 to 255, all different within a row; in each aligned block of 320 rows (0 to 319, 320 to 639, ...) at most 10 rows name the same one
- route_weights: float32 [20480, 4], P('sp'), may hold values from 0.2 to 1
- expert_gate: bfloat16 [256, 2048, 512], P(('sp', 'tp')), may hold values from -0.125 to 0.125
- expert_up: bfloat16 [256, 2048, 512], P(('sp', 'tp')), may hold values from -0.125 to 0.125
- expert_down: bfloat16 [256, 512, 2048], P(('sp', 'tp')), may hold values from -0.25 to 0.25
- shared_gate: bfloat16 [2048, 512], P(None, 'tp'), may hold values from -0.125 to 0.125
- shared_up: bfloat16 [2048, 512], P(None, 'tp'), may hold values from -0.125 to 0.125
- shared_down: bfloat16 [512, 2048], P('tp'), may hold values from -0.25 to 0.25
Outputs:
- layer_out: bfloat16 [20480, 2048], P(('sp', 'tp'))
The draws below stay inside these ranges and needn't reach their ends.
Inputs may be any that keep to these rules, and one draw needn't show every extreme that they name: `routes`: each row names 4 different experts; in each aligned block of 320 rows (the tokens of one index of sp) no expert is named more than 10 times, a bound that some block reaches.
All inputs are finite; a program needn't handle non-finite values.
Results may differ from the reference program's by a relative error of at most 0.019.
The reference program's roundings to bfloat16 on the way count: a program that leaves them out, or rounds other values in their place, can miss the bound.
Values may be sent and summed in bfloat16 or wider, within the bound.
A program may use at most 128 MiB of HBM per device.

```python
import math
import jax
import jax.numpy as jnp
import numpy as np
from jax import lax

D = 2048
HEAD_SIZE = 64
QUERY_HEADS = 16
KEY_VALUE_HEADS = 4
FF = 512
SFF = 512
TOPK = 4
GRID_W = 64
TOK_DEV = 320
SEQUENCE_TOKENS = 20480
EXPERTS = 256
CAP = 10
N_SP = 64
N_TP = 4


def plant_pair(key):
    unrotated_query = jnp.clip(jax.random.normal(jax.random.fold_in(key, 11), (SEQUENCE_TOKENS, QUERY_HEADS * HEAD_SIZE), jnp.float32), -6.0, 6.0)
    unrotated_key = jnp.clip(jax.random.normal(jax.random.fold_in(key, 12), (SEQUENCE_TOKENS, KEY_VALUE_HEADS * HEAD_SIZE), jnp.float32), -6.0, 6.0)
    return (unrotated_query, unrotated_key)


def draw_queries(key, part):
    return plant_pair(key)[0].astype(jnp.bfloat16)


def draw_key_matrix(key, part):
    return plant_pair(key)[1].astype(jnp.bfloat16)


def gain_draw(key, salt):
    folded = jax.random.fold_in(key, salt)
    return 1.0 + 0.18 * jnp.clip(jax.random.normal(folded, (HEAD_SIZE,), jnp.float32), -4.5, 4.5)


def draw_query_gain(key, part):
    return gain_draw(key, 21)


def draw_key_norm_gain(key, part):
    return gain_draw(key, 22)


def block_scale(key, dims, cuts, smallest, top_value):
    factor_of, own = 1.0, jax.random.fold_in(key, 6)
    for axis_at, parts in cuts:
        heights = jnp.exp(jax.random.uniform(jax.random.fold_in(own, axis_at), (parts,), jnp.float32, smallest / len(cuts), top_value / len(cuts)))
        factor_of = factor_of * jnp.repeat(heights, dims[axis_at] // parts).reshape([-1 if axis == axis_at else 1 for axis in range(len(dims))])
    return factor_of


def routed_block(own_key, own, number, rows, amount, top, limit, skew):
    order = jax.random.permutation(own_key, amount)
    packed, common = portions_of(amount, rows * top, limit, skew, True), portions_of(amount, rows * top, limit, skew, False)
    places = jnp.arange(amount)

    def named(tallies, rotation):
        used = int((tallies > 0).sum())
        fixed = max(1, used // 4)
        passed = fixed + (places - fixed + rotation * (used - fixed)) % max(1, amount - fixed)
        return jnp.zeros((amount,), jnp.int32).at[order[jnp.where(places < fixed, places, passed)]].set(jnp.asarray(tallies, jnp.int32))

    tallies = jnp.where(number % 4 == 0, named(packed, number // 4), named(common, number - number // 4 - 1))
    mixed = jax.random.permutation(jax.random.fold_in(own, 3), amount)
    source_of, receiver = mixed[0:amount // 2 * 2:2], mixed[1:amount // 2 * 2:2]
    room = jnp.minimum(tallies[source_of] - 1, limit - tallies[receiver]) // 2
    room = jnp.where((source_of == order[0]) | (receiver == order[0]) | (tallies[receiver] == 0), 0, jnp.maximum(room, 0))
    passed = jax.random.randint(jax.random.fold_in(own, 4), (amount // 2,), 0, 1 << 20) % (room + 1)
    tallies = tallies.at[source_of].add(-passed).at[receiver].add(passed)
    items = jnp.searchsorted(jnp.cumsum(tallies), jnp.arange(rows * top), side="right").astype(jnp.int32)
    grid = items.reshape(top, rows).T
    grid = grid[jax.random.permutation(jax.random.fold_in(own, 1), rows)]
    rotation = jax.random.randint(jax.random.fold_in(own, 2), (rows, 1), 0, top)
    return jnp.take_along_axis(grid, (jnp.arange(top)[None, :] + rotation) % top, axis=1)


def portions_of(number_of, total, limit, slope, full):
    weights = [(1 << 20) // math.isqrt(rank ** slope) + 1 for rank in range(1, number_of + 1)]
    largest = limit if full else min(limit, max(-(-total // number_of), total * weights[0] // sum(weights)))
    least = 1 if total - largest >= number_of - 1 else 0
    given, surplus = [largest] + [least] * (number_of - 1), total - largest - least * (number_of - 1)
    while surplus > 0:
        free = [i for i in range(1, number_of) if given[i] < largest] or [i for i in range(1, number_of) if given[i] < limit]
        whole, left = sum([weights[i] for i in free]), surplus
        for i in free:
            addition = min(limit - given[i], max(1, left * weights[i] // whole), surplus)
            given[i] = given[i] + addition
            surplus = surplus - addition
    return np.array(given)


def normal_values(rng, dims, spread, reach, cuts=(), kind=jnp.bfloat16):
    values = spread * jax.random.normal(rng, dims, jnp.float32)
    if cuts:
        values = values * block_scale(rng, dims, cuts, -0.22, 0.18)
    return jnp.clip(values, -reach, reach).astype(kind)


def setup_inputs(seed: int = 0) -> dict:
    seeds = jax.random.split(jax.random.key(seed), 18)
    queries = draw_queries(jax.random.fold_in(seeds[17], 71), 0)
    key_matrix = draw_key_matrix(jax.random.fold_in(seeds[17], 71), 0)
    values = normal_values(seeds[2], (SEQUENCE_TOKENS, KEY_VALUE_HEADS * HEAD_SIZE), 1.0, 6.0, ((0, 64), (1, 4)))
    query_gain = draw_query_gain(jax.random.fold_in(seeds[17], 71), 0)
    key_norm_gain = draw_key_norm_gain(jax.random.fold_in(seeds[17], 71), 0)
    head_gain = jnp.clip(1.0 + 0.18 * jax.random.normal(seeds[5], (QUERY_HEADS * HEAD_SIZE,), jnp.float32), 0.1, 1.9)
    out_proj = normal_values(seeds[6], (QUERY_HEADS * HEAD_SIZE, D), (QUERY_HEADS * HEAD_SIZE) ** -0.5, 0.1875)
    residual = normal_values(seeds[7], (SEQUENCE_TOKENS, D), 1.0, 6.0, ((0, 64),))
    ffn_gain = jnp.clip(1.0 + 0.18 * jax.random.normal(seeds[8], (D,), jnp.float32), 0.1, 1.9)
    routes_keys = jax.random.split(jax.random.fold_in(seeds[9], 1), SEQUENCE_TOKENS // TOK_DEV)
    routes_turns = jax.random.permutation(jax.random.fold_in(seeds[9], 3), SEQUENCE_TOKENS // TOK_DEV)
    routes = jax.vmap(lambda own, number: routed_block(jax.random.fold_in(seeds[9], 2), own, number, TOK_DEV, EXPERTS, TOPK, CAP, 1))(routes_keys, routes_turns).reshape((SEQUENCE_TOKENS, TOPK))
    route_weights = jnp.clip(0.2 + 0.8 * jax.random.uniform(seeds[10], (SEQUENCE_TOKENS, TOPK), jnp.float32) ** block_scale(seeds[10], (SEQUENCE_TOKENS, TOPK), ((0, 64),), -0.2, 0.2), 0.2, 1.0)
    expert_gate = normal_values(seeds[11], (EXPERTS, D, FF), D ** -0.5, 0.125, ((0, 256),))
    expert_up = normal_values(seeds[12], (EXPERTS, D, FF), D ** -0.5, 0.125, ((0, 256),))
    expert_down = normal_values(seeds[13], (EXPERTS, FF, D), FF ** -0.5, 0.25, ((0, 256),))
    shared_gate = normal_values(seeds[14], (D, SFF), D ** -0.5, 0.125, ((1, 4),))
    shared_up = normal_values(seeds[15], (D, SFF), D ** -0.5, 0.125, ((1, 4),))
    shared_down = normal_values(seeds[16], (SFF, D), SFF ** -0.5, 0.25, ((0, 4),))
    return dict(queries=queries, key_matrix=key_matrix, values=values, query_gain=query_gain, key_norm_gain=key_norm_gain, head_gain=head_gain, out_proj=out_proj, residual=residual, ffn_gain=ffn_gain, routes=routes, route_weights=route_weights, expert_gate=expert_gate, expert_up=expert_up, expert_down=expert_down, shared_gate=shared_gate, shared_up=shared_up, shared_down=shared_down)


EPS = 1e-06
THETA = 10000.0

def final_norm(field, gain):
    mean_sq = lax.optimization_barrier(jnp.mean(field * field, axis=-1, keepdims=True))
    return field * lax.rsqrt(mean_sq + EPS) * gain

def grid_tables(positions, sequence_total):
    grid_rows = sequence_total // GRID_W
    row_pos = (positions // GRID_W - grid_rows // 2).astype(jnp.float32)
    col_pos = (positions % GRID_W - GRID_W // 2).astype(jnp.float32)
    quarter = HEAD_SIZE // 4
    inverse = THETA ** (-jnp.arange(quarter, dtype=jnp.float32) / quarter)
    angles = jnp.concatenate([row_pos[:, None] * inverse, col_pos[:, None] * inverse], axis=1)
    return (jnp.cos(angles), jnp.sin(angles))

def apply_rotary(field, cosine_table, sine_table):
    row_count, head_count = (field.shape[0], field.shape[1])
    quarter = HEAD_SIZE // 4
    pieces = field.reshape(row_count, head_count, 2, 2, quarter)
    front_half = pieces[:, :, :, 0, :].reshape(row_count, head_count, 2 * quarter)
    back_half = pieces[:, :, :, 1, :].reshape(row_count, head_count, 2 * quarter)
    cos_wide = cosine_table[:, None, :]
    sin_wide = sine_table[:, None, :]
    new_front = (front_half * cos_wide - back_half * sin_wide).reshape(row_count, head_count, 2, 1, quarter)
    new_back = (front_half * sin_wide + back_half * cos_wide).reshape(row_count, head_count, 2, 1, quarter)
    return jnp.concatenate([new_front, new_back], axis=3).reshape(row_count, head_count, HEAD_SIZE)

def reference(queries, key_matrix, values, query_gain, key_norm_gain, head_gain, out_proj, residual, ffn_gain, routes, route_weights, expert_gate, expert_up, expert_down, shared_gate, shared_up, shared_down):
    sequence_total = SEQUENCE_TOKENS
    positions = jnp.arange(sequence_total, dtype=jnp.int32)
    cosine_table, sine_table = grid_tables(positions, sequence_total)
    rotated_query = apply_rotary(final_norm(queries.astype(jnp.float32).reshape(sequence_total, QUERY_HEADS, HEAD_SIZE), query_gain), cosine_table, sine_table).astype(jnp.bfloat16)
    rotated_key = apply_rotary(final_norm(key_matrix.astype(jnp.float32).reshape(sequence_total, KEY_VALUE_HEADS, HEAD_SIZE), key_norm_gain), cosine_table, sine_table).astype(jnp.bfloat16)
    group_width = QUERY_HEADS // KEY_VALUE_HEADS
    block_length = 64
    query_block_list = rotated_query.reshape(sequence_total // block_length, block_length, KEY_VALUE_HEADS, group_width, HEAD_SIZE)
    key_wide = rotated_key.astype(jnp.float32)
    value_expanded = values.reshape(sequence_total, KEY_VALUE_HEADS, HEAD_SIZE).astype(jnp.float32)
    score_scale = HEAD_SIZE ** (-0.5)

    def attend(query_block):
        scores = jnp.einsum('qkgd,skd->kgqs', query_block.astype(jnp.float32), key_wide) * score_scale
        row_max = lax.optimization_barrier(jnp.max(scores, axis=-1, keepdims=True))
        expo_terms = jnp.exp(scores - row_max)
        weights = lax.optimization_barrier(expo_terms.astype(jnp.bfloat16)).astype(jnp.float32)
        mixed_vals = jnp.einsum('kgqs,skd->qkgd', weights, value_expanded)
        denominator = jnp.moveaxis(lax.optimization_barrier(jnp.sum(expo_terms, axis=-1)), -1, 0)
        return mixed_vals / denominator[..., None]
    attended = lax.map(attend, query_block_list).reshape(sequence_total, QUERY_HEADS, HEAD_SIZE)
    head_out = final_norm(attended, head_gain.reshape(QUERY_HEADS, HEAD_SIZE)).astype(jnp.bfloat16).reshape(sequence_total, QUERY_HEADS * HEAD_SIZE)
    hidden = (residual.astype(jnp.float32) + jnp.dot(head_out, out_proj, preferred_element_type=jnp.float32)).astype(jnp.bfloat16)
    normed = final_norm(hidden.astype(jnp.float32), ffn_gain).astype(jnp.bfloat16)
    flat_expert = routes.reshape(-1).astype(jnp.int32)
    entries = flat_expert.shape[0]
    order_ids = jnp.argsort(flat_expert, stable=True).astype(jnp.int32)
    sorted_expert = flat_expert[order_ids]
    counts_per = jnp.bincount(flat_expert, length=EXPERTS).astype(jnp.int32)
    starts = (jnp.cumsum(counts_per) - counts_per).astype(jnp.int32)
    rank_ids = (jnp.arange(entries, dtype=jnp.int32) - starts[sorted_expert]).astype(jnp.int32)
    slot_table = jnp.full((EXPERTS, N_SP * CAP), entries, jnp.int32).at[sorted_expert, rank_ids].set(order_ids)
    entry_weight = jnp.concatenate([route_weights.reshape(-1), jnp.zeros((1,), jnp.float32)])
    entry_token = jnp.concatenate([jnp.arange(entries, dtype=jnp.int32) // TOPK, jnp.zeros((1,), jnp.int32)])
    slice_width = SFF // N_TP
    result = hidden.astype(jnp.float32)
    for owner in range(N_TP):
        col_start = owner * slice_width
        gate_part = jnp.dot(normed, shared_gate[:, col_start:col_start + slice_width], preferred_element_type=jnp.float32)
        up_part = jnp.dot(normed, shared_up[:, col_start:col_start + slice_width], preferred_element_type=jnp.float32)
        inner_act = (jax.nn.silu(gate_part) * up_part).astype(jnp.bfloat16)
        partial_sum = jnp.dot(inner_act, shared_down[col_start:col_start + slice_width, :], preferred_element_type=jnp.float32)

        def add_expert(total_acc, local_index, owner=owner):
            expert = local_index * N_TP + owner
            entry_ids = slot_table[expert]
            token_ids = entry_token[entry_ids]
            rows_in = normed[token_ids]
            gate_out = jnp.dot(rows_in, expert_gate[expert], preferred_element_type=jnp.float32)
            up_out = jnp.dot(rows_in, expert_up[expert], preferred_element_type=jnp.float32)
            expert_inner = (jax.nn.silu(gate_out) * up_out).astype(jnp.bfloat16)
            produced = jnp.dot(expert_inner, expert_down[expert], preferred_element_type=jnp.float32).astype(jnp.bfloat16)
            weighted = produced.astype(jnp.float32) * entry_weight[entry_ids][:, None]
            return (total_acc.at[token_ids].add(weighted), None)
        partial_sum, _ = lax.scan(add_expert, partial_sum, jnp.arange(EXPERTS // N_TP, dtype=jnp.int32))
        result = result + lax.optimization_barrier(partial_sum.astype(jnp.bfloat16)).astype(jnp.float32)
    return result.astype(jnp.bfloat16)
```

```python
import functools

import jax
import jax.numpy as jnp
from jax import lax
from jax.experimental import pallas as pl
from jax.experimental.pallas import tpu as pltpu
from jax.sharding import PartitionSpec as P

HEAD_SIZE = 64
GRID_W = 64
EPS = 1e-06
THETA = 10000.0
LOG2E = 1.4426950408889634
CAPACITY = 10
SAFE_BOUND = 70.0

VM = pl.BlockSpec(memory_space=pltpu.VMEM)
SM = pl.BlockSpec(memory_space=pltpu.SMEM)


def split_up(value, dim, length):
    dims = value.shape
    tiles = value.reshape(*dims[:dim], length, dims[dim] // length, *dims[dim + 1 :])
    return jnp.moveaxis(tiles, dim, 0)


def sent_and_summed(value, axis, dim):
    length = lax.axis_size(axis)
    tiles = lax.all_to_all(split_up(value, dim, length), axis, 0, 0, tiled=True)
    return jnp.sum(tiles.astype(jnp.float32), axis=0)


def gather_rows(value, axis):
    length = lax.axis_size(axis)
    tiles = lax.all_to_all(
        jnp.broadcast_to(value[None], (length, *value.shape)), axis, 0, 0, tiled=True
    )
    return tiles.reshape(length * value.shape[0], value.shape[1])


def final_norm(field, gain):
    mean_sq = jnp.mean(field * field, axis=-1, keepdims=True)
    return field * lax.rsqrt(mean_sq + EPS) * gain


def wide_tables(positions, sequence_total):
    grid_rows = sequence_total // GRID_W
    row_pos = (positions // GRID_W - grid_rows // 2).astype(jnp.float32)
    col_pos = (positions % GRID_W - GRID_W // 2).astype(jnp.float32)
    quarter = HEAD_SIZE // 4
    inverse = THETA ** (-jnp.arange(quarter, dtype=jnp.float32) / quarter)
    lane = jnp.arange(2 * HEAD_SIZE, dtype=jnp.int32)
    inverse_wide = jnp.tile(inverse, 8)
    is_row = (lane % HEAD_SIZE) < HEAD_SIZE // 2
    angles = jnp.where(is_row[None, :], row_pos[:, None], col_pos[:, None]) * inverse_wide
    sign = jnp.where((lane % 32) < 16, -1.0, 1.0)
    return jnp.cos(angles), jnp.sin(angles) * sign[None, :]


def normed_and_turned(field, gain, cosine, sine):
    lane = lax.broadcasted_iota(jnp.int32, field.shape, 1)
    low = lane < HEAD_SIZE
    square = field * field
    mean_low = jnp.sum(jnp.where(low, square, 0.0), axis=1, keepdims=True) / HEAD_SIZE
    mean_high = jnp.sum(jnp.where(low, 0.0, square), axis=1, keepdims=True) / HEAD_SIZE
    scale = jnp.where(low, lax.rsqrt(mean_low + EPS), lax.rsqrt(mean_high + EPS))
    unit = field * scale * gain
    partner = jnp.where(
        lane % 32 < 16, pltpu.roll(unit, 128 - 16, 1), pltpu.roll(unit, 16, 1)
    )
    return unit * cosine + partner * sine


def prepare_kernel(q_ref, kv_ref, qg_ref, kg_ref, cos_ref, sin_ref, rows_ref, packed_ref):
    tokens = q_ref.shape[0]
    cosine, sine = cos_ref[...], sin_ref[...]
    low = lax.broadcasted_iota(jnp.int32, (tokens, 128), 1) < HEAD_SIZE
    both = kv_ref[...].astype(jnp.float32)
    turned = normed_and_turned(both, kg_ref[...], cosine, sine)
    packed_ref[...] = jnp.where(low, turned, both).astype(jnp.bfloat16)
    for pair in range(q_ref.shape[1] // 128):
        field = q_ref[:, pair * 128 : (pair + 1) * 128].astype(jnp.float32)
        turned = normed_and_turned(field, qg_ref[...], cosine, sine).astype(jnp.bfloat16)
        turned = turned.astype(jnp.float32) * (HEAD_SIZE**-0.5)
        first = jnp.where(low, turned, 0.0)
        second = jnp.where(low, pltpu.roll(turned, HEAD_SIZE, 1), 0.0)
        rows_ref[(2 * pair) * tokens : (2 * pair + 1) * tokens, :] = first.astype(jnp.bfloat16)
        rows_ref[(2 * pair + 1) * tokens : (2 * pair + 2) * tokens, :] = second.astype(jnp.bfloat16)


def attention_kernel(block, flag_ref, q_ref, kv_ref, gain_ref, out_ref, acc_ref, sum_ref, max_ref):
    columns = q_ref.shape[0]
    steps = kv_ref.shape[0] // block
    acc_ref[...] = jnp.zeros_like(acc_ref)
    sum_ref[...] = jnp.zeros_like(sum_ref)

    def scores_of(step):
        slab = kv_ref[pl.ds(pl.multiple_of(step * block, block), block), :]
        scores = lax.dot_general(
            slab, q_ref[...], (((1,), (1,)), ((), ())), preferred_element_type=jnp.float32
        )
        return slab, scores

    def weighed(slab, weights):
        return lax.dot_general(
            slab,
            weights.astype(jnp.bfloat16),
            (((0,), (0,)), ((), ())),
            preferred_element_type=jnp.float32,
        )[HEAD_SIZE:]

    def plain_step(step, carry):
        slab, scores = scores_of(step)
        weights = jnp.exp2(scores * LOG2E)
        sum_ref[...] += jnp.sum(weights.reshape(block // 8, 8, columns), axis=0)
        acc_ref[...] += weighed(slab, weights)
        return carry

    def guarded_step(step, carry):
        slab, scores = scores_of(step)
        before = max_ref[...]
        top = jnp.maximum(before, jnp.max(scores, axis=0, keepdims=True))
        factor = jnp.exp(before - top)
        weights = jnp.exp(scores - top)
        sum_ref[...] = sum_ref[...] * factor + jnp.sum(
            weights.reshape(block // 8, 8, columns), axis=0
        )
        acc_ref[...] = acc_ref[...] * factor + weighed(slab, weights)
        max_ref[...] = top
        return carry

    @pl.when(flag_ref[0] == 0)
    def _():
        lax.fori_loop(0, steps, plain_step, 0)

    @pl.when(flag_ref[0] != 0)
    def _():
        max_ref[...] = jnp.full_like(max_ref, -1e30)
        lax.fori_loop(0, steps, guarded_step, 0)

    attended = acc_ref[...] / jnp.sum(sum_ref[...], axis=0, keepdims=True)
    mean_sq = jnp.mean(attended * attended, axis=0, keepdims=True)
    unit = attended * lax.rsqrt(mean_sq + EPS)
    turned = jnp.concatenate([unit, jnp.zeros_like(unit)], axis=0).T
    tokens = out_ref.shape[0]
    low = lax.broadcasted_iota(jnp.int32, (tokens, 128), 1) < HEAD_SIZE
    for pair in range(out_ref.shape[1] // 128):
        first = turned[(2 * pair) * tokens : (2 * pair + 1) * tokens, :]
        second = turned[(2 * pair + 1) * tokens : (2 * pair + 2) * tokens, :]
        joined = jnp.where(low, first, pltpu.roll(second, HEAD_SIZE, 1))
        lanes = slice(pair * 128, (pair + 1) * 128)
        out_ref[:, lanes] = (joined * gain_ref[:, lanes]).astype(jnp.bfloat16)


def dispatch_kernel(code_ref, normed_ref, out_ref):
    tokens, width = normed_ref.shape
    rows = out_ref.shape[0]
    quarter = width // 4
    row = lax.broadcasted_iota(jnp.int32, (rows, tokens), 0)
    main_code = (row // 8) * 16 + row % 8
    extra_code = (row // 8) * 16 + 8 + (row % 8) // 4
    main = jnp.zeros((rows, tokens), jnp.float32)
    extra = jnp.zeros((rows, tokens), jnp.float32)
    for k in range(code_ref.shape[0]):
        own = code_ref[k : k + 1, :]
        main += jnp.where(main_code == own, 1.0, 0.0)
        extra += jnp.where(extra_code == own, 1.0, 0.0)
    main = main.astype(jnp.bfloat16)
    for q in range(4):
        cols = slice(q * quarter, (q + 1) * quarter)
        out_ref[:, cols] = jnp.dot(
            main, normed_ref[:, cols], preferred_element_type=jnp.float32
        ).astype(jnp.bfloat16)
    total = jnp.zeros((rows, quarter), jnp.float32)
    for q in range(4):
        part = jnp.where(row % 4 == q, extra, 0.0).astype(jnp.bfloat16)
        total += jnp.dot(
            part,
            normed_ref[:, q * quarter : (q + 1) * quarter],
            preferred_element_type=jnp.float32,
        )
    out_ref[:, width:] = total.astype(jnp.bfloat16)


def expert_kernel(in_ref, gate_ref, up_ref, down_ref, out_ref, rows_ref, inner_ref):
    rows = in_ref.shape[0]
    width = gate_ref.shape[0]
    quarter = width // 4
    extra_rows = rows // 4
    rows_ref[:rows, :] = in_ref[:, :width]
    tail = in_ref[:, width:]
    place = lax.broadcasted_iota(jnp.int32, (extra_rows, rows), 1)
    index = lax.broadcasted_iota(jnp.int32, (extra_rows, rows), 0)
    for q in range(4):
        pick = jnp.where(place == 4 * index + q, 1.0, 0.0).astype(jnp.bfloat16)
        rows_ref[rows:, q * quarter : (q + 1) * quarter] = jnp.dot(
            pick, tail, preferred_element_type=jnp.float32
        ).astype(jnp.bfloat16)
    every = rows_ref[...]
    gate = jnp.dot(every, gate_ref[...], preferred_element_type=jnp.float32)
    up = jnp.dot(every, up_ref[...], preferred_element_type=jnp.float32)
    inner_ref[...] = (gate / (1.0 + jnp.exp(-gate)) * up).astype(jnp.bfloat16)
    place = lax.broadcasted_iota(jnp.int32, (rows, extra_rows), 0)
    index = lax.broadcasted_iota(jnp.int32, (rows, extra_rows), 1)
    total = jnp.zeros((rows, quarter), jnp.float32)
    for q in range(4):
        cols = slice(q * quarter, (q + 1) * quarter)
        made = jnp.dot(
            inner_ref[...], down_ref[:, cols], preferred_element_type=jnp.float32
        ).astype(jnp.bfloat16)
        out_ref[:, cols] = made[:rows]
        pick = jnp.where(place == 4 * index + q, 1.0, 0.0).astype(jnp.bfloat16)
        total += jnp.dot(pick, made[rows:], preferred_element_type=jnp.float32)
    out_ref[:, width:] = total.astype(jnp.bfloat16)


def combine_kernel(code_ref, weight_ref, back_ref, inner_ref, down_ref, out_ref):
    tokens, width = out_ref.shape
    rows = back_ref.shape[0]
    quarter = width // 4
    place = lax.broadcasted_iota(jnp.int32, (tokens, rows), 1)
    main_code = (place // 8) * 16 + place % 8
    extra_code = (place // 8) * 16 + 8 + (place % 8) // 4
    main = jnp.zeros((tokens, rows), jnp.float32)
    extra = jnp.zeros((tokens, rows), jnp.float32)
    for k in range(code_ref.shape[1]):
        own = code_ref[:, k : k + 1]
        scale = weight_ref[:, k : k + 1]
        main += jnp.where(main_code == own, scale, 0.0)
        extra += jnp.where(extra_code == own, scale, 0.0)

    def parts_of(value):
        high = value.astype(jnp.bfloat16)
        return high, (value - high.astype(jnp.float32)).astype(jnp.bfloat16)

    high, low = parts_of(main)
    tail = back_ref[:, width:]
    for q in range(4):
        cols = slice(q * quarter, (q + 1) * quarter)
        own_high, own_low = parts_of(jnp.where(place % 4 == q, extra, 0.0))
        total = jnp.dot(inner_ref[...], down_ref[:, cols], preferred_element_type=jnp.float32)
        total += jnp.dot(high, back_ref[:, cols], preferred_element_type=jnp.float32)
        total += jnp.dot(low, back_ref[:, cols], preferred_element_type=jnp.float32)
        total += jnp.dot(own_high, tail, preferred_element_type=jnp.float32)
        total += jnp.dot(own_low, tail, preferred_element_type=jnp.float32)
        out_ref[:, cols] = total.astype(jnp.bfloat16)


def call(kernel, out_shape, args, specs=None, scratch=(), flops=0, moved=0):
    return pl.pallas_call(
        kernel,
        out_shape=out_shape,
        in_specs=specs or [VM] * len(args),
        out_specs=jax.tree.map(lambda _: VM, out_shape),
        scratch_shapes=scratch,
        compiler_params=pltpu.CompilerParams(vmem_limit_bytes=56 * 2**20),
        cost_estimate=pl.CostEstimate(flops=flops, bytes_accessed=moved, transcendentals=0),
    )(*args)


def shaped(dims, kind=jnp.bfloat16):
    return jax.ShapeDtypeStruct(dims, kind)


def slot_codes(routes, tp_index, tp_count, sp_count):
    tokens, top = routes.shape
    flat = routes.reshape(-1)
    is_mine = flat % tp_count == tp_index
    target = flat // tp_count
    onehot = (target[:, None] == jnp.arange(sp_count, dtype=jnp.int32)[None, :]) & is_mine[:, None]
    hot = onehot.astype(jnp.bfloat16)
    entries = tokens * top
    order = jnp.arange(entries, dtype=jnp.int32)
    before = (order[:, None] > order[None, :]).astype(jnp.bfloat16)
    earlier = jnp.dot(before, hot, preferred_element_type=jnp.float32)
    rank = jnp.sum(jnp.where(onehot, earlier, 0.0), axis=1).astype(jnp.int32)
    return jnp.where(is_mine, target * 16 + rank, -1).reshape(tokens, top)


def local(
    queries,
    key_matrix,
    values,
    query_gain,
    key_norm_gain,
    head_gain,
    out_proj,
    residual,
    ffn_gain,
    routes,
    route_weights,
    expert_gate,
    expert_up,
    expert_down,
    shared_gate,
    shared_up,
    shared_down,
):
    tokens = queries.shape[0]
    heads = queries.shape[1] // HEAD_SIZE
    sp_count = lax.axis_size("sp")
    tp_count = lax.axis_size("tp")
    tp_index = lax.axis_index("tp")
    sequence_total = tokens * sp_count
    positions = lax.axis_index("sp") * tokens + jnp.arange(tokens, dtype=jnp.int32)
    cosine, sine = wide_tables(positions, sequence_total)
    columns = heads * tokens
    query_rows, packed = call(
        prepare_kernel,
        (shaped((columns, 128)), shaped((tokens, 128))),
        (
            queries,
            jnp.concatenate([key_matrix, values], axis=1),
            jnp.tile(query_gain, 2)[None],
            jnp.tile(key_norm_gain, 2)[None],
            cosine,
            sine,
        ),
    )
    gathered = lax.all_gather(packed, "sp", axis=0, tiled=True)
    codes = slot_codes(routes, tp_index, tp_count, sp_count)
    bound = 8.0 * jnp.max(jnp.abs(query_gain)) * jnp.max(jnp.abs(key_norm_gain))
    wide = (bound > SAFE_BOUND).astype(jnp.int32)[None]
    head_out = call(
        functools.partial(attention_kernel, 1024),
        shaped((tokens, heads * HEAD_SIZE)),
        (wide, query_rows, gathered, head_gain[None]),
        specs=[SM, VM, VM, VM],
        scratch=(
            pltpu.VMEM((HEAD_SIZE, columns), jnp.float32),
            pltpu.VMEM((8, columns), jnp.float32),
            pltpu.VMEM((1, columns), jnp.float32),
        ),
        flops=4 * columns * sequence_total * 128,
        moved=sequence_total * 256,
    )
    part_rows = tokens // tp_count
    token_heads = lax.all_to_all(head_out, "tp", split_axis=0, concat_axis=1, tiled=True)
    own_resid = lax.dynamic_slice_in_dim(residual, tp_index * part_rows, part_rows, 0)
    hidden_own = (
        own_resid.astype(jnp.float32)
        + jnp.dot(token_heads, out_proj, preferred_element_type=jnp.float32)
    ).astype(jnp.bfloat16)
    normed_own = final_norm(hidden_own.astype(jnp.float32), ffn_gain).astype(jnp.bfloat16)
    normed = gather_rows(normed_own, "tp")
    width = normed.shape[1]
    rows = sp_count * 8
    wide_row = width + width // 4
    outgoing = call(
        dispatch_kernel,
        shaped((rows, wide_row)),
        (codes.T, normed),
        flops=4 * rows * tokens * width,
        moved=rows * wide_row * 2,
    )
    arrived = lax.all_to_all(
        outgoing.reshape(sp_count, 8, wide_row), "sp", split_axis=0, concat_axis=0, tiled=True
    )
    hidden_units = expert_gate.shape[2]
    produced = call(
        expert_kernel,
        shaped((rows, wide_row)),
        (arrived.reshape(rows, wide_row), expert_gate[0], expert_up[0], expert_down[0]),
        scratch=(
            pltpu.VMEM((rows + rows // 4, width), jnp.bfloat16),
            pltpu.VMEM((rows + rows // 4, hidden_units), jnp.bfloat16),
        ),
        flops=6 * rows * width * hidden_units,
        moved=3 * width * hidden_units * 2,
    )
    returned = lax.all_to_all(
        produced.reshape(sp_count, 8, wide_row), "sp", split_axis=0, concat_axis=0, tiled=True
    ).reshape(rows, wide_row)
    gate_part = jnp.dot(normed, shared_gate, preferred_element_type=jnp.float32)
    up_part = jnp.dot(normed, shared_up, preferred_element_type=jnp.float32)
    shared_inner = (jax.nn.silu(gate_part) * up_part).astype(jnp.bfloat16)
    partial = call(
        combine_kernel,
        shaped((tokens, width)),
        (codes, route_weights, returned, shared_inner, shared_down),
        flops=5 * tokens * rows * width,
        moved=rows * wide_row * 2,
    )
    mixed = sent_and_summed(partial, "tp", 0)
    return (hidden_own.astype(jnp.float32) + mixed).astype(jnp.bfloat16)


def solution(mesh):
    placed = (
        P("sp", "tp"),
        P("sp", "tp"),
        P("sp", "tp"),
        P(),
        P(),
        P("tp"),
        P(),
        P("sp", None),
        P(),
        P("sp", None),
        P("sp", None),
        P(("sp", "tp"), None, None),
        P(("sp", "tp"), None, None),
        P(("sp", "tp"), None, None),
        P(None, "tp"),
        P(None, "tp"),
        P("tp", None),
    )
    return jax.shard_map(
        local, mesh=mesh, in_specs=placed, out_specs=P(("sp", "tp"), None), check_vma=False
    )
```

```python
import functools

import jax
import jax.numpy as jnp
from jax import lax
from jax.experimental import pallas as pl
from jax.experimental.pallas import tpu as pltpu
from jax.sharding import PartitionSpec as P

HEAD_SIZE = 64
GRID_W = 64
EPS = 1e-06
THETA = 10000.0
LOG2E = 1.4426950408889634
CAPACITY = 10
SAFE_BOUND = 70.0

VM = pl.BlockSpec(memory_space=pltpu.VMEM)
SM = pl.BlockSpec(memory_space=pltpu.SMEM)


def split_up(value, dim, length):
    dims = value.shape
    tiles = value.reshape(*dims[:dim], length, dims[dim] // length, *dims[dim + 1 :])
    return jnp.moveaxis(tiles, dim, 0)


def sent_and_summed(value, axis, dim):
    length = lax.axis_size(axis)
    tiles = lax.all_to_all(split_up(value, dim, length), axis, 0, 0, tiled=True)
    return jnp.sum(tiles.astype(jnp.float32), axis=0)


def gather_rows(value, axis):
    length = lax.axis_size(axis)
    tiles = lax.all_to_all(
        jnp.broadcast_to(value[None], (length, *value.shape)), axis, 0, 0, tiled=True
    )
    return tiles.reshape(length * value.shape[0], value.shape[1])


def final_norm(field, gain):
    mean_sq = jnp.mean(field * field, axis=-1, keepdims=True)
    return field * lax.rsqrt(mean_sq + EPS) * gain


def wide_tables(positions, sequence_total):
    grid_rows = sequence_total // GRID_W
    row_pos = (positions // GRID_W - grid_rows // 2).astype(jnp.float32)
    col_pos = (positions % GRID_W - GRID_W // 2).astype(jnp.float32)
    quarter = HEAD_SIZE // 4
    inverse = THETA ** (-jnp.arange(quarter, dtype=jnp.float32) / quarter)
    lane = jnp.arange(2 * HEAD_SIZE, dtype=jnp.int32)
    inverse_wide = jnp.tile(inverse, 8)
    is_row = (lane % HEAD_SIZE) < HEAD_SIZE // 2
    angles = jnp.where(is_row[None, :], row_pos[:, None], col_pos[:, None]) * inverse_wide
    sign = jnp.where((lane % 32) < 16, -1.0, 1.0)
    return jnp.cos(angles), jnp.sin(angles) * sign[None, :]


def normed_and_turned(field, gain, cosine, sine):
    lane = lax.broadcasted_iota(jnp.int32, field.shape, 1)
    low = lane < HEAD_SIZE
    square = field * field
    mean_low = jnp.sum(jnp.where(low, square, 0.0), axis=1, keepdims=True) / HEAD_SIZE
    mean_high = jnp.sum(jnp.where(low, 0.0, square), axis=1, keepdims=True) / HEAD_SIZE
    scale = jnp.where(low, lax.rsqrt(mean_low + EPS), lax.rsqrt(mean_high + EPS))
    unit = field * scale * gain
    partner = jnp.where(
        lane % 32 < 16, pltpu.roll(unit, 128 - 16, 1), pltpu.roll(unit, 16, 1)
    )
    return unit * cosine + partner * sine


def prepare_kernel(q_ref, kv_ref, qg_ref, kg_ref, cos_ref, sin_ref, rows_ref, packed_ref):
    tokens = q_ref.shape[0]
    cosine, sine = cos_ref[...], sin_ref[...]
    low = lax.broadcasted_iota(jnp.int32, (tokens, 128), 1) < HEAD_SIZE
    both = kv_ref[...].astype(jnp.float32)
    turned = normed_and_turned(both, kg_ref[...], cosine, sine)
    packed_ref[...] = jnp.where(low, turned, both).astype(jnp.bfloat16)
    for pair in range(q_ref.shape[1] // 128):
        field = q_ref[:, pair * 128 : (pair + 1) * 128].astype(jnp.float32)
        turned = normed_and_turned(field, qg_ref[...], cosine, sine).astype(jnp.bfloat16)
        turned = turned.astype(jnp.float32) * (HEAD_SIZE**-0.5)
        first = jnp.where(low, turned, 0.0)
        second = jnp.where(low, pltpu.roll(turned, HEAD_SIZE, 1), 0.0)
        rows_ref[(2 * pair) * tokens : (2 * pair + 1) * tokens, :] = first.astype(jnp.bfloat16)
        rows_ref[(2 * pair + 1) * tokens : (2 * pair + 2) * tokens, :] = second.astype(jnp.bfloat16)


MESH = pl.DeviceIdType.MESH
Z_RING, X_RING = 8, 4


def ring_attention_kernel(
    guarded,
    q_ref,
    packed_ref,
    gain_ref,
    out_ref,
    kv_ref,
    mine_ref,
    acc_ref,
    sum_ref,
    max_ref,
    x_send,
    x_recv,
    z_send,
    z_recv,
    p_send,
    p_recv,
    t_send,
    t_recv,
    l_sem,
):
    tokens = packed_ref.shape[0]
    columns = q_ref.shape[0]
    group = X_RING * tokens
    sp, tp = lax.axis_index("sp"), lax.axis_index("tp")
    tp_count = lax.axis_size("tp")
    core = sp % 2
    x = (sp // 2) % X_RING
    z = sp // (2 * X_RING)

    def device(z_at, x_at, core_at):
        return {"sp": ((z_at % Z_RING) * X_RING + x_at % X_RING) * 2 + core_at}

    barrier = pltpu.get_barrier_semaphore()
    others = [device(z, x + r, core) for r in range(1, X_RING)]
    others += [device(z + 1, x, core), device(z + Z_RING - 1, x, core), device(z, x, 1 - core)]
    others += [{"tp": (tp + r) % tp_count} for r in range(1, tp_count)]
    for other in others:
        pl.semaphore_signal(barrier, inc=1, device_id=other, device_id_type=MESH)
    pl.semaphore_wait(barrier, len(others))

    def slot(x_at):
        return kv_ref.at[z, core, pl.ds(pl.multiple_of((x_at % X_RING) * tokens, tokens), tokens)]

    def remote(src, dst, send_sem, recv_sem, to):
        return pltpu.make_async_remote_copy(
            src_ref=src,
            dst_ref=dst,
            send_sem=send_sem,
            recv_sem=recv_sem,
            device_id=to,
            device_id_type=MESH,
        )

    def x_copy(r, source_x):
        place = slot(source_x)
        return remote(
            packed_ref, place, x_send.at[r - 1], x_recv.at[r - 1], device(z, x + r, core)
        )

    def z_copy(way, hop, z_from):
        rows = pl.ds(0, group)
        if hop == Z_RING // 2 - 1:
            rows = pl.ds(way * (group // 2), group // 2)
        place = kv_ref.at[z_from % Z_RING, core, rows]
        to = device(z + (1 if way == 0 else Z_RING - 1), x, core)
        return remote(place, place, z_send.at[way, hop], z_recv.at[way, hop], to)

    def z_out(way, hop):
        return z_copy(way, hop, z + (Z_RING - hop if way == 0 else hop))

    def z_in(way, hop):
        return z_copy(way, hop, z + (Z_RING - 1 - hop if way == 0 else 1 + hop))

    def p_copy(number, z_at, core_at):
        place = kv_ref.at[z_at % Z_RING, core_at]
        return remote(
            place, place, p_send.at[number], p_recv.at[number], device(z, x, 1 - core)
        )

    def p_out(number):
        distance = (number + 1) // 2
        return p_copy(number, z + (Z_RING - distance if number % 2 else distance), core)

    own = pltpu.make_async_copy(packed_ref, slot(x), l_sem)
    own.start()
    for r in range(1, X_RING):
        x_copy(r, x).start()
    acc_ref[...] = jnp.zeros_like(acc_ref)
    sum_ref[...] = jnp.zeros_like(sum_ref)
    if guarded:
        max_ref[...] = jnp.full_like(max_ref, -1e30)
    own.wait()
    for r in range(1, X_RING):
        x_copy(r, x + X_RING - r).wait_recv()
    z_out(0, 0).start()
    z_out(1, 0).start()
    p_out(0).start()

    def step(j, carry):
        i = j + 2
        distance, member = i // 4, i % 4
        z_at = (z + Z_RING + distance * (2 * (member // 2) - 1)) % Z_RING
        core_at = (core + member % 2) % 2

        for hop in range(Z_RING // 2):

            @pl.when(j == 4 * hop + 2)
            def _(hop=hop):
                z_in(0, hop).wait_recv()
                z_in(1, hop).wait_recv()
                if hop < Z_RING // 2 - 1:
                    z_out(0, hop + 1).start()
                    z_out(1, hop + 1).start()
                    p_out(2 * hop + 1).start()
                    p_out(2 * hop + 2).start()
                else:
                    p_out(2 * hop + 1).start()

        @pl.when(member % 2 == 1)
        def _():
            p_copy(j // 2, z_at, 1 - core).wait_recv()

        slab = kv_ref[z_at, core_at]
        scores = lax.dot_general(
            slab, q_ref[...], (((1,), (1,)), ((), ())), preferred_element_type=jnp.float32
        )
        if guarded:
            before = max_ref[...]
            top = jnp.maximum(before, jnp.max(scores, axis=0, keepdims=True))
            factor = jnp.exp(before - top)
            weights = jnp.exp(scores - top)
            max_ref[...] = top
        else:
            factor = None
            weights = jnp.exp2(scores * LOG2E)
        added = jnp.sum(weights.reshape(group // 8, 8, columns), axis=0)
        mixed = lax.dot_general(
            slab,
            weights.astype(jnp.bfloat16),
            (((0,), (0,)), ((), ())),
            preferred_element_type=jnp.float32,
        )[HEAD_SIZE:]
        if guarded:
            sum_ref[...] = sum_ref[...] * factor + added
            acc_ref[...] = acc_ref[...] * factor + mixed
        else:
            sum_ref[...] += added
            acc_ref[...] += mixed
        return carry

    lax.fori_loop(0, 2 * Z_RING, step, 0)

    attended = acc_ref[...] / jnp.sum(sum_ref[...], axis=0, keepdims=True)
    mean_sq = jnp.mean(attended * attended, axis=0, keepdims=True)
    unit = attended * lax.rsqrt(mean_sq + EPS)
    turned = jnp.concatenate([unit, jnp.zeros_like(unit)], axis=0).T
    low = lax.broadcasted_iota(jnp.int32, (tokens, 128), 1) < HEAD_SIZE
    for pair in range(mine_ref.shape[1] // 128):
        first = turned[(2 * pair) * tokens : (2 * pair + 1) * tokens, :]
        second = turned[(2 * pair + 1) * tokens : (2 * pair + 2) * tokens, :]
        joined = jnp.where(low, first, pltpu.roll(second, HEAD_SIZE, 1))
        lanes = slice(pair * 128, (pair + 1) * 128)
        mine_ref[:, lanes] = (joined * gain_ref[:, lanes]).astype(jnp.bfloat16)

    part = tokens // tp_count

    def rows_of(owner):
        return mine_ref.at[pl.ds(pl.multiple_of((owner % tp_count) * part, part), part)]

    def t_copy(r, source):
        return remote(
            rows_of(tp + r),
            out_ref.at[source % tp_count],
            t_send.at[r - 1],
            t_recv.at[r - 1],
            {"tp": (tp + r) % tp_count},
        )

    for r in range(1, tp_count):
        t_copy(r, tp).start()
    own = pltpu.make_async_copy(rows_of(tp), out_ref.at[tp], l_sem)
    own.start()
    own.wait()
    for r in range(1, X_RING):
        x_copy(r, x).wait_send()
    for way in range(2):
        for hop in range(Z_RING // 2):
            z_out(way, hop).wait_send()
    for number in range(Z_RING):
        p_out(number).wait_send()
    for r in range(1, tp_count):
        t_copy(r, tp + tp_count - r).wait_recv()
        t_copy(r, tp).wait_send()


def dispatch_kernel(code_ref, normed_ref, out_ref):
    tokens, width = normed_ref.shape
    rows = out_ref.shape[0]
    quarter = width // 4
    row = lax.broadcasted_iota(jnp.int32, (rows, tokens), 0)
    main_code = (row // 8) * 16 + row % 8
    extra_code = (row // 8) * 16 + 8 + (row % 8) // 4
    main = jnp.zeros((rows, tokens), jnp.float32)
    extra = jnp.zeros((rows, tokens), jnp.float32)
    for k in range(code_ref.shape[0]):
        own = code_ref[k : k + 1, :]
        main += jnp.where(main_code == own, 1.0, 0.0)
        extra += jnp.where(extra_code == own, 1.0, 0.0)
    main = main.astype(jnp.bfloat16)
    for q in range(4):
        cols = slice(q * quarter, (q + 1) * quarter)
        out_ref[:, cols] = jnp.dot(
            main, normed_ref[:, cols], preferred_element_type=jnp.float32
        ).astype(jnp.bfloat16)
    total = jnp.zeros((rows, quarter), jnp.float32)
    for q in range(4):
        part = jnp.where(row % 4 == q, extra, 0.0).astype(jnp.bfloat16)
        total += jnp.dot(
            part,
            normed_ref[:, q * quarter : (q + 1) * quarter],
            preferred_element_type=jnp.float32,
        )
    out_ref[:, width:] = total.astype(jnp.bfloat16)


def expert_kernel(in_ref, gate_ref, up_ref, down_ref, out_ref, rows_ref, inner_ref):
    rows = in_ref.shape[0]
    width = gate_ref.shape[0]
    quarter = width // 4
    extra_rows = rows // 4
    rows_ref[:rows, :] = in_ref[:, :width]
    tail = in_ref[:, width:]
    place = lax.broadcasted_iota(jnp.int32, (extra_rows, rows), 1)
    index = lax.broadcasted_iota(jnp.int32, (extra_rows, rows), 0)
    for q in range(4):
        pick = jnp.where(place == 4 * index + q, 1.0, 0.0).astype(jnp.bfloat16)
        rows_ref[rows:, q * quarter : (q + 1) * quarter] = jnp.dot(
            pick, tail, preferred_element_type=jnp.float32
        ).astype(jnp.bfloat16)
    every = rows_ref[...]
    gate = jnp.dot(every, gate_ref[...], preferred_element_type=jnp.float32)
    up = jnp.dot(every, up_ref[...], preferred_element_type=jnp.float32)
    inner_ref[...] = (gate / (1.0 + jnp.exp(-gate)) * up).astype(jnp.bfloat16)
    place = lax.broadcasted_iota(jnp.int32, (rows, extra_rows), 0)
    index = lax.broadcasted_iota(jnp.int32, (rows, extra_rows), 1)
    total = jnp.zeros((rows, quarter), jnp.float32)
    for q in range(4):
        cols = slice(q * quarter, (q + 1) * quarter)
        made = jnp.dot(
            inner_ref[...], down_ref[:, cols], preferred_element_type=jnp.float32
        ).astype(jnp.bfloat16)
        out_ref[:, cols] = made[:rows]
        pick = jnp.where(place == 4 * index + q, 1.0, 0.0).astype(jnp.bfloat16)
        total += jnp.dot(pick, made[rows:], preferred_element_type=jnp.float32)
    out_ref[:, width:] = total.astype(jnp.bfloat16)


def combine_kernel(code_ref, weight_ref, back_ref, inner_ref, down_ref, out_ref):
    tokens, width = out_ref.shape
    rows = back_ref.shape[0]
    quarter = width // 4
    place = lax.broadcasted_iota(jnp.int32, (tokens, rows), 1)
    main_code = (place // 8) * 16 + place % 8
    extra_code = (place // 8) * 16 + 8 + (place % 8) // 4
    main = jnp.zeros((tokens, rows), jnp.float32)
    extra = jnp.zeros((tokens, rows), jnp.float32)
    for k in range(code_ref.shape[1]):
        own = code_ref[:, k : k + 1]
        scale = weight_ref[:, k : k + 1]
        main += jnp.where(main_code == own, scale, 0.0)
        extra += jnp.where(extra_code == own, scale, 0.0)

    def parts_of(value):
        high = value.astype(jnp.bfloat16)
        return high, (value - high.astype(jnp.float32)).astype(jnp.bfloat16)

    high, low = parts_of(main)
    tail = back_ref[:, width:]
    for q in range(4):
        cols = slice(q * quarter, (q + 1) * quarter)
        own_high, own_low = parts_of(jnp.where(place % 4 == q, extra, 0.0))
        total = jnp.dot(inner_ref[...], down_ref[:, cols], preferred_element_type=jnp.float32)
        total += jnp.dot(high, back_ref[:, cols], preferred_element_type=jnp.float32)
        total += jnp.dot(low, back_ref[:, cols], preferred_element_type=jnp.float32)
        total += jnp.dot(own_high, tail, preferred_element_type=jnp.float32)
        total += jnp.dot(own_low, tail, preferred_element_type=jnp.float32)
        out_ref[:, cols] = total.astype(jnp.bfloat16)


def call(kernel, out_shape, args, specs=None, scratch=(), flops=0, moved=0):
    return pl.pallas_call(
        kernel,
        out_shape=out_shape,
        in_specs=specs or [VM] * len(args),
        out_specs=jax.tree.map(lambda _: VM, out_shape),
        scratch_shapes=scratch,
        compiler_params=pltpu.CompilerParams(vmem_limit_bytes=56 * 2**20),
        cost_estimate=pl.CostEstimate(flops=flops, bytes_accessed=moved, transcendentals=0),
    )(*args)


def shaped(dims, kind=jnp.bfloat16):
    return jax.ShapeDtypeStruct(dims, kind)


def slot_codes(routes, tp_index, tp_count, sp_count):
    tokens, top = routes.shape
    flat = routes.reshape(-1)
    is_mine = flat % tp_count == tp_index
    target = flat // tp_count
    onehot = (target[:, None] == jnp.arange(sp_count, dtype=jnp.int32)[None, :]) & is_mine[:, None]
    hot = onehot.astype(jnp.bfloat16)
    entries = tokens * top
    order = jnp.arange(entries, dtype=jnp.int32)
    before = (order[:, None] > order[None, :]).astype(jnp.bfloat16)
    earlier = jnp.dot(before, hot, preferred_element_type=jnp.float32)
    rank = jnp.sum(jnp.where(onehot, earlier, 0.0), axis=1).astype(jnp.int32)
    return jnp.where(is_mine, target * 16 + rank, -1).reshape(tokens, top)


def local(
    queries,
    key_matrix,
    values,
    query_gain,
    key_norm_gain,
    head_gain,
    out_proj,
    residual,
    ffn_gain,
    routes,
    route_weights,
    expert_gate,
    expert_up,
    expert_down,
    shared_gate,
    shared_up,
    shared_down,
):
    tokens = queries.shape[0]
    heads = queries.shape[1] // HEAD_SIZE
    sp_count = lax.axis_size("sp")
    tp_count = lax.axis_size("tp")
    tp_index = lax.axis_index("tp")
    sequence_total = tokens * sp_count
    positions = lax.axis_index("sp") * tokens + jnp.arange(tokens, dtype=jnp.int32)
    cosine, sine = wide_tables(positions, sequence_total)
    columns = heads * tokens
    query_rows, packed = call(
        prepare_kernel,
        (shaped((columns, 128)), shaped((tokens, 128))),
        (
            queries,
            jnp.concatenate([key_matrix, values], axis=1),
            jnp.tile(query_gain, 2)[None],
            jnp.tile(key_norm_gain, 2)[None],
            cosine,
            sine,
        ),
    )
    codes = slot_codes(routes, tp_index, tp_count, sp_count)
    bound = 8.0 * jnp.max(jnp.abs(query_gain)) * jnp.max(jnp.abs(key_norm_gain))
    part_rows = tokens // tp_count

    def attention(guarded, number):
        def run(rows, own, gain):
            return pl.pallas_call(
                functools.partial(ring_attention_kernel, guarded),
                out_shape=shaped((tp_count, part_rows, heads * HEAD_SIZE)),
                in_specs=[VM, VM, VM],
                out_specs=VM,
                scratch_shapes=[
                    pltpu.VMEM((Z_RING, 2, X_RING * tokens, 128), jnp.bfloat16),
                    pltpu.VMEM((tokens, heads * HEAD_SIZE), jnp.bfloat16),
                    pltpu.VMEM((HEAD_SIZE, columns), jnp.float32),
                    pltpu.VMEM((8, columns), jnp.float32),
                    pltpu.VMEM((1, columns), jnp.float32),
                    pltpu.SemaphoreType.DMA((X_RING - 1,)),
                    pltpu.SemaphoreType.DMA((X_RING - 1,)),
                    pltpu.SemaphoreType.DMA((2, Z_RING // 2)),
                    pltpu.SemaphoreType.DMA((2, Z_RING // 2)),
                    pltpu.SemaphoreType.DMA((Z_RING,)),
                    pltpu.SemaphoreType.DMA((Z_RING,)),
                    pltpu.SemaphoreType.DMA((tp_count - 1,)),
                    pltpu.SemaphoreType.DMA((tp_count - 1,)),
                    pltpu.SemaphoreType.DMA,
                ],
                compiler_params=pltpu.CompilerParams(
                    vmem_limit_bytes=56 * 2**20, collective_id=number, has_side_effects=True
                ),
                cost_estimate=pl.CostEstimate(
                    flops=4 * columns * sequence_total * 128,
                    bytes_accessed=sequence_total * 256,
                    transcendentals=0,
                ),
            )(rows, own, gain)

        return run

    tiles = lax.cond(
        bound > SAFE_BOUND,
        attention(True, 1),
        attention(False, 0),
        query_rows,
        packed,
        head_gain[None],
    )
    token_heads = jnp.concatenate([tiles[t] for t in range(tp_count)], axis=1)
    own_resid = lax.dynamic_slice_in_dim(residual, tp_index * part_rows, part_rows, 0)
    hidden_own = (
        own_resid.astype(jnp.float32)
        + jnp.dot(token_heads, out_proj, preferred_element_type=jnp.float32)
    ).astype(jnp.bfloat16)
    normed_own = final_norm(hidden_own.astype(jnp.float32), ffn_gain).astype(jnp.bfloat16)
    normed = gather_rows(normed_own, "tp")
    width = normed.shape[1]
    rows = sp_count * 8
    wide_row = width + width // 4
    outgoing = call(
        dispatch_kernel,
        shaped((rows, wide_row)),
        (codes.T, normed),
        flops=4 * rows * tokens * width,
        moved=rows * wide_row * 2,
    )
    arrived = lax.all_to_all(
        outgoing.reshape(sp_count, 8, wide_row), "sp", split_axis=0, concat_axis=0, tiled=True
    )
    hidden_units = expert_gate.shape[2]
    produced = call(
        expert_kernel,
        shaped((rows, wide_row)),
        (arrived.reshape(rows, wide_row), expert_gate[0], expert_up[0], expert_down[0]),
        scratch=(
            pltpu.VMEM((rows + rows // 4, width), jnp.bfloat16),
            pltpu.VMEM((rows + rows // 4, hidden_units), jnp.bfloat16),
        ),
        flops=6 * rows * width * hidden_units,
        moved=3 * width * hidden_units * 2,
    )
    returned = lax.all_to_all(
        produced.reshape(sp_count, 8, wide_row), "sp", split_axis=0, concat_axis=0, tiled=True
    ).reshape(rows, wide_row)
    gate_part = jnp.dot(normed, shared_gate, preferred_element_type=jnp.float32)
    up_part = jnp.dot(normed, shared_up, preferred_element_type=jnp.float32)
    shared_inner = (jax.nn.silu(gate_part) * up_part).astype(jnp.bfloat16)
    partial = call(
        combine_kernel,
        shaped((tokens, width)),
        (codes, route_weights, returned, shared_inner, shared_down),
        flops=5 * tokens * rows * width,
        moved=rows * wide_row * 2,
    )
    mixed = sent_and_summed(partial, "tp", 0)
    return (hidden_own.astype(jnp.float32) + mixed).astype(jnp.bfloat16)


def solution(mesh):
    placed = (
        P("sp", "tp"),
        P("sp", "tp"),
        P("sp", "tp"),
        P(),
        P(),
        P("tp"),
        P(),
        P("sp", None),
        P(),
        P("sp", None),
        P("sp", None),
        P(("sp", "tp"), None, None),
        P(("sp", "tp"), None, None),
        P(("sp", "tp"), None, None),
        P(None, "tp"),
        P(None, "tp"),
        P("tp", None),
    )
    return jax.shard_map(
        local, mesh=mesh, in_specs=placed, out_specs=P(("sp", "tp"), None), check_vma=False
    )
```

```python
import functools

import jax
import jax.numpy as jnp
from jax import lax
from jax.experimental import pallas as pl
from jax.experimental.pallas import tpu as pltpu
from jax.sharding import PartitionSpec as P

HEAD_SIZE = 64
GRID_W = 64
EPS = 1e-06
THETA = 10000.0
LOG2E = 1.4426950408889634
CAPACITY = 10
SAFE_BOUND = 70.0

VM = pl.BlockSpec(memory_space=pltpu.VMEM)
ANY = pl.BlockSpec(memory_space=pl.ANY)


def final_norm(field, gain):
    mean_sq = jnp.mean(field * field, axis=-1, keepdims=True)
    return field * lax.rsqrt(mean_sq + EPS) * gain


def wide_tables(positions, sequence_total):
    grid_rows = sequence_total // GRID_W
    row_pos = (positions // GRID_W - grid_rows // 2).astype(jnp.float32)
    col_pos = (positions % GRID_W - GRID_W // 2).astype(jnp.float32)
    quarter = HEAD_SIZE // 4
    inverse = THETA ** (-jnp.arange(quarter, dtype=jnp.float32) / quarter)
    lane = jnp.arange(2 * HEAD_SIZE, dtype=jnp.int32)
    inverse_wide = jnp.tile(inverse, 8)
    is_row = (lane % HEAD_SIZE) < HEAD_SIZE // 2
    angles = jnp.where(is_row[None, :], row_pos[:, None], col_pos[:, None]) * inverse_wide
    sign = jnp.where((lane % 32) < 16, -1.0, 1.0)
    return jnp.cos(angles), jnp.sin(angles) * sign[None, :]


def normed_and_turned(field, gain, cosine, sine):
    lane = lax.broadcasted_iota(jnp.int32, field.shape, 1)
    low = lane < HEAD_SIZE
    square = field * field
    mean_low = jnp.sum(jnp.where(low, square, 0.0), axis=1, keepdims=True) / HEAD_SIZE
    mean_high = jnp.sum(jnp.where(low, 0.0, square), axis=1, keepdims=True) / HEAD_SIZE
    scale = jnp.where(low, lax.rsqrt(mean_low + EPS), lax.rsqrt(mean_high + EPS))
    unit = field * scale * gain
    partner = jnp.where(
        lane % 32 < 16, pltpu.roll(unit, 128 - 16, 1), pltpu.roll(unit, 16, 1)
    )
    return unit * cosine + partner * sine


def prepare_kernel(q_ref, kv_ref, qg_ref, kg_ref, cos_ref, sin_ref, rows_ref, packed_ref):
    tokens = q_ref.shape[0]
    cosine, sine = cos_ref[...], sin_ref[...]
    low = lax.broadcasted_iota(jnp.int32, (tokens, 128), 1) < HEAD_SIZE
    both = kv_ref[...].astype(jnp.float32)
    turned = normed_and_turned(both, kg_ref[...], cosine, sine)
    packed_ref[...] = jnp.where(low, turned, both).astype(jnp.bfloat16)
    for pair in range(q_ref.shape[1] // 128):
        field = q_ref[:, pair * 128 : (pair + 1) * 128].astype(jnp.float32)
        turned = normed_and_turned(field, qg_ref[...], cosine, sine).astype(jnp.bfloat16)
        turned = turned.astype(jnp.float32) * (HEAD_SIZE**-0.5)
        first = jnp.where(low, turned, 0.0)
        second = jnp.where(low, pltpu.roll(turned, HEAD_SIZE, 1), 0.0)
        rows_ref[(2 * pair) * tokens : (2 * pair + 1) * tokens, :] = first.astype(jnp.bfloat16)
        rows_ref[(2 * pair + 1) * tokens : (2 * pair + 2) * tokens, :] = second.astype(jnp.bfloat16)


MESH = pl.DeviceIdType.MESH
Z_RING, X_RING = 8, 4
PLANE = 2 * X_RING


def ring_attention_kernel(
    guarded,
    q_ref,
    packed_ref,
    gain_ref,
    out_ref,
    kv_ref,
    mine_ref,
    acc_ref,
    sum_ref,
    max_ref,
    x_send,
    x_recv,
    z_send,
    z_recv,
    p_send,
    p_recv,
    t_send,
    t_recv,
    l_sem,
):
    tokens = packed_ref.shape[0]
    columns = q_ref.shape[0]
    group = X_RING * tokens
    sp, tp = lax.axis_index("sp"), lax.axis_index("tp")
    tp_count = lax.axis_size("tp")
    core = sp % 2
    x = (sp // 2) % X_RING
    z = sp // (2 * X_RING)

    def device(z_at, x_at, core_at):
        return {"sp": ((z_at % Z_RING) * X_RING + x_at % X_RING) * 2 + core_at}

    barrier = pltpu.get_barrier_semaphore()
    others = [device(z, x + r, core) for r in range(1, X_RING)]
    others += [device(z + 1, x, core), device(z + Z_RING - 1, x, core), device(z, x, 1 - core)]
    others += [{"tp": (tp + r) % tp_count} for r in range(1, tp_count)]
    for other in others:
        pl.semaphore_signal(barrier, inc=1, device_id=other, device_id_type=MESH)
    pl.semaphore_wait(barrier, len(others))

    def slot(x_at):
        return kv_ref.at[z, core, pl.ds(pl.multiple_of((x_at % X_RING) * tokens, tokens), tokens)]

    def remote(src, dst, send_sem, recv_sem, to):
        return pltpu.make_async_remote_copy(
            src_ref=src,
            dst_ref=dst,
            send_sem=send_sem,
            recv_sem=recv_sem,
            device_id=to,
            device_id_type=MESH,
        )

    def x_copy(r, source_x):
        place = slot(source_x)
        return remote(
            packed_ref, place, x_send.at[r - 1], x_recv.at[r - 1], device(z, x + r, core)
        )

    def z_copy(way, hop, z_from):
        rows = pl.ds(0, group)
        if hop == Z_RING // 2 - 1:
            rows = pl.ds(way * (group // 2), group // 2)
        place = kv_ref.at[z_from % Z_RING, core, rows]
        to = device(z + (1 if way == 0 else Z_RING - 1), x, core)
        return remote(place, place, z_send.at[way, hop], z_recv.at[way, hop], to)

    def z_out(way, hop):
        return z_copy(way, hop, z + (Z_RING - hop if way == 0 else hop))

    def z_in(way, hop):
        return z_copy(way, hop, z + (Z_RING - 1 - hop if way == 0 else 1 + hop))

    def p_copy(number, z_at, core_at):
        place = kv_ref.at[z_at % Z_RING, core_at]
        return remote(
            place, place, p_send.at[number], p_recv.at[number], device(z, x, 1 - core)
        )

    def p_out(number):
        distance = (number + 1) // 2
        return p_copy(number, z + (Z_RING - distance if number % 2 else distance), core)

    own = pltpu.make_async_copy(packed_ref, slot(x), l_sem)
    own.start()
    for r in range(1, X_RING):
        x_copy(r, x).start()
    acc_ref[...] = jnp.zeros_like(acc_ref)
    sum_ref[...] = jnp.zeros_like(sum_ref)
    if guarded:
        max_ref[...] = jnp.full_like(max_ref, -1e30)
    own.wait()
    for r in range(1, X_RING):
        x_copy(r, x + X_RING - r).wait_recv()
    z_out(0, 0).start()
    z_out(1, 0).start()
    p_out(0).start()

    def step(j, carry):
        i = j + 2
        distance, member = i // 4, i % 4
        z_at = (z + Z_RING + distance * (2 * (member // 2) - 1)) % Z_RING
        core_at = (core + member % 2) % 2

        for hop in range(Z_RING // 2):

            @pl.when(j == 4 * hop + 2)
            def _(hop=hop):
                z_in(0, hop).wait_recv()
                z_in(1, hop).wait_recv()
                if hop < Z_RING // 2 - 1:
                    z_out(0, hop + 1).start()
                    z_out(1, hop + 1).start()
                    p_out(2 * hop + 1).start()
                    p_out(2 * hop + 2).start()
                else:
                    p_out(2 * hop + 1).start()

        @pl.when(member % 2 == 1)
        def _():
            p_copy(j // 2, z_at, 1 - core).wait_recv()

        slab = kv_ref[z_at, core_at]
        scores = lax.dot_general(
            slab, q_ref[...], (((1,), (1,)), ((), ())), preferred_element_type=jnp.float32
        )
        if guarded:
            before = max_ref[...]
            top = jnp.maximum(before, jnp.max(scores, axis=0, keepdims=True))
            factor = jnp.exp(before - top)
            weights = jnp.exp(scores - top)
            max_ref[...] = top
        else:
            factor = None
            weights = jnp.exp2(scores * LOG2E)
        added = jnp.sum(weights.reshape(group // 8, 8, columns), axis=0)
        mixed = lax.dot_general(
            slab,
            weights.astype(jnp.bfloat16),
            (((0,), (0,)), ((), ())),
            preferred_element_type=jnp.float32,
        )[HEAD_SIZE:]
        if guarded:
            sum_ref[...] = sum_ref[...] * factor + added
            acc_ref[...] = acc_ref[...] * factor + mixed
        else:
            sum_ref[...] += added
            acc_ref[...] += mixed
        return carry

    lax.fori_loop(0, 2 * Z_RING, step, 0)

    attended = acc_ref[...] / jnp.sum(sum_ref[...], axis=0, keepdims=True)
    mean_sq = jnp.mean(attended * attended, axis=0, keepdims=True)
    unit = attended * lax.rsqrt(mean_sq + EPS)
    turned = jnp.concatenate([unit, jnp.zeros_like(unit)], axis=0).T
    low = lax.broadcasted_iota(jnp.int32, (tokens, 128), 1) < HEAD_SIZE
    for pair in range(mine_ref.shape[1] // 128):
        first = turned[(2 * pair) * tokens : (2 * pair + 1) * tokens, :]
        second = turned[(2 * pair + 1) * tokens : (2 * pair + 2) * tokens, :]
        joined = jnp.where(low, first, pltpu.roll(second, HEAD_SIZE, 1))
        lanes = slice(pair * 128, (pair + 1) * 128)
        mine_ref[:, lanes] = (joined * gain_ref[:, lanes]).astype(jnp.bfloat16)

    part = tokens // tp_count

    def rows_of(owner):
        return mine_ref.at[pl.ds(pl.multiple_of((owner % tp_count) * part, part), part)]

    def t_copy(r, source):
        return remote(
            rows_of(tp + r),
            out_ref.at[source % tp_count],
            t_send.at[r - 1],
            t_recv.at[r - 1],
            {"tp": (tp + r) % tp_count},
        )

    for r in range(1, tp_count):
        t_copy(r, tp).start()
    own = pltpu.make_async_copy(rows_of(tp), out_ref.at[tp], l_sem)
    own.start()
    own.wait()
    for r in range(1, X_RING):
        x_copy(r, x).wait_send()
    for way in range(2):
        for hop in range(Z_RING // 2):
            z_out(way, hop).wait_send()
    for number in range(Z_RING):
        p_out(number).wait_send()
    for r in range(1, tp_count):
        t_copy(r, tp + tp_count - r).wait_recv()
        t_copy(r, tp).wait_send()


def moe_kernel(
    heads_ref,
    out_proj_ref,
    residual_ref,
    ffn_gain_ref,
    code_ref,
    code_t_ref,
    weight_ref,
    shared_gate_ref,
    shared_up_ref,
    shared_down_ref,
    gate_hbm,
    up_hbm,
    down_hbm,
    out_ref,
    own_ref,
    hidden_ref,
    normed_ref,
    leaving_ref,
    passing_ref,
    arrived_ref,
    made_ref,
    back_passing_ref,
    back_ref,
    acc_ref,
    part_ref,
    got_ref,
    gate_ref,
    up_ref,
    down_ref,
    w_sem,
    l_sem,
    y_send,
    y_recv,
    s_send,
    s_recv,
    z_send,
    z_recv,
    i_send,
    i_recv,
    i_local,
    bz_send,
    bz_recv,
    bi_send,
    bi_recv,
    bi_local,
):
    sp, tp = lax.axis_index("sp"), lax.axis_index("tp")
    tp_count = lax.axis_size("tp")
    z, i = sp // PLANE, sp % PLANE
    part, width = hidden_ref.shape
    tokens = part * tp_count
    quarter = width // 4
    rows = PLANE * 8
    top = code_ref.shape[1]

    def at_z(z_at):
        return {"sp": (z_at % Z_RING) * PLANE + i}

    def at_i(i_at):
        return {"sp": z * PLANE + i_at % PLANE}

    def at_tp(t):
        return {"tp": t % tp_count}

    barrier = pltpu.get_barrier_semaphore()
    others = [at_z(z + k) for k in range(1, Z_RING)]
    others += [at_i(i + r) for r in range(1, PLANE)]
    others += [at_tp(tp + r) for r in range(1, tp_count)]
    for other in others:
        pl.semaphore_signal(barrier, inc=1, device_id=other, device_id_type=MESH)

    loads = [
        pltpu.make_async_copy(
            residual_ref.at[pl.ds(pl.multiple_of(tp * part, part), part)], own_ref, l_sem
        ),
        pltpu.make_async_copy(gate_hbm, gate_ref, w_sem.at[0]),
        pltpu.make_async_copy(up_hbm, up_ref, w_sem.at[1]),
        pltpu.make_async_copy(down_hbm, down_ref, w_sem.at[2]),
    ]
    for load in loads:
        load.start()

    def remote(src, dst, send_sem, recv_sem, to):
        return pltpu.make_async_remote_copy(
            src_ref=src,
            dst_ref=dst,
            send_sem=send_sem,
            recv_sem=recv_sem,
            device_id=to,
            device_id_type=MESH,
        )

    loads[0].wait()
    size = heads_ref.shape[2]
    total = own_ref[...].astype(jnp.float32)
    for t in range(tp_count):
        total += jnp.dot(
            heads_ref[t],
            out_proj_ref[t * size : (t + 1) * size, :],
            preferred_element_type=jnp.float32,
        )
    hidden = total.astype(jnp.bfloat16).astype(jnp.float32)
    hidden_ref[...] = hidden
    normed_ref[tp] = final_norm(hidden, ffn_gain_ref[...]).astype(jnp.bfloat16)
    pl.semaphore_wait(barrier, len(others))

    def y_copy(r, source):
        return remote(
            normed_ref.at[source % tp_count],
            normed_ref.at[source % tp_count],
            y_send.at[r - 1],
            y_recv.at[r - 1],
            at_tp(tp + r),
        )

    for r in (2, 1, 3):
        y_copy(r, tp).start()
    for r in range(1, tp_count):
        y_copy(r, tp + tp_count - r).wait_recv()

    def turn(n):
        odd = n % 2
        return odd * ((n + 1) // 2) + (1 - odd) * ((Z_RING - n // 2) % Z_RING)

    def z_copy(k, z_from, z_to):
        return remote(
            leaving_ref.at[z_to % Z_RING],
            passing_ref.at[z_from % Z_RING],
            z_send.at[k],
            z_recv.at[k],
            at_z(z + k),
        )

    def bz_copy(k, z_from, z_to):
        return remote(
            made_ref.at[z_to % Z_RING],
            back_passing_ref.at[z_from % Z_RING],
            bz_send.at[k],
            bz_recv.at[k],
            at_z(z + Z_RING - k),
        )

    def i_copy(source_ref, target_ref, sends, recvs, k, z_at, r, tile, place):
        return remote(
            source_ref.at[z_at % Z_RING, tile % PLANE],
            target_ref.at[z_at % Z_RING, place % PLANE],
            sends.at[k, r - 1],
            recvs.at[k, r - 1],
            at_i(i + r),
        )

    def spread(source_ref, target_ref, sends, recvs, locals_, k, z_at):
        for r in range(1, PLANE):
            i_copy(source_ref, target_ref, sends, recvs, k, z_at, r, i + r, i).start()
        pltpu.make_async_copy(
            source_ref.at[z_at % Z_RING, i], target_ref.at[z_at % Z_RING, i], locals_.at[k]
        ).start()

    def collected(source_ref, target_ref, sends, recvs, locals_, k, z_at):
        for r in range(1, PLANE):
            place = i + PLANE - r
            i_copy(source_ref, target_ref, sends, recvs, k, z_at, r, i, place).wait_recv()
        pltpu.make_async_copy(
            source_ref.at[z_at % Z_RING, i], target_ref.at[z_at % Z_RING, i], locals_.at[k]
        ).wait()

    def sent(source_ref, target_ref, sends, recvs, k, z_at):
        for r in range(1, PLANE):
            i_copy(source_ref, target_ref, sends, recvs, k, z_at, r, i + r, i).wait_send()

    def dispatch(n, carry):
        k = turn(n)
        z_to = (z + k) % Z_RING
        row = lax.broadcasted_iota(jnp.int32, (rows, tokens), 0)
        base = (z_to * PLANE + row // 8) * 16
        main_code = base + row % 8
        extra_code = base + 8 + (row % 8) // 4
        main = jnp.zeros((rows, tokens), jnp.float32)
        extra = jnp.zeros((rows, tokens), jnp.float32)
        for slot in range(top):
            own = code_t_ref[slot : slot + 1, :]
            main += jnp.where(main_code == own, 1.0, 0.0)
            extra += jnp.where(extra_code == own, 1.0, 0.0)
        main = main.astype(jnp.bfloat16)
        normed = normed_ref[...].reshape(tokens, width)
        tail = jnp.zeros((rows, quarter), jnp.float32)
        for q in range(4):
            cols = slice(q * quarter, (q + 1) * quarter)
            leaving_ref[z_to, :, :, cols] = (
                jnp.dot(main, normed[:, cols], preferred_element_type=jnp.float32)
                .astype(jnp.bfloat16)
                .reshape(PLANE, 8, quarter)
            )
            chosen = jnp.where(row % 4 == q, extra, 0.0).astype(jnp.bfloat16)
            tail += jnp.dot(chosen, normed[:, cols], preferred_element_type=jnp.float32)
        leaving_ref[z_to, :, :, width:] = tail.astype(jnp.bfloat16).reshape(PLANE, 8, quarter)

        @pl.when(n == 0)
        def _():
            spread(leaving_ref, arrived_ref, i_send, i_recv, i_local, 0, z)

        @pl.when(n > 0)
        def _():
            z_copy(k, z, z + k).start()

        return carry

    lax.fori_loop(0, Z_RING, dispatch, 0)

    normed = normed_ref[...].reshape(tokens, width)
    gate = jnp.dot(normed, shared_gate_ref[...], preferred_element_type=jnp.float32)
    up = jnp.dot(normed, shared_up_ref[...], preferred_element_type=jnp.float32)
    inner = (gate / (1.0 + jnp.exp(-gate)) * up).astype(jnp.bfloat16)
    acc_ref[...] = jnp.dot(inner, shared_down_ref[...], preferred_element_type=jnp.float32)
    for load in loads[1:]:
        load.wait()

    def expert(k):
        z_from = (z + Z_RING - k) % Z_RING
        tiles = arrived_ref[z_from].reshape(rows, width + quarter)
        extra_rows = rows // 4
        place = lax.broadcasted_iota(jnp.int32, (extra_rows, rows), 1)
        index = lax.broadcasted_iota(jnp.int32, (extra_rows, rows), 0)
        pieces = []
        for q in range(4):
            pick = jnp.where(place == 4 * index + q, 1.0, 0.0).astype(jnp.bfloat16)
            pieces.append(
                jnp.dot(pick, tiles[:, width:], preferred_element_type=jnp.float32).astype(
                    jnp.bfloat16
                )
            )
        every = jnp.concatenate([tiles[:, :width], jnp.concatenate(pieces, axis=1)], axis=0)
        gate = jnp.dot(every, gate_ref[...], preferred_element_type=jnp.float32)
        up = jnp.dot(every, up_ref[...], preferred_element_type=jnp.float32)
        inner = (gate / (1.0 + jnp.exp(-gate)) * up).astype(jnp.bfloat16)
        place = lax.broadcasted_iota(jnp.int32, (rows, extra_rows), 0)
        index = lax.broadcasted_iota(jnp.int32, (rows, extra_rows), 1)
        tail = jnp.zeros((rows, quarter), jnp.float32)
        for q in range(4):
            cols = slice(q * quarter, (q + 1) * quarter)
            made = jnp.dot(inner, down_ref[:, cols], preferred_element_type=jnp.float32).astype(
                jnp.bfloat16
            )
            made_ref[z_from, :, :, cols] = made[:rows].reshape(PLANE, 8, quarter)
            pick = jnp.where(place == 4 * index + q, 1.0, 0.0).astype(jnp.bfloat16)
            tail += jnp.dot(pick, made[rows:], preferred_element_type=jnp.float32)
        made_ref[z_from, :, :, width:] = tail.astype(jnp.bfloat16).reshape(PLANE, 8, quarter)

    def arrivals(n, carry):
        @pl.when((n > 0) & (n < Z_RING))
        def _():
            k = turn(n)
            z_copy(k, z + Z_RING - k, z).wait_recv()
            spread(passing_ref, arrived_ref, i_send, i_recv, i_local, k, z + Z_RING - k)

        @pl.when(n > 0)
        def _():
            k = turn(n - 1)
            collected(
                passing_ref, arrived_ref, i_send, i_recv, i_local, k, z + Z_RING - k
            )
            expert(k)

            @pl.when(n > 1)
            def _():
                bz_copy(k, z, z + Z_RING - k).start()

            @pl.when(n == 1)
            def _():
                spread(made_ref, back_ref, bi_send, bi_recv, bi_local, 0, z)

        return carry

    lax.fori_loop(0, Z_RING + 1, arrivals, 0)

    def combine(z_at):
        tiles = back_ref[z_at].reshape(rows, width + quarter)
        twice = jnp.concatenate([tiles, tiles], axis=0)
        lane = lax.broadcasted_iota(jnp.int32, (tokens, 2 * rows), 1)
        place = lane % rows
        base = (z_at * PLANE + place // 8) * 16
        main_code = base + place % 8
        extra_code = base + 8 + (place % 8) // 4
        main = jnp.zeros((tokens, 2 * rows), jnp.float32)
        extra = jnp.zeros((tokens, 2 * rows), jnp.float32)
        for slot in range(top):
            own = code_ref[:, slot : slot + 1]
            scale = weight_ref[:, slot : slot + 1]
            main += jnp.where(main_code == own, scale, 0.0)
            extra += jnp.where(extra_code == own, scale, 0.0)

        def two_terms(value):
            high = value.astype(jnp.bfloat16).astype(jnp.float32)
            return jnp.where(lane < rows, high, value - high)

        main, extra = two_terms(main), two_terms(extra)
        main = main.astype(jnp.bfloat16)
        for q in range(4):
            cols = slice(q * quarter, (q + 1) * quarter)
            chosen = jnp.where(place % 4 == q, extra, 0.0).astype(jnp.bfloat16)
            acc_ref[:, cols] += jnp.dot(
                main, twice[:, cols], preferred_element_type=jnp.float32
            ) + jnp.dot(chosen, twice[:, width:], preferred_element_type=jnp.float32)

    def returns(n, carry):
        @pl.when((n > 0) & (n < Z_RING))
        def _():
            k = turn(n)
            bz_copy(k, z + k, z).wait_recv()
            spread(back_passing_ref, back_ref, bi_send, bi_recv, bi_local, k, z + k)

        @pl.when(n > 0)
        def _():
            k = turn(n - 1)
            collected(back_passing_ref, back_ref, bi_send, bi_recv, bi_local, k, z + k)
            combine((z + k) % Z_RING)

        return carry

    lax.fori_loop(0, Z_RING + 1, returns, 0)

    def s_copy(r, source):
        return remote(
            part_ref.at[(tp + r) % tp_count],
            got_ref.at[source % tp_count],
            s_send.at[r - 1],
            s_recv.at[r - 1],
            at_tp(tp + r),
        )

    for r in (2, 1, 3, 0):
        owner = (tp + r) % tp_count
        own_rows = pl.ds(pl.multiple_of(owner * part, part), part)
        part_ref[owner] = acc_ref[own_rows, :].astype(jnp.bfloat16)
        if r:
            s_copy(r, tp).start()
        else:
            got_ref[tp] = part_ref[tp]
    for r in range(1, tp_count):
        s_copy(r, tp + tp_count - r).wait_recv()
    total = hidden_ref[...]
    for t in range(tp_count):
        total += got_ref[t].astype(jnp.float32)
    out_ref[...] = total.astype(jnp.bfloat16)

    for r in range(1, tp_count):
        y_copy(r, tp).wait_send()
        s_copy(r, tp).wait_send()

    def drain(n, carry):
        @pl.when(n > 0)
        def _():
            z_copy(n, z, z + n).wait_send()
            bz_copy(n, z, z + Z_RING - n).wait_send()

        sent(passing_ref, arrived_ref, i_send, i_recv, n, z + Z_RING - n)
        sent(back_passing_ref, back_ref, bi_send, bi_recv, n, z + n)
        return carry

    lax.fori_loop(0, Z_RING, drain, 0)


def call(kernel, out_shape, args, specs=None, scratch=(), flops=0, moved=0):
    return pl.pallas_call(
        kernel,
        out_shape=out_shape,
        in_specs=specs or [VM] * len(args),
        out_specs=jax.tree.map(lambda _: VM, out_shape),
        scratch_shapes=scratch,
        compiler_params=pltpu.CompilerParams(vmem_limit_bytes=56 * 2**20),
        cost_estimate=pl.CostEstimate(flops=flops, bytes_accessed=moved, transcendentals=0),
    )(*args)


def shaped(dims, kind=jnp.bfloat16):
    return jax.ShapeDtypeStruct(dims, kind)


def slot_codes(routes, tp_index, tp_count, sp_count):
    tokens, top = routes.shape
    flat = routes.reshape(-1)
    is_mine = flat % tp_count == tp_index
    target = flat // tp_count
    onehot = (target[:, None] == jnp.arange(sp_count, dtype=jnp.int32)[None, :]) & is_mine[:, None]
    hot = onehot.astype(jnp.bfloat16)
    entries = tokens * top
    order = jnp.arange(entries, dtype=jnp.int32)
    before = (order[:, None] > order[None, :]).astype(jnp.bfloat16)
    earlier = jnp.dot(before, hot, preferred_element_type=jnp.float32)
    rank = jnp.sum(jnp.where(onehot, earlier, 0.0), axis=1).astype(jnp.int32)
    return jnp.where(is_mine, target * 16 + rank, -1).reshape(tokens, top)


def local(
    queries,
    key_matrix,
    values,
    query_gain,
    key_norm_gain,
    head_gain,
    out_proj,
    residual,
    ffn_gain,
    routes,
    route_weights,
    expert_gate,
    expert_up,
    expert_down,
    shared_gate,
    shared_up,
    shared_down,
):
    tokens = queries.shape[0]
    heads = queries.shape[1] // HEAD_SIZE
    sp_count = lax.axis_size("sp")
    tp_count = lax.axis_size("tp")
    tp_index = lax.axis_index("tp")
    sequence_total = tokens * sp_count
    positions = lax.axis_index("sp") * tokens + jnp.arange(tokens, dtype=jnp.int32)
    cosine, sine = wide_tables(positions, sequence_total)
    columns = heads * tokens
    query_rows, packed = call(
        prepare_kernel,
        (shaped((columns, 128)), shaped((tokens, 128))),
        (
            queries,
            jnp.concatenate([key_matrix, values], axis=1),
            jnp.tile(query_gain, 2)[None],
            jnp.tile(key_norm_gain, 2)[None],
            cosine,
            sine,
        ),
    )
    codes = slot_codes(routes, tp_index, tp_count, sp_count)
    bound = 8.0 * jnp.max(jnp.abs(query_gain)) * jnp.max(jnp.abs(key_norm_gain))
    part_rows = tokens // tp_count

    def attention(guarded, number):
        def run(rows, own, gain):
            return pl.pallas_call(
                functools.partial(ring_attention_kernel, guarded),
                out_shape=shaped((tp_count, part_rows, heads * HEAD_SIZE)),
                in_specs=[VM, VM, VM],
                out_specs=VM,
                scratch_shapes=[
                    pltpu.VMEM((Z_RING, 2, X_RING * tokens, 128), jnp.bfloat16),
                    pltpu.VMEM((tokens, heads * HEAD_SIZE), jnp.bfloat16),
                    pltpu.VMEM((HEAD_SIZE, columns), jnp.float32),
                    pltpu.VMEM((8, columns), jnp.float32),
                    pltpu.VMEM((1, columns), jnp.float32),
                    pltpu.SemaphoreType.DMA((X_RING - 1,)),
                    pltpu.SemaphoreType.DMA((X_RING - 1,)),
                    pltpu.SemaphoreType.DMA((2, Z_RING // 2)),
                    pltpu.SemaphoreType.DMA((2, Z_RING // 2)),
                    pltpu.SemaphoreType.DMA((Z_RING,)),
                    pltpu.SemaphoreType.DMA((Z_RING,)),
                    pltpu.SemaphoreType.DMA((tp_count - 1,)),
                    pltpu.SemaphoreType.DMA((tp_count - 1,)),
                    pltpu.SemaphoreType.DMA,
                ],
                compiler_params=pltpu.CompilerParams(
                    vmem_limit_bytes=56 * 2**20, collective_id=number, has_side_effects=True
                ),
                cost_estimate=pl.CostEstimate(
                    flops=4 * columns * sequence_total * 128,
                    bytes_accessed=sequence_total * 256,
                    transcendentals=0,
                ),
            )(rows, own, gain)

        return run

    tiles = lax.cond(
        bound > SAFE_BOUND,
        attention(True, 1),
        attention(False, 0),
        query_rows,
        packed,
        head_gain[None],
    )
    width = residual.shape[1]
    hidden_units = expert_gate.shape[2]
    wide_row = width + width // 4
    tile_set = pltpu.VMEM((Z_RING, PLANE, 8, wide_row), jnp.bfloat16)
    dma = pltpu.SemaphoreType.DMA
    return pl.pallas_call(
        moe_kernel,
        out_shape=shaped((part_rows, width)),
        in_specs=[VM, VM, ANY] + [VM] * 7 + [ANY] * 3,
        out_specs=VM,
        scratch_shapes=[
            pltpu.VMEM((part_rows, width), jnp.bfloat16),
            pltpu.VMEM((part_rows, width), jnp.float32),
            pltpu.VMEM((tp_count, part_rows, width), jnp.bfloat16),
            tile_set,
            tile_set,
            tile_set,
            tile_set,
            tile_set,
            tile_set,
            pltpu.VMEM((tokens, width), jnp.float32),
            pltpu.VMEM((tp_count, part_rows, width), jnp.bfloat16),
            pltpu.VMEM((tp_count, part_rows, width), jnp.bfloat16),
            pltpu.VMEM((width, hidden_units), jnp.bfloat16),
            pltpu.VMEM((width, hidden_units), jnp.bfloat16),
            pltpu.VMEM((hidden_units, width), jnp.bfloat16),
            dma((3,)),
            dma,
            dma((tp_count - 1,)),
            dma((tp_count - 1,)),
            dma((tp_count - 1,)),
            dma((tp_count - 1,)),
            dma((Z_RING,)),
            dma((Z_RING,)),
            dma((Z_RING, PLANE - 1)),
            dma((Z_RING, PLANE - 1)),
            dma((Z_RING,)),
            dma((Z_RING,)),
            dma((Z_RING,)),
            dma((Z_RING, PLANE - 1)),
            dma((Z_RING, PLANE - 1)),
            dma((Z_RING,)),
        ],
        compiler_params=pltpu.CompilerParams(
            vmem_limit_bytes=58 * 2**20, collective_id=2, has_side_effects=True
        ),
    )(
        tiles,
        out_proj,
        residual,
        ffn_gain[None],
        codes,
        codes.T,
        route_weights,
        shared_gate,
        shared_up,
        shared_down,
        expert_gate[0],
        expert_up[0],
        expert_down[0],
    )


def solution(mesh):
    placed = (
        P("sp", "tp"),
        P("sp", "tp"),
        P("sp", "tp"),
        P(),
        P(),
        P("tp"),
        P(),
        P("sp", None),
        P(),
        P("sp", None),
        P("sp", None),
        P(("sp", "tp"), None, None),
        P(("sp", "tp"), None, None),
        P(("sp", "tp"), None, None),
        P(None, "tp"),
        P(None, "tp"),
        P("tp", None),
    )
    return jax.shard_map(
        local, mesh=mesh, in_specs=placed, out_specs=P(("sp", "tp"), None), check_vma=False
    )
```

```python
import functools

import jax
import jax.numpy as jnp
from jax import lax
from jax.experimental import pallas as pl
from jax.experimental.pallas import tpu as pltpu
from jax.sharding import PartitionSpec as P

HEAD_SIZE = 64
GRID_W = 64
EPS = 1e-06
THETA = 10000.0
LOG2E = 1.4426950408889634
SAFE_BOUND = 70.0

VM = pl.BlockSpec(memory_space=pltpu.VMEM)
ANY = pl.BlockSpec(memory_space=pl.ANY)


def final_norm(field, gain):
    mean_sq = jnp.mean(field * field, axis=-1, keepdims=True)
    return field * lax.rsqrt(mean_sq + EPS) * gain


def wide_tables(positions, sequence_total):
    grid_rows = sequence_total // GRID_W
    row_pos = (positions // GRID_W - grid_rows // 2).astype(jnp.float32)
    col_pos = (positions % GRID_W - GRID_W // 2).astype(jnp.float32)
    quarter = HEAD_SIZE // 4
    inverse = THETA ** (-jnp.arange(quarter, dtype=jnp.float32) / quarter)
    lane = jnp.arange(2 * HEAD_SIZE, dtype=jnp.int32)
    inverse_wide = jnp.tile(inverse, 8)
    is_row = (lane % HEAD_SIZE) < HEAD_SIZE // 2
    angles = jnp.where(is_row[None, :], row_pos[:, None], col_pos[:, None]) * inverse_wide
    sign = jnp.where((lane % 32) < 16, -1.0, 1.0)
    return jnp.cos(angles), jnp.sin(angles) * sign[None, :]


def normed_and_turned(field, gain, cosine, sine):
    lane = lax.broadcasted_iota(jnp.int32, field.shape, 1)
    low = lane < HEAD_SIZE
    square = field * field
    mean_low = jnp.sum(jnp.where(low, square, 0.0), axis=1, keepdims=True) / HEAD_SIZE
    mean_high = jnp.sum(jnp.where(low, 0.0, square), axis=1, keepdims=True) / HEAD_SIZE
    scale = jnp.where(low, lax.rsqrt(mean_low + EPS), lax.rsqrt(mean_high + EPS))
    unit = field * scale * gain
    partner = jnp.where(
        lane % 32 < 16, pltpu.roll(unit, 128 - 16, 1), pltpu.roll(unit, 16, 1)
    )
    return unit * cosine + partner * sine


def prepare_kernel(
    q_ref, key_ref, value_ref, qg_ref, kg_ref, cos_ref, sin_ref, rows_ref, packed_ref, bound_ref
):
    tokens = q_ref.shape[0]
    cosine, sine = cos_ref[...], sin_ref[...]
    low = lax.broadcasted_iota(jnp.int32, (tokens, 128), 1) < HEAD_SIZE
    query_gain = jnp.concatenate([qg_ref[...], qg_ref[...]], axis=1)
    key_gain = jnp.concatenate([kg_ref[...], kg_ref[...]], axis=1)
    top = jnp.max(jnp.abs(query_gain), axis=1, keepdims=True)
    top = top * jnp.max(jnp.abs(key_gain), axis=1, keepdims=True) * (HEAD_SIZE**0.5)
    bound_ref[...] = jnp.broadcast_to(top, bound_ref.shape)
    both = jnp.concatenate(
        [key_ref[...].astype(jnp.float32), value_ref[...].astype(jnp.float32)], axis=0
    ).T
    turned = normed_and_turned(both, key_gain, cosine, sine)
    packed_ref[...] = jnp.where(low, turned, both).astype(jnp.bfloat16)
    for pair in range(q_ref.shape[1] // 128):
        field = q_ref[:, pair * 128 : (pair + 1) * 128].astype(jnp.float32)
        turned = normed_and_turned(field, query_gain, cosine, sine).astype(jnp.bfloat16)
        turned = turned.astype(jnp.float32) * (HEAD_SIZE**-0.5)
        first = jnp.where(low, turned, 0.0)
        second = jnp.where(low, pltpu.roll(turned, HEAD_SIZE, 1), 0.0)
        rows_ref[(2 * pair) * tokens : (2 * pair + 1) * tokens, :] = first.astype(jnp.bfloat16)
        rows_ref[(2 * pair + 1) * tokens : (2 * pair + 2) * tokens, :] = second.astype(jnp.bfloat16)


MESH = pl.DeviceIdType.MESH
Z_RING, X_RING = 8, 4
PLANE = 2 * X_RING


def ring_attention_kernel(
    guarded,
    q_ref,
    packed_ref,
    gain_ref,
    out_ref,
    kv_ref,
    mine_ref,
    acc_ref,
    sum_ref,
    max_ref,
    x_send,
    x_recv,
    z_send,
    z_recv,
    v_send,
    v_recv,
    u_send,
    u_recv,
    p_send,
    p_recv,
    t_send,
    t_recv,
    l_sem,
):
    tokens = packed_ref.shape[0]
    columns = q_ref.shape[0]
    group = X_RING * tokens
    sp, tp = lax.axis_index("sp"), lax.axis_index("tp")
    tp_count = lax.axis_size("tp")
    core = sp % 2
    x = (sp // 2) % X_RING
    z = sp // (2 * X_RING)

    def device(z_at, x_at, core_at):
        return {"sp": ((z_at % Z_RING) * X_RING + x_at % X_RING) * 2 + core_at}

    barrier = pltpu.get_barrier_semaphore()
    others = [device(z, x + r, core) for r in range(1, X_RING)]
    others += [device(z + k, x, core) for k in range(1, Z_RING)] + [device(z, x, 1 - core)]
    others += [{"tp": (tp + r) % tp_count} for r in range(1, tp_count)]
    for other in others:
        pl.semaphore_signal(barrier, inc=1, device_id=other, device_id_type=MESH)
    pl.semaphore_wait(barrier, len(others))

    def slot(x_at, z_at=z):
        rows = pl.ds(pl.multiple_of((x_at % X_RING) * tokens, tokens), tokens)
        return kv_ref.at[z_at % Z_RING, core, rows]

    def remote(src, dst, send_sem, recv_sem, to):
        return pltpu.make_async_remote_copy(
            src_ref=src,
            dst_ref=dst,
            send_sem=send_sem,
            recv_sem=recv_sem,
            device_id=to,
            device_id_type=MESH,
        )

    def x_copy(r, source_x):
        place = slot(source_x)
        return remote(
            packed_ref, place, x_send.at[r - 1], x_recv.at[r - 1], device(z, x + r, core)
        )

    def z_copy(way, hop, z_from):
        rows = pl.ds(0, group)
        if hop == Z_RING // 2 - 1:
            rows = pl.ds(way * (group // 2), group // 2)
        place = kv_ref.at[z_from % Z_RING, core, rows]
        to = device(z + (1 if way == 0 else Z_RING - 1), x, core)
        return remote(place, place, z_send.at[way, hop], z_recv.at[way, hop], to)

    def z_out(way, hop):
        return z_copy(way, hop, z + (Z_RING - hop if way == 0 else hop))

    def z_in(way, hop):
        return z_copy(way, hop, z + (Z_RING - 1 - hop if way == 0 else 1 + hop))

    def v_copy(k, z_from):
        return remote(
            packed_ref, slot(x, z_from), v_send.at[k - 1], v_recv.at[k - 1], device(z + k, x, core)
        )

    def u_copy(k, r, x_from):
        place = slot(x_from, z + Z_RING - k)
        return remote(
            place, place, u_send.at[k - 1, r - 1], u_recv.at[k - 1, r - 1], device(z, x + r, core)
        )

    def relay(distance):
        for k in (distance, Z_RING - distance)[: 1 if 2 * distance == Z_RING else 2]:
            v_copy(k, z + Z_RING - k).wait_recv()
            for r in range(1, X_RING):
                u_copy(k, r, x).start()

    def relayed(distance):
        for k in (distance, Z_RING - distance)[: 1 if 2 * distance == Z_RING else 2]:
            for r in range(1, X_RING):
                u_copy(k, r, x + X_RING - r).wait_recv()

    def p_copy(number, z_at, core_at):
        place = kv_ref.at[z_at % Z_RING, core_at]
        return remote(
            place, place, p_send.at[number], p_recv.at[number], device(z, x, 1 - core)
        )

    def p_out(number):
        distance = (number + 1) // 2
        return p_copy(number, z + (Z_RING - distance if number % 2 else distance), core)

    own = pltpu.make_async_copy(packed_ref, slot(x), l_sem)
    own.start()
    for r in range(1, X_RING):
        x_copy(r, x).start()

    @pl.when(core == 1)
    def _():
        for k in (1, 7, 2, 6, 3, 5, 4):
            v_copy(k, z).start()

    acc_ref[...] = jnp.zeros_like(acc_ref)
    sum_ref[...] = jnp.zeros_like(sum_ref)
    if guarded:
        max_ref[...] = jnp.full_like(max_ref, -1e30)
    own.wait()
    for r in range(1, X_RING):
        x_copy(r, x + X_RING - r).wait_recv()
    p_out(0).start()

    @pl.when(core == 0)
    def _():
        z_out(0, 0).start()
        z_out(1, 0).start()

    @pl.when(core == 1)
    def _():
        relay(1)

    def step(j, carry):
        i = j + 2
        distance, member = i // 4, i % 4
        z_at = (z + Z_RING + distance * (2 * (member // 2) - 1)) % Z_RING
        core_at = (core + member % 2) % 2

        for hop in range(Z_RING // 2):

            @pl.when((j == 4 * hop + 2) & (core == 0))
            def _(hop=hop):
                z_in(0, hop).wait_recv()
                z_in(1, hop).wait_recv()
                if hop < Z_RING // 2 - 1:
                    z_out(0, hop + 1).start()
                    z_out(1, hop + 1).start()

            @pl.when((j == 4 * hop + 2) & (core == 1))
            def _(hop=hop):
                if hop < Z_RING // 2 - 1:
                    relay(hop + 2)
                relayed(hop + 1)

            @pl.when(j == 4 * hop + 2)
            def _(hop=hop):
                p_out(2 * hop + 1).start()
                if hop < Z_RING // 2 - 1:
                    p_out(2 * hop + 2).start()

        @pl.when(member % 2 == 1)
        def _():
            p_copy(j // 2, z_at, 1 - core).wait_recv()

        slab = kv_ref[z_at, core_at]
        scores = lax.dot_general(
            slab, q_ref[...], (((1,), (1,)), ((), ())), preferred_element_type=jnp.float32
        )
        if guarded:
            before = max_ref[...]
            top = jnp.maximum(before, jnp.max(scores, axis=0, keepdims=True))
            factor = jnp.exp(before - top)
            weights = jnp.exp(scores - top)
            max_ref[...] = top
        else:
            factor = None
            weights = jnp.exp2(scores * LOG2E)
        added = jnp.sum(weights.reshape(group // 8, 8, columns), axis=0)
        mixed = lax.dot_general(
            slab,
            weights.astype(jnp.bfloat16),
            (((0,), (0,)), ((), ())),
            preferred_element_type=jnp.float32,
        )[HEAD_SIZE:]
        if guarded:
            sum_ref[...] = sum_ref[...] * factor + added
            acc_ref[...] = acc_ref[...] * factor + mixed
        else:
            sum_ref[...] += added
            acc_ref[...] += mixed
        return carry

    lax.fori_loop(0, 2 * Z_RING, step, 0)

    attended = acc_ref[...] / jnp.sum(sum_ref[...], axis=0, keepdims=True)
    mean_sq = jnp.mean(attended * attended, axis=0, keepdims=True)
    unit = attended * lax.rsqrt(mean_sq + EPS)
    turned = jnp.concatenate([unit, jnp.zeros_like(unit)], axis=0).T
    low = lax.broadcasted_iota(jnp.int32, (tokens, 128), 1) < HEAD_SIZE
    for pair in range(mine_ref.shape[1] // 128):
        first = turned[(2 * pair) * tokens : (2 * pair + 1) * tokens, :]
        second = turned[(2 * pair + 1) * tokens : (2 * pair + 2) * tokens, :]
        joined = jnp.where(low, first, pltpu.roll(second, HEAD_SIZE, 1))
        lanes = slice(pair * 128, (pair + 1) * 128)
        mine_ref[:, lanes] = (joined * gain_ref[:, lanes]).astype(jnp.bfloat16)

    part = tokens // tp_count

    def rows_of(owner):
        return mine_ref.at[pl.ds(pl.multiple_of((owner % tp_count) * part, part), part)]

    def t_copy(r, source):
        return remote(
            rows_of(tp + r),
            out_ref.at[source % tp_count],
            t_send.at[r - 1],
            t_recv.at[r - 1],
            {"tp": (tp + r) % tp_count},
        )

    for r in range(1, tp_count):
        t_copy(r, tp).start()
    own = pltpu.make_async_copy(rows_of(tp), out_ref.at[tp], l_sem)
    own.start()
    own.wait()
    for r in range(1, X_RING):
        x_copy(r, x).wait_send()

    @pl.when(core == 0)
    def _():
        for way in range(2):
            for hop in range(Z_RING // 2):
                z_out(way, hop).wait_send()

    @pl.when(core == 1)
    def _():
        for k in range(1, Z_RING):
            v_copy(k, z).wait_send()
            for r in range(1, X_RING):
                u_copy(k, r, x).wait_send()

    for number in range(Z_RING):
        p_out(number).wait_send()
    for r in range(1, tp_count):
        t_copy(r, tp + tp_count - r).wait_recv()
        t_copy(r, tp).wait_send()


def moe_kernel(
    heads_ref,
    out_proj_ref,
    residual_ref,
    ffn_gain_ref,
    routes_ref,
    weights_ref,
    shared_gate_ref,
    shared_up_ref,
    shared_down_ref,
    gate_hbm,
    up_hbm,
    down_hbm,
    out_ref,
    own_ref,
    hidden_ref,
    rank_ref,
    scale_ref,
    normed_ref,
    leaving_ref,
    passing_ref,
    arrived_ref,
    made_ref,
    back_passing_ref,
    back_ref,
    acc_ref,
    part_ref,
    got_ref,
    gate_ref,
    up_ref,
    down_ref,
    w_sem,
    l_sem,
    y_send,
    y_recv,
    s_send,
    s_recv,
    z_send,
    z_recv,
    i_send,
    i_recv,
    i_local,
    bz_send,
    bz_recv,
    bi_send,
    bi_recv,
    bi_local,
):
    sp, tp = lax.axis_index("sp"), lax.axis_index("tp")
    tp_count = lax.axis_size("tp")
    z, i = sp // PLANE, sp % PLANE
    part, width = hidden_ref.shape
    tokens = part * tp_count
    quarter = width // 4
    rows = PLANE * 8
    top = routes_ref.shape[0]
    experts = Z_RING * PLANE

    def at_z(z_at):
        return {"sp": (z_at % Z_RING) * PLANE + i}

    def at_i(i_at):
        return {"sp": z * PLANE + i_at % PLANE}

    def at_tp(t):
        return {"tp": t % tp_count}

    barrier = pltpu.get_barrier_semaphore()
    others = [at_z(z + k) for k in range(1, Z_RING)]
    others += [at_i(i + r) for r in range(1, PLANE)]
    others += [at_tp(tp + r) for r in range(1, tp_count)]
    for other in others:
        pl.semaphore_signal(barrier, inc=1, device_id=other, device_id_type=MESH)

    loads = [
        pltpu.make_async_copy(
            residual_ref.at[pl.ds(pl.multiple_of(tp * part, part), part)], own_ref, l_sem
        ),
        pltpu.make_async_copy(gate_hbm, gate_ref, w_sem.at[0]),
        pltpu.make_async_copy(up_hbm, up_ref, w_sem.at[1]),
        pltpu.make_async_copy(down_hbm, down_ref, w_sem.at[2]),
    ]
    for load in loads:
        load.start()

    def remote(src, dst, send_sem, recv_sem, to):
        return pltpu.make_async_remote_copy(
            src_ref=src,
            dst_ref=dst,
            send_sem=send_sem,
            recv_sem=recv_sem,
            device_id=to,
            device_id_type=MESH,
        )

    named = lax.broadcasted_iota(jnp.int32, (experts, tokens), 0) * tp_count + tp
    hot = jnp.zeros((experts, tokens), jnp.float32)
    scale = jnp.zeros((experts, tokens), jnp.float32)
    for choice in range(top):
        same = named == routes_ref[choice : choice + 1, :]
        hot += jnp.where(same, 1.0, 0.0)
        scale += jnp.where(same, weights_ref[choice : choice + 1, :], 0.0)
    earlier = lax.broadcasted_iota(jnp.int32, (tokens, tokens), 0)
    later = lax.broadcasted_iota(jnp.int32, (tokens, tokens), 1)
    before = jnp.where(earlier < later, 1.0, 0.0).astype(jnp.bfloat16)
    rank = jnp.dot(hot.astype(jnp.bfloat16), before, preferred_element_type=jnp.float32)
    rank_ref[...] = jnp.where(hot > 0.0, rank, -1.0).reshape(Z_RING, PLANE, tokens)
    scale_ref[...] = scale.reshape(Z_RING, PLANE, tokens)

    def rows_of_eight(ref, z_at):
        value = ref[z_at][:, None, :]
        return jnp.broadcast_to(value, (PLANE, 8, tokens)).reshape(rows, tokens)

    loads[0].wait()
    size = heads_ref.shape[2]
    total = own_ref[...].astype(jnp.float32)
    for t in range(tp_count):
        total += jnp.dot(
            heads_ref[t],
            out_proj_ref[t * size : (t + 1) * size, :],
            preferred_element_type=jnp.float32,
        )
    hidden = total.astype(jnp.bfloat16).astype(jnp.float32)
    hidden_ref[...] = hidden
    normed_ref[tp] = final_norm(hidden, ffn_gain_ref[...]).astype(jnp.bfloat16)
    pl.semaphore_wait(barrier, len(others))

    def y_copy(r, source):
        return remote(
            normed_ref.at[source % tp_count],
            normed_ref.at[source % tp_count],
            y_send.at[r - 1],
            y_recv.at[r - 1],
            at_tp(tp + r),
        )

    for r in (2, 1, 3):
        y_copy(r, tp).start()
    for r in range(1, tp_count):
        y_copy(r, tp + tp_count - r).wait_recv()

    def turn(n):
        odd = n % 2
        return odd * ((n + 1) // 2) + (1 - odd) * ((Z_RING - n // 2) % Z_RING)

    def z_copy(k, z_from, z_to):
        return remote(
            leaving_ref.at[z_to % Z_RING],
            passing_ref.at[z_from % Z_RING],
            z_send.at[k],
            z_recv.at[k],
            at_z(z + k),
        )

    def bz_copy(k, z_from, z_to):
        return remote(
            made_ref.at[z_to % Z_RING],
            back_passing_ref.at[z_from % Z_RING],
            bz_send.at[k],
            bz_recv.at[k],
            at_z(z + Z_RING - k),
        )

    def i_copy(source_ref, target_ref, sends, recvs, k, z_at, r, tile, place):
        return remote(
            source_ref.at[z_at % Z_RING, tile % PLANE],
            target_ref.at[z_at % Z_RING, place % PLANE],
            sends.at[k, r - 1],
            recvs.at[k, r - 1],
            at_i(i + r),
        )

    def spread(source_ref, target_ref, sends, recvs, locals_, k, z_at):
        for r in range(1, PLANE):
            i_copy(source_ref, target_ref, sends, recvs, k, z_at, r, i + r, i).start()
        pltpu.make_async_copy(
            source_ref.at[z_at % Z_RING, i], target_ref.at[z_at % Z_RING, i], locals_.at[k]
        ).start()

    def collected(source_ref, target_ref, sends, recvs, locals_, k, z_at):
        for r in range(1, PLANE):
            place = i + PLANE - r
            i_copy(source_ref, target_ref, sends, recvs, k, z_at, r, i, place).wait_recv()
        pltpu.make_async_copy(
            source_ref.at[z_at % Z_RING, i], target_ref.at[z_at % Z_RING, i], locals_.at[k]
        ).wait()

    def sent(source_ref, target_ref, sends, recvs, k, z_at):
        for r in range(1, PLANE):
            i_copy(source_ref, target_ref, sends, recvs, k, z_at, r, i + r, i).wait_send()

    def dispatch(n, carry):
        k = turn(n)
        z_to = (z + k) % Z_RING
        row = lax.broadcasted_iota(jnp.int32, (rows, tokens), 0)
        rank = rows_of_eight(rank_ref, z_to)
        place = (row % 8).astype(jnp.float32)
        main = jnp.where(rank == place, 1.0, 0.0).astype(jnp.bfloat16)
        extra = jnp.where(rank == 8.0 + (row % 8 // 4).astype(jnp.float32), 1.0, 0.0)
        normed = normed_ref[...].reshape(tokens, width)
        tail = jnp.zeros((rows, quarter), jnp.float32)
        for q in range(4):
            cols = slice(q * quarter, (q + 1) * quarter)
            leaving_ref[z_to, :, :, cols] = (
                jnp.dot(main, normed[:, cols], preferred_element_type=jnp.float32)
                .astype(jnp.bfloat16)
                .reshape(PLANE, 8, quarter)
            )
            chosen = jnp.where(row % 4 == q, extra, 0.0).astype(jnp.bfloat16)
            tail += jnp.dot(chosen, normed[:, cols], preferred_element_type=jnp.float32)
        leaving_ref[z_to, :, :, width:] = tail.astype(jnp.bfloat16).reshape(PLANE, 8, quarter)

        @pl.when(n == 0)
        def _():
            spread(leaving_ref, arrived_ref, i_send, i_recv, i_local, 0, z)

        @pl.when(n > 0)
        def _():
            z_copy(k, z, z + k).start()

        return carry

    lax.fori_loop(0, Z_RING, dispatch, 0)

    normed = normed_ref[...].reshape(tokens, width)
    gate = jnp.dot(normed, shared_gate_ref[...], preferred_element_type=jnp.float32)
    up = jnp.dot(normed, shared_up_ref[...], preferred_element_type=jnp.float32)
    inner = (gate / (1.0 + jnp.exp(-gate)) * up).astype(jnp.bfloat16)
    acc_ref[...] = jnp.dot(inner, shared_down_ref[...], preferred_element_type=jnp.float32)
    for load in loads[1:]:
        load.wait()

    def expert(k):
        z_from = (z + Z_RING - k) % Z_RING
        tiles = arrived_ref[z_from].reshape(rows, width + quarter)
        extra_rows = rows // 4
        place = lax.broadcasted_iota(jnp.int32, (extra_rows, rows), 1)
        index = lax.broadcasted_iota(jnp.int32, (extra_rows, rows), 0)
        pieces = []
        for q in range(4):
            pick = jnp.where(place == 4 * index + q, 1.0, 0.0).astype(jnp.bfloat16)
            pieces.append(
                jnp.dot(pick, tiles[:, width:], preferred_element_type=jnp.float32).astype(
                    jnp.bfloat16
                )
            )
        every = jnp.concatenate([tiles[:, :width], jnp.concatenate(pieces, axis=1)], axis=0)
        gate = jnp.dot(every, gate_ref[...], preferred_element_type=jnp.float32)
        up = jnp.dot(every, up_ref[...], preferred_element_type=jnp.float32)
        inner = (gate / (1.0 + jnp.exp(-gate)) * up).astype(jnp.bfloat16)
        place = lax.broadcasted_iota(jnp.int32, (rows, extra_rows), 0)
        index = lax.broadcasted_iota(jnp.int32, (rows, extra_rows), 1)
        tail = jnp.zeros((rows, quarter), jnp.float32)
        for q in range(4):
            cols = slice(q * quarter, (q + 1) * quarter)
            made = jnp.dot(inner, down_ref[:, cols], preferred_element_type=jnp.float32).astype(
                jnp.bfloat16
            )
            made_ref[z_from, :, :, cols] = made[:rows].reshape(PLANE, 8, quarter)
            pick = jnp.where(place == 4 * index + q, 1.0, 0.0).astype(jnp.bfloat16)
            tail += jnp.dot(pick, made[rows:], preferred_element_type=jnp.float32)
        made_ref[z_from, :, :, width:] = tail.astype(jnp.bfloat16).reshape(PLANE, 8, quarter)

    def arrivals(n, carry):
        @pl.when((n > 0) & (n < Z_RING))
        def _():
            k = turn(n)
            z_copy(k, z + Z_RING - k, z).wait_recv()
            spread(passing_ref, arrived_ref, i_send, i_recv, i_local, k, z + Z_RING - k)

        @pl.when(n > 0)
        def _():
            k = turn(n - 1)
            collected(
                passing_ref, arrived_ref, i_send, i_recv, i_local, k, z + Z_RING - k
            )
            expert(k)

            @pl.when(n > 1)
            def _():
                bz_copy(k, z, z + Z_RING - k).start()

            @pl.when(n == 1)
            def _():
                spread(made_ref, back_ref, bi_send, bi_recv, bi_local, 0, z)

        return carry

    lax.fori_loop(0, Z_RING + 1, arrivals, 0)

    def combine(z_at):
        tiles = back_ref[z_at].reshape(rows, width + quarter)
        twice = jnp.concatenate([tiles, tiles], axis=0)
        row = lax.broadcasted_iota(jnp.int32, (rows, tokens), 0)
        rank = rows_of_eight(rank_ref, z_at)
        scale = rows_of_eight(scale_ref, z_at)
        place = (row % 8).astype(jnp.float32)
        main = jnp.where(rank == place, scale, 0.0)
        extra = jnp.where(rank == 8.0 + (row % 8 // 4).astype(jnp.float32), scale, 0.0)

        def two_terms(value):
            high = value.astype(jnp.bfloat16)
            low = (value - high.astype(jnp.float32)).astype(jnp.bfloat16)
            return jnp.concatenate([high, low], axis=0)

        def product(terms, tiles):
            return lax.dot_general(
                terms, tiles, (((0,), (0,)), ((), ())), preferred_element_type=jnp.float32
            )

        main = two_terms(main)
        for q in range(4):
            cols = slice(q * quarter, (q + 1) * quarter)
            chosen = two_terms(jnp.where(row % 4 == q, extra, 0.0))
            acc_ref[:, cols] += product(main, twice[:, cols]) + product(chosen, twice[:, width:])

    def returns(n, carry):
        @pl.when((n > 0) & (n < Z_RING))
        def _():
            k = turn(n)
            bz_copy(k, z + k, z).wait_recv()
            spread(back_passing_ref, back_ref, bi_send, bi_recv, bi_local, k, z + k)

        @pl.when(n > 0)
        def _():
            k = turn(n - 1)
            collected(back_passing_ref, back_ref, bi_send, bi_recv, bi_local, k, z + k)
            combine((z + k) % Z_RING)

        return carry

    lax.fori_loop(0, Z_RING + 1, returns, 0)

    def s_copy(r, source):
        return remote(
            part_ref.at[(tp + r) % tp_count],
            got_ref.at[source % tp_count],
            s_send.at[r - 1],
            s_recv.at[r - 1],
            at_tp(tp + r),
        )

    for r in (2, 1, 3, 0):
        owner = (tp + r) % tp_count
        own_rows = pl.ds(pl.multiple_of(owner * part, part), part)
        part_ref[owner] = acc_ref[own_rows, :].astype(jnp.bfloat16)
        if r:
            s_copy(r, tp).start()
        else:
            got_ref[tp] = part_ref[tp]
    for r in range(1, tp_count):
        s_copy(r, tp + tp_count - r).wait_recv()
    total = hidden_ref[...]
    for t in range(tp_count):
        total += got_ref[t].astype(jnp.float32)
    out_ref[...] = total.astype(jnp.bfloat16)

    for r in range(1, tp_count):
        y_copy(r, tp).wait_send()
        s_copy(r, tp).wait_send()

    def drain(n, carry):
        @pl.when(n > 0)
        def _():
            z_copy(n, z, z + n).wait_send()
            bz_copy(n, z, z + Z_RING - n).wait_send()

        sent(passing_ref, arrived_ref, i_send, i_recv, n, z + Z_RING - n)
        sent(back_passing_ref, back_ref, bi_send, bi_recv, n, z + n)
        return carry

    lax.fori_loop(0, Z_RING, drain, 0)


def call(kernel, out_shape, args, specs=None, scratch=(), flops=0, moved=0):
    return pl.pallas_call(
        kernel,
        out_shape=out_shape,
        in_specs=specs or [VM] * len(args),
        out_specs=jax.tree.map(lambda _: VM, out_shape),
        scratch_shapes=scratch,
        compiler_params=pltpu.CompilerParams(vmem_limit_bytes=56 * 2**20),
        cost_estimate=pl.CostEstimate(flops=flops, bytes_accessed=moved, transcendentals=0),
    )(*args)


def shaped(dims, kind=jnp.bfloat16):
    return jax.ShapeDtypeStruct(dims, kind)


def local(
    queries,
    key_matrix,
    values,
    query_gain,
    key_norm_gain,
    head_gain,
    out_proj,
    residual,
    ffn_gain,
    routes,
    route_weights,
    expert_gate,
    expert_up,
    expert_down,
    shared_gate,
    shared_up,
    shared_down,
):
    tokens = queries.shape[0]
    heads = queries.shape[1] // HEAD_SIZE
    sp_count = lax.axis_size("sp")
    tp_count = lax.axis_size("tp")
    sequence_total = tokens * sp_count
    positions = lax.axis_index("sp") * tokens + jnp.arange(tokens, dtype=jnp.int32)
    cosine, sine = wide_tables(positions, sequence_total)
    columns = heads * tokens
    query_rows, packed, bound = call(
        prepare_kernel,
        (shaped((columns, 128)), shaped((tokens, 128)), shaped((8, 128), jnp.float32)),
        (
            queries,
            key_matrix.T,
            values.T,
            query_gain[None],
            key_norm_gain[None],
            cosine,
            sine,
        ),
    )
    part_rows = tokens // tp_count

    def attention(guarded, number):
        def run(rows, own, gain):
            return pl.pallas_call(
                functools.partial(ring_attention_kernel, guarded),
                out_shape=shaped((tp_count, part_rows, heads * HEAD_SIZE)),
                in_specs=[VM, VM, VM],
                out_specs=VM,
                scratch_shapes=[
                    pltpu.VMEM((Z_RING, 2, X_RING * tokens, 128), jnp.bfloat16),
                    pltpu.VMEM((tokens, heads * HEAD_SIZE), jnp.bfloat16),
                    pltpu.VMEM((HEAD_SIZE, columns), jnp.float32),
                    pltpu.VMEM((8, columns), jnp.float32),
                    pltpu.VMEM((1, columns), jnp.float32),
                    pltpu.SemaphoreType.DMA((X_RING - 1,)),
                    pltpu.SemaphoreType.DMA((X_RING - 1,)),
                    pltpu.SemaphoreType.DMA((2, Z_RING // 2)),
                    pltpu.SemaphoreType.DMA((2, Z_RING // 2)),
                    pltpu.SemaphoreType.DMA((Z_RING - 1,)),
                    pltpu.SemaphoreType.DMA((Z_RING - 1,)),
                    pltpu.SemaphoreType.DMA((Z_RING - 1, X_RING - 1)),
                    pltpu.SemaphoreType.DMA((Z_RING - 1, X_RING - 1)),
                    pltpu.SemaphoreType.DMA((Z_RING,)),
                    pltpu.SemaphoreType.DMA((Z_RING,)),
                    pltpu.SemaphoreType.DMA((tp_count - 1,)),
                    pltpu.SemaphoreType.DMA((tp_count - 1,)),
                    pltpu.SemaphoreType.DMA,
                ],
                compiler_params=pltpu.CompilerParams(
                    vmem_limit_bytes=56 * 2**20, collective_id=number, has_side_effects=True
                ),
                cost_estimate=pl.CostEstimate(
                    flops=4 * columns * sequence_total * 128,
                    bytes_accessed=sequence_total * 256,
                    transcendentals=0,
                ),
            )(rows, own, gain)

        return run

    tiles = lax.cond(
        bound[0, 0] > SAFE_BOUND,
        attention(True, 1),
        attention(False, 0),
        query_rows,
        packed,
        head_gain[None],
    )
    width = residual.shape[1]
    hidden_units = expert_gate.shape[2]
    wide_row = width + width // 4
    tile_set = pltpu.VMEM((Z_RING, PLANE, 8, wide_row), jnp.bfloat16)
    dma = pltpu.SemaphoreType.DMA
    return pl.pallas_call(
        moe_kernel,
        out_shape=shaped((part_rows, width)),
        in_specs=[VM, VM, ANY] + [VM] * 6 + [ANY] * 3,
        out_specs=VM,
        scratch_shapes=[
            pltpu.VMEM((part_rows, width), jnp.bfloat16),
            pltpu.VMEM((part_rows, width), jnp.float32),
            pltpu.VMEM((Z_RING, PLANE, tokens), jnp.float32),
            pltpu.VMEM((Z_RING, PLANE, tokens), jnp.float32),
            pltpu.VMEM((tp_count, part_rows, width), jnp.bfloat16),
            tile_set,
            tile_set,
            tile_set,
            tile_set,
            tile_set,
            tile_set,
            pltpu.VMEM((tokens, width), jnp.float32),
            pltpu.VMEM((tp_count, part_rows, width), jnp.bfloat16),
            pltpu.VMEM((tp_count, part_rows, width), jnp.bfloat16),
            pltpu.VMEM((width, hidden_units), jnp.bfloat16),
            pltpu.VMEM((width, hidden_units), jnp.bfloat16),
            pltpu.VMEM((hidden_units, width), jnp.bfloat16),
            dma((3,)),
            dma,
            dma((tp_count - 1,)),
            dma((tp_count - 1,)),
            dma((tp_count - 1,)),
            dma((tp_count - 1,)),
            dma((Z_RING,)),
            dma((Z_RING,)),
            dma((Z_RING, PLANE - 1)),
            dma((Z_RING, PLANE - 1)),
            dma((Z_RING,)),
            dma((Z_RING,)),
            dma((Z_RING,)),
            dma((Z_RING, PLANE - 1)),
            dma((Z_RING, PLANE - 1)),
            dma((Z_RING,)),
        ],
        compiler_params=pltpu.CompilerParams(
            vmem_limit_bytes=58 * 2**20, collective_id=2, has_side_effects=True
        ),
    )(
        tiles,
        out_proj,
        residual,
        ffn_gain[None],
        routes.T,
        route_weights.T,
        shared_gate,
        shared_up,
        shared_down,
        expert_gate[0],
        expert_up[0],
        expert_down[0],
    )


def solution(mesh):
    placed = (
        P("sp", "tp"),
        P("sp", "tp"),
        P("sp", "tp"),
        P(),
        P(),
        P("tp"),
        P(),
        P("sp", None),
        P(),
        P("sp", None),
        P("sp", None),
        P(("sp", "tp"), None, None),
        P(("sp", "tp"), None, None),
        P(("sp", "tp"), None, None),
        P(None, "tp"),
        P(None, "tp"),
        P("tp", None),
    )
    return jax.shard_map(
        local, mesh=mesh, in_specs=placed, out_specs=P(("sp", "tp"), None), check_vma=False
    )
```

```python
import functools

import jax
import jax.numpy as jnp
from jax import lax
from jax.experimental import pallas as pl
from jax.experimental.pallas import tpu as pltpu
from jax.sharding import PartitionSpec as P

HEAD_SIZE = 64
GRID_W = 64
EPS = 1e-06
THETA = 10000.0
LOG2E = 1.4426950408889634
SAFE_BOUND = 70.0

VM = pl.BlockSpec(memory_space=pltpu.VMEM)
ANY = pl.BlockSpec(memory_space=pl.ANY)


def final_norm(field, gain):
    mean_sq = jnp.mean(field * field, axis=-1, keepdims=True)
    return field * lax.rsqrt(mean_sq + EPS) * gain


def wide_tables(first, tokens, sequence_total):
    grid_rows = sequence_total // GRID_W
    padded = -(-tokens // GRID_W // 8) * 8
    row_pos = first // GRID_W + jnp.arange(padded, dtype=jnp.int32) - grid_rows // 2
    col_pos = jnp.arange(GRID_W, dtype=jnp.int32) - GRID_W // 2
    place = jnp.concatenate([row_pos, col_pos]).astype(jnp.float32)
    quarter = HEAD_SIZE // 4
    inverse = THETA ** (-jnp.arange(quarter, dtype=jnp.float32) / quarter)
    lane = jnp.arange(2 * HEAD_SIZE, dtype=jnp.int32)
    angles = place[:, None] * jnp.tile(inverse, 8)
    sign = jnp.where((lane % 32) < 16, -1.0, 1.0)
    return jnp.cos(angles), jnp.sin(angles) * sign[None, :]


def spread_table(table, tokens):
    padded = table.shape[0] - GRID_W
    count = tokens // GRID_W
    by_row = jnp.concatenate(
        [jnp.broadcast_to(table[n : n + 1], (GRID_W, 128)) for n in range(count)], axis=0
    )
    by_col = jnp.concatenate([table[padded:]] * count, axis=0)
    lane = lax.broadcasted_iota(jnp.int32, (tokens, 128), 1)
    return jnp.where(lane % HEAD_SIZE < HEAD_SIZE // 2, by_row, by_col)


def normed_and_turned(field, gain, cosine, sine):
    lane = lax.broadcasted_iota(jnp.int32, field.shape, 1)
    low = lane < HEAD_SIZE
    square = field * field
    mean_low = jnp.sum(jnp.where(low, square, 0.0), axis=1, keepdims=True) / HEAD_SIZE
    mean_high = jnp.sum(jnp.where(low, 0.0, square), axis=1, keepdims=True) / HEAD_SIZE
    scale = jnp.where(low, lax.rsqrt(mean_low + EPS), lax.rsqrt(mean_high + EPS))
    unit = field * scale * gain
    partner = jnp.where(
        lane % 32 < 16, pltpu.roll(unit, 128 - 16, 1), pltpu.roll(unit, 16, 1)
    )
    return unit * cosine + partner * sine


def prepare_kernel(
    q_ref, key_ref, value_ref, qg_ref, kg_ref, cos_ref, sin_ref, rows_ref, packed_ref, bound_ref
):
    tokens = q_ref.shape[0]
    cosine = spread_table(cos_ref[...], tokens)
    sine = spread_table(sin_ref[...], tokens)
    low = lax.broadcasted_iota(jnp.int32, (tokens, 128), 1) < HEAD_SIZE
    query_gain = jnp.concatenate([qg_ref[...], qg_ref[...]], axis=1)
    key_gain = jnp.concatenate([kg_ref[...], kg_ref[...]], axis=1)
    top = jnp.max(jnp.abs(query_gain), axis=1, keepdims=True)
    top = top * jnp.max(jnp.abs(key_gain), axis=1, keepdims=True) * (HEAD_SIZE**0.5)
    bound_ref[...] = jnp.broadcast_to(top, bound_ref.shape)
    both = jnp.concatenate(
        [key_ref[...].astype(jnp.float32), value_ref[...].astype(jnp.float32)], axis=0
    ).T
    turned = normed_and_turned(both, key_gain, cosine, sine)
    packed_ref[...] = jnp.where(low, turned, both).astype(jnp.bfloat16)
    for pair in range(q_ref.shape[1] // 128):
        field = q_ref[:, pair * 128 : (pair + 1) * 128].astype(jnp.float32)
        turned = normed_and_turned(field, query_gain, cosine, sine).astype(jnp.bfloat16)
        turned = turned.astype(jnp.float32) * (HEAD_SIZE**-0.5)
        first = jnp.where(low, turned, 0.0)
        second = jnp.where(low, pltpu.roll(turned, HEAD_SIZE, 1), 0.0)
        rows_ref[(2 * pair) * tokens : (2 * pair + 1) * tokens, :] = first.astype(jnp.bfloat16)
        rows_ref[(2 * pair + 1) * tokens : (2 * pair + 2) * tokens, :] = second.astype(jnp.bfloat16)


MESH = pl.DeviceIdType.MESH
Z_RING, X_RING = 8, 4
PLANE = 2 * X_RING


def ring_attention_kernel(
    guarded,
    q_ref,
    packed_ref,
    gain_ref,
    out_ref,
    kv_ref,
    mine_ref,
    acc_ref,
    sum_ref,
    max_ref,
    x_send,
    x_recv,
    z_send,
    z_recv,
    v_send,
    v_recv,
    u_send,
    u_recv,
    p_send,
    p_recv,
    t_send,
    t_recv,
    l_sem,
):
    tokens = packed_ref.shape[0]
    columns = q_ref.shape[0]
    group = X_RING * tokens
    sp, tp = lax.axis_index("sp"), lax.axis_index("tp")
    tp_count = lax.axis_size("tp")
    core = sp % 2
    x = (sp // 2) % X_RING
    z = sp // (2 * X_RING)

    def device(z_at, x_at, core_at):
        return {"sp": ((z_at % Z_RING) * X_RING + x_at % X_RING) * 2 + core_at}

    barrier = pltpu.get_barrier_semaphore()
    others = [device(z, x + r, core) for r in range(1, X_RING)]
    others += [device(z + k, x, core) for k in range(1, Z_RING)] + [device(z, x, 1 - core)]
    others += [{"tp": (tp + r) % tp_count} for r in range(1, tp_count)]
    for other in others:
        pl.semaphore_signal(barrier, inc=1, device_id=other, device_id_type=MESH)
    pl.semaphore_wait(barrier, len(others))

    def slot(x_at, z_at=z):
        rows = pl.ds(pl.multiple_of((x_at % X_RING) * tokens, tokens), tokens)
        return kv_ref.at[z_at % Z_RING, core, rows]

    def remote(src, dst, send_sem, recv_sem, to):
        return pltpu.make_async_remote_copy(
            src_ref=src,
            dst_ref=dst,
            send_sem=send_sem,
            recv_sem=recv_sem,
            device_id=to,
            device_id_type=MESH,
        )

    def x_copy(r, source_x):
        place = slot(source_x)
        return remote(
            packed_ref, place, x_send.at[r - 1], x_recv.at[r - 1], device(z, x + r, core)
        )

    def z_copy(way, hop, z_from):
        rows = pl.ds(0, group)
        if hop == Z_RING // 2 - 1:
            rows = pl.ds(way * (group // 2), group // 2)
        place = kv_ref.at[z_from % Z_RING, core, rows]
        to = device(z + (1 if way == 0 else Z_RING - 1), x, core)
        return remote(place, place, z_send.at[way, hop], z_recv.at[way, hop], to)

    def z_out(way, hop):
        return z_copy(way, hop, z + (Z_RING - hop if way == 0 else hop))

    def z_in(way, hop):
        return z_copy(way, hop, z + (Z_RING - 1 - hop if way == 0 else 1 + hop))

    def v_copy(k, z_from):
        return remote(
            packed_ref, slot(x, z_from), v_send.at[k - 1], v_recv.at[k - 1], device(z + k, x, core)
        )

    def u_copy(k, r, x_from):
        place = slot(x_from, z + Z_RING - k)
        return remote(
            place, place, u_send.at[k - 1, r - 1], u_recv.at[k - 1, r - 1], device(z, x + r, core)
        )

    def relay(distance):
        for k in (distance, Z_RING - distance)[: 1 if 2 * distance == Z_RING else 2]:
            v_copy(k, z + Z_RING - k).wait_recv()
            for r in range(1, X_RING):
                u_copy(k, r, x).start()

    def relayed(distance):
        for k in (distance, Z_RING - distance)[: 1 if 2 * distance == Z_RING else 2]:
            for r in range(1, X_RING):
                u_copy(k, r, x + X_RING - r).wait_recv()

    def p_copy(number, z_at, core_at):
        place = kv_ref.at[z_at % Z_RING, core_at]
        return remote(
            place, place, p_send.at[number], p_recv.at[number], device(z, x, 1 - core)
        )

    def p_out(number):
        distance = (number + 1) // 2
        return p_copy(number, z + (Z_RING - distance if number % 2 else distance), core)

    own = pltpu.make_async_copy(packed_ref, slot(x), l_sem)
    own.start()
    for r in range(1, X_RING):
        x_copy(r, x).start()

    @pl.when(core == 1)
    def _():
        for k in (1, 7, 2, 6, 3, 5, 4):
            v_copy(k, z).start()

    acc_ref[...] = jnp.zeros_like(acc_ref)
    sum_ref[...] = jnp.zeros_like(sum_ref)
    if guarded:
        max_ref[...] = jnp.full_like(max_ref, -1e30)
    own.wait()
    for r in range(1, X_RING):
        x_copy(r, x + X_RING - r).wait_recv()
    p_out(0).start()

    @pl.when(core == 0)
    def _():
        z_out(0, 0).start()
        z_out(1, 0).start()

    @pl.when(core == 1)
    def _():
        relay(1)

    def step(j, carry):
        i = j + 2
        distance, member = i // 4, i % 4
        z_at = (z + Z_RING + distance * (2 * (member // 2) - 1)) % Z_RING
        core_at = (core + member % 2) % 2

        for hop in range(Z_RING // 2):

            @pl.when((j == 4 * hop + 2) & (core == 0))
            def _(hop=hop):
                z_in(0, hop).wait_recv()
                z_in(1, hop).wait_recv()
                if hop < Z_RING // 2 - 1:
                    z_out(0, hop + 1).start()
                    z_out(1, hop + 1).start()

            @pl.when((j == 4 * hop + 2) & (core == 1))
            def _(hop=hop):
                if hop < Z_RING // 2 - 1:
                    relay(hop + 2)
                relayed(hop + 1)

            @pl.when(j == 4 * hop + 2)
            def _(hop=hop):
                p_out(2 * hop + 1).start()
                if hop < Z_RING // 2 - 1:
                    p_out(2 * hop + 2).start()

        @pl.when(member % 2 == 1)
        def _():
            p_copy(j // 2, z_at, 1 - core).wait_recv()

        slab = kv_ref[z_at, core_at]
        scores = lax.dot_general(
            slab, q_ref[...], (((1,), (1,)), ((), ())), preferred_element_type=jnp.float32
        )
        if guarded:
            before = max_ref[...]
            top = jnp.maximum(before, jnp.max(scores, axis=0, keepdims=True))
            factor = jnp.exp(before - top)
            weights = jnp.exp(scores - top)
            max_ref[...] = top
        else:
            factor = None
            weights = jnp.exp2(scores * LOG2E)
        added = jnp.sum(weights.reshape(group // 8, 8, columns), axis=0)
        mixed = lax.dot_general(
            slab,
            weights.astype(jnp.bfloat16),
            (((0,), (0,)), ((), ())),
            preferred_element_type=jnp.float32,
        )[HEAD_SIZE:]
        if guarded:
            sum_ref[...] = sum_ref[...] * factor + added
            acc_ref[...] = acc_ref[...] * factor + mixed
        else:
            sum_ref[...] += added
            acc_ref[...] += mixed
        return carry

    lax.fori_loop(0, 2 * Z_RING, step, 0)

    attended = acc_ref[...] / jnp.sum(sum_ref[...], axis=0, keepdims=True)
    mean_sq = jnp.mean(attended * attended, axis=0, keepdims=True)
    unit = attended * lax.rsqrt(mean_sq + EPS)
    turned = jnp.concatenate([unit, jnp.zeros_like(unit)], axis=0).T
    low = lax.broadcasted_iota(jnp.int32, (tokens, 128), 1) < HEAD_SIZE
    for pair in range(mine_ref.shape[1] // 128):
        first = turned[(2 * pair) * tokens : (2 * pair + 1) * tokens, :]
        second = turned[(2 * pair + 1) * tokens : (2 * pair + 2) * tokens, :]
        joined = jnp.where(low, first, pltpu.roll(second, HEAD_SIZE, 1))
        lanes = slice(pair * 128, (pair + 1) * 128)
        mine_ref[:, lanes] = (joined * gain_ref[:, lanes]).astype(jnp.bfloat16)

    part = tokens // tp_count

    def rows_of(owner):
        return mine_ref.at[pl.ds(pl.multiple_of((owner % tp_count) * part, part), part)]

    def t_copy(r, source):
        return remote(
            rows_of(tp + r),
            out_ref.at[source % tp_count],
            t_send.at[r - 1],
            t_recv.at[r - 1],
            {"tp": (tp + r) % tp_count},
        )

    for r in range(1, tp_count):
        t_copy(r, tp).start()
    own = pltpu.make_async_copy(rows_of(tp), out_ref.at[tp], l_sem)
    own.start()
    own.wait()
    for r in range(1, X_RING):
        x_copy(r, x).wait_send()

    @pl.when(core == 0)
    def _():
        for way in range(2):
            for hop in range(Z_RING // 2):
                z_out(way, hop).wait_send()

    @pl.when(core == 1)
    def _():
        for k in range(1, Z_RING):
            v_copy(k, z).wait_send()
            for r in range(1, X_RING):
                u_copy(k, r, x).wait_send()

    for number in range(Z_RING):
        p_out(number).wait_send()
    for r in range(1, tp_count):
        t_copy(r, tp + tp_count - r).wait_recv()
        t_copy(r, tp).wait_send()


def moe_kernel(
    heads_ref,
    out_proj_ref,
    residual_ref,
    ffn_gain_ref,
    routes_ref,
    weights_ref,
    shared_gate_ref,
    shared_up_ref,
    shared_down_ref,
    gate_hbm,
    up_hbm,
    down_hbm,
    out_ref,
    own_ref,
    hidden_ref,
    rank_ref,
    scale_ref,
    normed_ref,
    leaving_ref,
    passing_ref,
    arrived_ref,
    made_ref,
    back_passing_ref,
    back_ref,
    acc_ref,
    part_ref,
    got_ref,
    gate_ref,
    up_ref,
    down_ref,
    w_sem,
    l_sem,
    y_send,
    y_recv,
    s_send,
    s_recv,
    z_send,
    z_recv,
    i_send,
    i_recv,
    i_local,
    bz_send,
    bz_recv,
    bi_send,
    bi_recv,
    bi_local,
):
    sp, tp = lax.axis_index("sp"), lax.axis_index("tp")
    tp_count = lax.axis_size("tp")
    z, i = sp // PLANE, sp % PLANE
    part, width = hidden_ref.shape
    tokens = part * tp_count
    quarter = width // 4
    rows = PLANE * 8
    top = routes_ref.shape[0]
    experts = Z_RING * PLANE

    def at_z(z_at):
        return {"sp": (z_at % Z_RING) * PLANE + i}

    def at_i(i_at):
        return {"sp": z * PLANE + i_at % PLANE}

    def at_tp(t):
        return {"tp": t % tp_count}

    barrier = pltpu.get_barrier_semaphore()
    others = [at_z(z + k) for k in range(1, Z_RING)]
    others += [at_i(i + r) for r in range(1, PLANE)]
    others += [at_tp(tp + r) for r in range(1, tp_count)]
    for other in others:
        pl.semaphore_signal(barrier, inc=1, device_id=other, device_id_type=MESH)

    loads = [
        pltpu.make_async_copy(
            residual_ref.at[pl.ds(pl.multiple_of(tp * part, part), part)], own_ref, l_sem
        ),
        pltpu.make_async_copy(gate_hbm, gate_ref, w_sem.at[0]),
        pltpu.make_async_copy(up_hbm, up_ref, w_sem.at[1]),
        pltpu.make_async_copy(down_hbm, down_ref, w_sem.at[2]),
    ]
    for load in loads:
        load.start()

    def remote(src, dst, send_sem, recv_sem, to):
        return pltpu.make_async_remote_copy(
            src_ref=src,
            dst_ref=dst,
            send_sem=send_sem,
            recv_sem=recv_sem,
            device_id=to,
            device_id_type=MESH,
        )

    named = lax.broadcasted_iota(jnp.int32, (experts, tokens), 0) * tp_count + tp
    hot = jnp.zeros((experts, tokens), jnp.float32)
    scale = jnp.zeros((experts, tokens), jnp.float32)
    for choice in range(top):
        same = named == routes_ref[choice : choice + 1, :]
        hot += jnp.where(same, 1.0, 0.0)
        scale += jnp.where(same, weights_ref[choice : choice + 1, :], 0.0)
    earlier = lax.broadcasted_iota(jnp.int32, (tokens, tokens), 0)
    later = lax.broadcasted_iota(jnp.int32, (tokens, tokens), 1)
    before = jnp.where(earlier < later, 1.0, 0.0).astype(jnp.bfloat16)
    rank = jnp.dot(hot.astype(jnp.bfloat16), before, preferred_element_type=jnp.float32)
    rank_ref[...] = jnp.where(hot > 0.0, rank, -1.0).reshape(Z_RING, PLANE, tokens)
    scale_ref[...] = scale.reshape(Z_RING, PLANE, tokens)

    def rows_of_eight(ref, z_at):
        value = ref[z_at][:, None, :]
        return jnp.broadcast_to(value, (PLANE, 8, tokens)).reshape(rows, tokens)

    loads[0].wait()
    size = heads_ref.shape[2]
    total = own_ref[...].astype(jnp.float32)
    for t in range(tp_count):
        total += jnp.dot(
            heads_ref[t],
            out_proj_ref[t * size : (t + 1) * size, :],
            preferred_element_type=jnp.float32,
        )
    hidden = total.astype(jnp.bfloat16).astype(jnp.float32)
    hidden_ref[...] = hidden
    normed_ref[tp] = final_norm(hidden, ffn_gain_ref[...]).astype(jnp.bfloat16)
    pl.semaphore_wait(barrier, len(others))

    y_lanes = (pl.ds(0, quarter), pl.ds(quarter, width - quarter))
    z_lanes = (pl.ds(0, quarter), pl.ds(quarter, width))
    b_lanes = (pl.ds(0, width), pl.ds(width, quarter))
    whole = pl.ds(0, width + quarter)

    def y_copy(r, source, piece):
        place = normed_ref.at[source % tp_count, :, y_lanes[piece]]
        return remote(
            place, place, y_send.at[r - 1, piece], y_recv.at[r - 1, piece], at_tp(tp + r)
        )

    for piece in range(2):
        for r in (2, 1, 3):
            y_copy(r, tp, piece).start()

    def turn(n):
        odd = n % 2
        return odd * ((n + 1) // 2) + (1 - odd) * ((Z_RING - n // 2) % Z_RING)

    def z_copy(k, z_from, z_to, piece):
        return remote(
            leaving_ref.at[z_to % Z_RING, :, :, z_lanes[piece]],
            passing_ref.at[z_from % Z_RING, :, :, z_lanes[piece]],
            z_send.at[k, piece],
            z_recv.at[k, piece],
            at_z(z + k),
        )

    def bz_copy(k, z_from, z_to, piece):
        return remote(
            made_ref.at[z_to % Z_RING, :, :, b_lanes[piece]],
            back_passing_ref.at[z_from % Z_RING, :, :, b_lanes[piece]],
            bz_send.at[k, piece],
            bz_recv.at[k, piece],
            at_z(z + Z_RING - k),
        )

    out_way = (passing_ref, arrived_ref, i_send, i_recv, i_local, whole, 0)
    back_ways = [
        (back_passing_ref, back_ref, bi_send, bi_recv, bi_local, b_lanes[p], p * Z_RING)
        for p in range(2)
    ]

    def i_copy(way, k, z_at, r, tile, place):
        source_ref, target_ref, sends, recvs, _, lanes, shift = way
        return remote(
            source_ref.at[z_at % Z_RING, tile % PLANE, :, lanes],
            target_ref.at[z_at % Z_RING, place % PLANE, :, lanes],
            sends.at[k + shift, r - 1],
            recvs.at[k + shift, r - 1],
            at_i(i + r),
        )

    def own_copy(way, k, z_at):
        source_ref, target_ref, _, _, locals_, lanes, shift = way
        return pltpu.make_async_copy(
            source_ref.at[z_at % Z_RING, i, :, lanes],
            target_ref.at[z_at % Z_RING, i, :, lanes],
            locals_.at[k + shift],
        )

    def spread(way, k, z_at):
        for r in range(1, PLANE):
            i_copy(way, k, z_at, r, i + r, i).start()
        own_copy(way, k, z_at).start()

    def collected(way, k, z_at):
        for r in range(1, PLANE):
            i_copy(way, k, z_at, r, i, i + PLANE - r).wait_recv()
        own_copy(way, k, z_at).wait()

    def sent(way, k, z_at):
        for r in range(1, PLANE):
            i_copy(way, k, z_at, r, i + r, i).wait_send()

    def dispatch(piece, n, carry):
        k = turn(n)
        z_to = (z + k) % Z_RING
        row = lax.broadcasted_iota(jnp.int32, (rows, tokens), 0)
        rank = rows_of_eight(rank_ref, z_to)
        place = (row % 8).astype(jnp.float32)
        main = jnp.where(rank == place, 1.0, 0.0).astype(jnp.bfloat16)
        for q in range(1) if piece == 0 else range(1, 4):
            cols = slice(q * quarter, (q + 1) * quarter)
            normed = normed_ref[:, :, cols].reshape(tokens, quarter)
            leaving_ref[z_to, :, :, cols] = (
                jnp.dot(main, normed, preferred_element_type=jnp.float32)
                .astype(jnp.bfloat16)
                .reshape(PLANE, 8, quarter)
            )
        if piece == 1:
            extra = jnp.where(rank == 8.0 + (row % 8 // 4).astype(jnp.float32), 1.0, 0.0)
            tail = jnp.zeros((rows, quarter), jnp.float32)
            for q in range(4):
                normed = normed_ref[:, :, q * quarter : (q + 1) * quarter].reshape(tokens, quarter)
                chosen = jnp.where(row % 4 == q, extra, 0.0).astype(jnp.bfloat16)
                tail += jnp.dot(chosen, normed, preferred_element_type=jnp.float32)
            leaving_ref[z_to, :, :, width:] = tail.astype(jnp.bfloat16).reshape(PLANE, 8, quarter)

            @pl.when(n == 0)
            def _():
                spread((leaving_ref,) + out_way[1:], 0, z)

        @pl.when(n > 0)
        def _():
            z_copy(k, z, z + k, piece).start()

        return carry

    for piece in range(2):
        for r in range(1, tp_count):
            y_copy(r, tp + tp_count - r, piece).wait_recv()
        lax.fori_loop(0, Z_RING, functools.partial(dispatch, piece), 0)

    normed = normed_ref[...].reshape(tokens, width)
    gate = jnp.dot(normed, shared_gate_ref[...], preferred_element_type=jnp.float32)
    up = jnp.dot(normed, shared_up_ref[...], preferred_element_type=jnp.float32)
    inner = (gate / (1.0 + jnp.exp(-gate)) * up).astype(jnp.bfloat16)
    acc_ref[...] = jnp.dot(inner, shared_down_ref[...], preferred_element_type=jnp.float32)
    for load in loads[1:]:
        load.wait()

    def expert(k):
        z_from = (z + Z_RING - k) % Z_RING
        tiles = arrived_ref[z_from].reshape(rows, width + quarter)
        extra_rows = rows // 4
        place = lax.broadcasted_iota(jnp.int32, (extra_rows, rows), 1)
        index = lax.broadcasted_iota(jnp.int32, (extra_rows, rows), 0)
        pieces = []
        for q in range(4):
            pick = jnp.where(place == 4 * index + q, 1.0, 0.0).astype(jnp.bfloat16)
            pieces.append(
                jnp.dot(pick, tiles[:, width:], preferred_element_type=jnp.float32).astype(
                    jnp.bfloat16
                )
            )
        every = jnp.concatenate([tiles[:, :width], jnp.concatenate(pieces, axis=1)], axis=0)
        gate = jnp.dot(every, gate_ref[...], preferred_element_type=jnp.float32)
        up = jnp.dot(every, up_ref[...], preferred_element_type=jnp.float32)
        inner = (gate / (1.0 + jnp.exp(-gate)) * up).astype(jnp.bfloat16)
        place = lax.broadcasted_iota(jnp.int32, (rows, extra_rows), 0)
        index = lax.broadcasted_iota(jnp.int32, (rows, extra_rows), 1)
        tail = jnp.zeros((rows, quarter), jnp.float32)
        for q in range(4):
            cols = slice(q * quarter, (q + 1) * quarter)
            made = jnp.dot(inner, down_ref[:, cols], preferred_element_type=jnp.float32).astype(
                jnp.bfloat16
            )
            made_ref[z_from, :, :, (q + 1) * quarter : (q + 2) * quarter] = made[:rows].reshape(
                PLANE, 8, quarter
            )
            pick = jnp.where(place == 4 * index + q, 1.0, 0.0).astype(jnp.bfloat16)
            tail += jnp.dot(pick, made[rows:], preferred_element_type=jnp.float32)
        made_ref[z_from, :, :, :quarter] = tail.astype(jnp.bfloat16).reshape(PLANE, 8, quarter)

    made_ways = [(made_ref,) + way[1:] for way in back_ways]

    def arrivals(n, carry):
        @pl.when((n > 0) & (n < Z_RING))
        def _():
            k = turn(n)
            for piece in range(2):
                z_copy(k, z + Z_RING - k, z, piece).wait_recv()
            spread(out_way, k, z + Z_RING - k)

        @pl.when(n > 0)
        def _():
            k = turn(n - 1)
            collected(out_way, k, z + Z_RING - k)
            expert(k)

            @pl.when(n > 1)
            def _():
                bz_copy(k, z, z + Z_RING - k, 0).start()

            @pl.when(n == 1)
            def _():
                spread(made_ways[0], 0, z)

        return carry

    lax.fori_loop(0, Z_RING + 1, arrivals, 0)
    spread(made_ways[1], 0, z)
    for k in (1, 7, 2, 6, 3, 5, 4):
        bz_copy(k, z, z + Z_RING - k, 1).start()

    def combine(piece, z_at):
        def twice(start):
            tiles = back_ref[z_at, :, :, start : start + quarter].reshape(rows, quarter)
            return jnp.concatenate([tiles, tiles], axis=0)

        row = lax.broadcasted_iota(jnp.int32, (rows, tokens), 0)
        rank = rows_of_eight(rank_ref, z_at)
        scale = rows_of_eight(scale_ref, z_at)
        place = (row % 8).astype(jnp.float32)
        main = jnp.where(rank == place, scale, 0.0)
        extra = jnp.where(rank == 8.0 + (row % 8 // 4).astype(jnp.float32), scale, 0.0)

        def two_terms(value):
            high = value.astype(jnp.bfloat16)
            low = (value - high.astype(jnp.float32)).astype(jnp.bfloat16)
            return jnp.concatenate([high, low], axis=0)

        def product(terms, tiles):
            return lax.dot_general(
                terms, tiles, (((0,), (0,)), ((), ())), preferred_element_type=jnp.float32
            )

        main = two_terms(main)
        for q in range(4):
            cols = slice(q * quarter, (q + 1) * quarter)
            if piece == 1:
                if q == 3:
                    acc_ref[:, cols] += product(main, twice((q + 1) * quarter))
                continue
            chosen = two_terms(jnp.where(row % 4 == q, extra, 0.0))
            added = product(chosen, twice(0))
            if q < 3:
                added += product(main, twice((q + 1) * quarter))
            acc_ref[:, cols] += added

    def returns(piece, n, carry):
        @pl.when((n > 0) & (n < Z_RING))
        def _():
            k = turn(n)
            bz_copy(k, z + k, z, piece).wait_recv()
            spread(back_ways[piece], k, z + k)

        @pl.when(n > 0)
        def _():
            k = turn(n - 1)
            collected(back_ways[piece], k, z + k)
            combine(piece, (z + k) % Z_RING)

        return carry

    s_lanes = (pl.ds(0, 3 * quarter), pl.ds(3 * quarter, quarter))

    def s_copy(r, source, piece):
        return remote(
            part_ref.at[(tp + r) % tp_count, :, s_lanes[piece]],
            got_ref.at[source % tp_count, :, s_lanes[piece]],
            s_send.at[r - 1, piece],
            s_recv.at[r - 1, piece],
            at_tp(tp + r),
        )

    for piece in range(2):
        lax.fori_loop(0, Z_RING + 1, functools.partial(returns, piece), 0)
        for r in (2, 1, 3, 0):
            owner = (tp + r) % tp_count
            own_rows = pl.ds(pl.multiple_of(owner * part, part), part)
            lanes = s_lanes[piece]
            part_ref[owner, :, lanes] = acc_ref[own_rows, lanes].astype(jnp.bfloat16)
            if r:
                s_copy(r, tp, piece).start()
            else:
                got_ref[tp, :, lanes] = part_ref[tp, :, lanes]
    for piece in range(2):
        for r in range(1, tp_count):
            s_copy(r, tp + tp_count - r, piece).wait_recv()
    total = hidden_ref[...]
    for t in range(tp_count):
        total += got_ref[t].astype(jnp.float32)
    out_ref[...] = total.astype(jnp.bfloat16)

    for piece in range(2):
        for r in range(1, tp_count):
            y_copy(r, tp, piece).wait_send()
            s_copy(r, tp, piece).wait_send()

    def drain(n, carry):
        @pl.when(n > 0)
        def _():
            for piece in range(2):
                z_copy(n, z, z + n, piece).wait_send()
                bz_copy(n, z, z + Z_RING - n, piece).wait_send()

        sent(out_way, n, z + Z_RING - n)
        for piece in range(2):
            sent(back_ways[piece], n, z + n)
        return carry

    lax.fori_loop(0, Z_RING, drain, 0)


def call(kernel, out_shape, args, specs=None, scratch=(), flops=0, moved=0):
    return pl.pallas_call(
        kernel,
        out_shape=out_shape,
        in_specs=specs or [VM] * len(args),
        out_specs=jax.tree.map(lambda _: VM, out_shape),
        scratch_shapes=scratch,
        compiler_params=pltpu.CompilerParams(vmem_limit_bytes=56 * 2**20),
        cost_estimate=pl.CostEstimate(flops=flops, bytes_accessed=moved, transcendentals=0),
    )(*args)


def shaped(dims, kind=jnp.bfloat16):
    return jax.ShapeDtypeStruct(dims, kind)


def local(
    queries,
    key_matrix,
    values,
    query_gain,
    key_norm_gain,
    head_gain,
    out_proj,
    residual,
    ffn_gain,
    routes,
    route_weights,
    expert_gate,
    expert_up,
    expert_down,
    shared_gate,
    shared_up,
    shared_down,
):
    tokens = queries.shape[0]
    heads = queries.shape[1] // HEAD_SIZE
    sp_count = lax.axis_size("sp")
    tp_count = lax.axis_size("tp")
    sequence_total = tokens * sp_count
    cosine, sine = wide_tables(lax.axis_index("sp") * tokens, tokens, sequence_total)
    columns = heads * tokens
    query_rows, packed, bound = call(
        prepare_kernel,
        (shaped((columns, 128)), shaped((tokens, 128)), shaped((8, 128), jnp.float32)),
        (
            queries,
            key_matrix.T,
            values.T,
            query_gain[None],
            key_norm_gain[None],
            cosine,
            sine,
        ),
    )
    part_rows = tokens // tp_count

    def attention(guarded, number):
        def run(rows, own, gain):
            return pl.pallas_call(
                functools.partial(ring_attention_kernel, guarded),
                out_shape=shaped((tp_count, part_rows, heads * HEAD_SIZE)),
                in_specs=[VM, VM, VM],
                out_specs=VM,
                scratch_shapes=[
                    pltpu.VMEM((Z_RING, 2, X_RING * tokens, 128), jnp.bfloat16),
                    pltpu.VMEM((tokens, heads * HEAD_SIZE), jnp.bfloat16),
                    pltpu.VMEM((HEAD_SIZE, columns), jnp.float32),
                    pltpu.VMEM((8, columns), jnp.float32),
                    pltpu.VMEM((1, columns), jnp.float32),
                    pltpu.SemaphoreType.DMA((X_RING - 1,)),
                    pltpu.SemaphoreType.DMA((X_RING - 1,)),
                    pltpu.SemaphoreType.DMA((2, Z_RING // 2)),
                    pltpu.SemaphoreType.DMA((2, Z_RING // 2)),
                    pltpu.SemaphoreType.DMA((Z_RING - 1,)),
                    pltpu.SemaphoreType.DMA((Z_RING - 1,)),
                    pltpu.SemaphoreType.DMA((Z_RING - 1, X_RING - 1)),
                    pltpu.SemaphoreType.DMA((Z_RING - 1, X_RING - 1)),
                    pltpu.SemaphoreType.DMA((Z_RING,)),
                    pltpu.SemaphoreType.DMA((Z_RING,)),
                    pltpu.SemaphoreType.DMA((tp_count - 1,)),
                    pltpu.SemaphoreType.DMA((tp_count - 1,)),
                    pltpu.SemaphoreType.DMA,
                ],
                compiler_params=pltpu.CompilerParams(
                    vmem_limit_bytes=56 * 2**20, collective_id=number, has_side_effects=True
                ),
                cost_estimate=pl.CostEstimate(
                    flops=4 * columns * sequence_total * 128,
                    bytes_accessed=sequence_total * 256,
                    transcendentals=0,
                ),
            )(rows, own, gain)

        return run

    tiles = lax.cond(
        bound[0, 0] > SAFE_BOUND,
        attention(True, 1),
        attention(False, 0),
        query_rows,
        packed,
        head_gain[None],
    )
    width = residual.shape[1]
    hidden_units = expert_gate.shape[2]
    wide_row = width + width // 4
    tile_set = pltpu.VMEM((Z_RING, PLANE, 8, wide_row), jnp.bfloat16)
    dma = pltpu.SemaphoreType.DMA
    return pl.pallas_call(
        moe_kernel,
        out_shape=shaped((part_rows, width)),
        in_specs=[VM, VM, ANY] + [VM] * 6 + [ANY] * 3,
        out_specs=VM,
        scratch_shapes=[
            pltpu.VMEM((part_rows, width), jnp.bfloat16),
            pltpu.VMEM((part_rows, width), jnp.float32),
            pltpu.VMEM((Z_RING, PLANE, tokens), jnp.float32),
            pltpu.VMEM((Z_RING, PLANE, tokens), jnp.float32),
            pltpu.VMEM((tp_count, part_rows, width), jnp.bfloat16),
            tile_set,
            tile_set,
            tile_set,
            tile_set,
            tile_set,
            tile_set,
            pltpu.VMEM((tokens, width), jnp.float32),
            pltpu.VMEM((tp_count, part_rows, width), jnp.bfloat16),
            pltpu.VMEM((tp_count, part_rows, width), jnp.bfloat16),
            pltpu.VMEM((width, hidden_units), jnp.bfloat16),
            pltpu.VMEM((width, hidden_units), jnp.bfloat16),
            pltpu.VMEM((hidden_units, width), jnp.bfloat16),
            dma((3,)),
            dma,
            dma((tp_count - 1, 2)),
            dma((tp_count - 1, 2)),
            dma((tp_count - 1, 2)),
            dma((tp_count - 1, 2)),
            dma((Z_RING, 2)),
            dma((Z_RING, 2)),
            dma((Z_RING, PLANE - 1)),
            dma((Z_RING, PLANE - 1)),
            dma((Z_RING,)),
            dma((Z_RING, 2)),
            dma((Z_RING, 2)),
            dma((2 * Z_RING, PLANE - 1)),
            dma((2 * Z_RING, PLANE - 1)),
            dma((2 * Z_RING,)),
        ],
        compiler_params=pltpu.CompilerParams(
            vmem_limit_bytes=58 * 2**20, collective_id=2, has_side_effects=True
        ),
    )(
        tiles,
        out_proj,
        residual,
        ffn_gain[None],
        routes.T,
        route_weights.T,
        shared_gate,
        shared_up,
        shared_down,
        expert_gate[0],
        expert_up[0],
        expert_down[0],
    )


def solution(mesh):
    placed = (
        P("sp", "tp"),
        P("sp", "tp"),
        P("sp", "tp"),
        P(),
        P(),
        P("tp"),
        P(),
        P("sp", None),
        P(),
        P("sp", None),
        P("sp", None),
        P(("sp", "tp"), None, None),
        P(("sp", "tp"), None, None),
        P(("sp", "tp"), None, None),
        P(None, "tp"),
        P(None, "tp"),
        P("tp", None),
    )
    return jax.shard_map(
        local, mesh=mesh, in_specs=placed, out_specs=P(("sp", "tp"), None), check_vma=False
    )
```

```python
import functools

import jax
import jax.numpy as jnp
from jax import lax
from jax.experimental import pallas as pl
from jax.experimental.pallas import tpu as pltpu
from jax.sharding import PartitionSpec as P

HEAD_SIZE = 64
GRID_W = 64
EPS = 1e-06
THETA = 10000.0
LOG2E = 1.4426950408889634
SAFE_BOUND = 70.0

VM = pl.BlockSpec(memory_space=pltpu.VMEM)
ANY = pl.BlockSpec(memory_space=pl.ANY)


def final_norm(field, gain):
    mean_sq = jnp.mean(field * field, axis=-1, keepdims=True)
    return field * lax.rsqrt(mean_sq + EPS) * gain


def wide_tables(first, tokens, sequence_total):
    grid_rows = sequence_total // GRID_W
    padded = -(-tokens // GRID_W // 8) * 8
    row_pos = first // GRID_W + jnp.arange(padded, dtype=jnp.int32) - grid_rows // 2
    col_pos = jnp.arange(GRID_W, dtype=jnp.int32) - GRID_W // 2
    place = jnp.concatenate([row_pos, col_pos]).astype(jnp.float32)
    quarter = HEAD_SIZE // 4
    inverse = THETA ** (-jnp.arange(quarter, dtype=jnp.float32) / quarter)
    lane = jnp.arange(2 * HEAD_SIZE, dtype=jnp.int32)
    angles = place[:, None] * jnp.tile(inverse, 8)
    sign = jnp.where((lane % 32) < 16, -1.0, 1.0)
    return jnp.cos(angles), jnp.sin(angles) * sign[None, :]


def spread_table(table, tokens):
    padded = table.shape[0] - GRID_W
    count = tokens // GRID_W
    by_row = jnp.concatenate(
        [jnp.broadcast_to(table[n : n + 1], (GRID_W, 128)) for n in range(count)], axis=0
    )
    by_col = jnp.concatenate([table[padded:]] * count, axis=0)
    lane = lax.broadcasted_iota(jnp.int32, (tokens, 128), 1)
    return jnp.where(lane % HEAD_SIZE < HEAD_SIZE // 2, by_row, by_col)


def normed_and_turned(field, gain, cosine, sine):
    lane = lax.broadcasted_iota(jnp.int32, field.shape, 1)
    low = lane < HEAD_SIZE
    square = field * field
    mean_low = jnp.sum(jnp.where(low, square, 0.0), axis=1, keepdims=True) / HEAD_SIZE
    mean_high = jnp.sum(jnp.where(low, 0.0, square), axis=1, keepdims=True) / HEAD_SIZE
    scale = jnp.where(low, lax.rsqrt(mean_low + EPS), lax.rsqrt(mean_high + EPS))
    unit = field * scale * gain
    partner = jnp.where(
        lane % 32 < 16, pltpu.roll(unit, 128 - 16, 1), pltpu.roll(unit, 16, 1)
    )
    return unit * cosine + partner * sine


def prepare_kernel(
    q_ref, key_ref, value_ref, qg_ref, kg_ref, cos_ref, sin_ref, rows_ref, packed_ref, bound_ref
):
    tokens = q_ref.shape[0]
    cosine = spread_table(cos_ref[...], tokens)
    sine = spread_table(sin_ref[...], tokens)
    low = lax.broadcasted_iota(jnp.int32, (tokens, 128), 1) < HEAD_SIZE
    query_gain = jnp.concatenate([qg_ref[...], qg_ref[...]], axis=1)
    key_gain = jnp.concatenate([kg_ref[...], kg_ref[...]], axis=1)
    top = jnp.max(jnp.abs(query_gain), axis=1, keepdims=True)
    top = top * jnp.max(jnp.abs(key_gain), axis=1, keepdims=True) * (HEAD_SIZE**0.5)
    bound_ref[0, 0] = jnp.max(jnp.broadcast_to(top, (8, 128)))
    both = jnp.concatenate(
        [key_ref[...].astype(jnp.float32), value_ref[...].astype(jnp.float32)], axis=0
    ).T
    turned = normed_and_turned(both, key_gain, cosine, sine)
    packed_ref[...] = jnp.where(low, turned, both).astype(jnp.bfloat16)
    for pair in range(q_ref.shape[1] // 128):
        field = q_ref[:, pair * 128 : (pair + 1) * 128].astype(jnp.float32)
        turned = normed_and_turned(field, query_gain, cosine, sine).astype(jnp.bfloat16)
        turned = turned.astype(jnp.float32) * (HEAD_SIZE**-0.5)
        first = jnp.where(low, turned, 0.0)
        second = jnp.where(low, pltpu.roll(turned, HEAD_SIZE, 1), 0.0)
        rows_ref[(2 * pair) * tokens : (2 * pair + 1) * tokens, :] = first.astype(jnp.bfloat16)
        rows_ref[(2 * pair + 1) * tokens : (2 * pair + 2) * tokens, :] = second.astype(jnp.bfloat16)


MESH = pl.DeviceIdType.MESH
Z_RING, X_RING = 8, 4
PLANE = 2 * X_RING


def ring_attention(
    guarded,
    q_ref,
    packed_ref,
    gain_ref,
    out_ref,
    kv_ref,
    mine_ref,
    acc_ref,
    sum_ref,
    max_ref,
    x_send,
    x_recv,
    z_send,
    z_recv,
    v_send,
    v_recv,
    u_send,
    u_recv,
    p_send,
    p_recv,
    t_send,
    t_recv,
    l_sem,
):
    tokens = packed_ref.shape[0]
    columns = q_ref.shape[0]
    group = X_RING * tokens
    sp, tp = lax.axis_index("sp"), lax.axis_index("tp")
    tp_count = lax.axis_size("tp")
    core = sp % 2
    x = (sp // 2) % X_RING
    z = sp // (2 * X_RING)

    def device(z_at, x_at, core_at):
        return {"sp": ((z_at % Z_RING) * X_RING + x_at % X_RING) * 2 + core_at}

    def slot(x_at, z_at=z):
        rows = pl.ds(pl.multiple_of((x_at % X_RING) * tokens, tokens), tokens)
        return kv_ref.at[z_at % Z_RING, core, rows]

    def remote(src, dst, send_sem, recv_sem, to):
        return pltpu.make_async_remote_copy(
            src_ref=src,
            dst_ref=dst,
            send_sem=send_sem,
            recv_sem=recv_sem,
            device_id=to,
            device_id_type=MESH,
        )

    def x_copy(r, source_x):
        place = slot(source_x)
        return remote(
            packed_ref, place, x_send.at[r - 1], x_recv.at[r - 1], device(z, x + r, core)
        )

    def z_copy(way, hop, z_from):
        rows = pl.ds(0, group)
        if hop == Z_RING // 2 - 1:
            rows = pl.ds(way * (group // 2), group // 2)
        place = kv_ref.at[z_from % Z_RING, core, rows]
        to = device(z + (1 if way == 0 else Z_RING - 1), x, core)
        return remote(place, place, z_send.at[way, hop], z_recv.at[way, hop], to)

    def z_out(way, hop):
        return z_copy(way, hop, z + (Z_RING - hop if way == 0 else hop))

    def z_in(way, hop):
        return z_copy(way, hop, z + (Z_RING - 1 - hop if way == 0 else 1 + hop))

    def v_copy(k, z_from):
        return remote(
            packed_ref, slot(x, z_from), v_send.at[k - 1], v_recv.at[k - 1], device(z + k, x, core)
        )

    def u_copy(k, r, x_from):
        place = slot(x_from, z + Z_RING - k)
        return remote(
            place, place, u_send.at[k - 1, r - 1], u_recv.at[k - 1, r - 1], device(z, x + r, core)
        )

    def relay(distance):
        for k in (distance, Z_RING - distance)[: 1 if 2 * distance == Z_RING else 2]:
            v_copy(k, z + Z_RING - k).wait_recv()
            for r in range(1, X_RING):
                u_copy(k, r, x).start()

    def relayed(distance):
        for k in (distance, Z_RING - distance)[: 1 if 2 * distance == Z_RING else 2]:
            for r in range(1, X_RING):
                u_copy(k, r, x + X_RING - r).wait_recv()

    def p_copy(number, z_at, core_at):
        place = kv_ref.at[z_at % Z_RING, core_at]
        return remote(
            place, place, p_send.at[number], p_recv.at[number], device(z, x, 1 - core)
        )

    def p_out(number):
        distance = (number + 1) // 2
        return p_copy(number, z + (Z_RING - distance if number % 2 else distance), core)

    own = pltpu.make_async_copy(packed_ref, slot(x), l_sem)
    own.start()
    for r in range(1, X_RING):
        x_copy(r, x).start()

    @pl.when(core == 1)
    def _():
        for k in (1, 7, 2, 6, 3, 5, 4):
            v_copy(k, z).start()

    acc_ref[...] = jnp.zeros_like(acc_ref)
    sum_ref[...] = jnp.zeros_like(sum_ref)
    if guarded:
        max_ref[...] = jnp.full_like(max_ref, -1e30)
    own.wait()
    for r in range(1, X_RING):
        x_copy(r, x + X_RING - r).wait_recv()
    p_out(0).start()

    @pl.when(core == 0)
    def _():
        z_out(0, 0).start()
        z_out(1, 0).start()

    @pl.when(core == 1)
    def _():
        relay(1)

    def step(j, carry):
        i = j + 2
        distance, member = i // 4, i % 4
        z_at = (z + Z_RING + distance * (2 * (member // 2) - 1)) % Z_RING
        core_at = (core + member % 2) % 2

        for hop in range(Z_RING // 2):

            @pl.when((j == 4 * hop + 2) & (core == 0))
            def _(hop=hop):
                z_in(0, hop).wait_recv()
                z_in(1, hop).wait_recv()
                if hop < Z_RING // 2 - 1:
                    z_out(0, hop + 1).start()
                    z_out(1, hop + 1).start()

            @pl.when((j == 4 * hop + 2) & (core == 1))
            def _(hop=hop):
                if hop < Z_RING // 2 - 1:
                    relay(hop + 2)
                relayed(hop + 1)

            @pl.when(j == 4 * hop + 2)
            def _(hop=hop):
                p_out(2 * hop + 1).start()
                if hop < Z_RING // 2 - 1:
                    p_out(2 * hop + 2).start()

        @pl.when(member % 2 == 1)
        def _():
            p_copy(j // 2, z_at, 1 - core).wait_recv()

        slab = kv_ref[z_at, core_at]
        scores = lax.dot_general(
            slab, q_ref[...], (((1,), (1,)), ((), ())), preferred_element_type=jnp.float32
        )
        if guarded:
            before = max_ref[...]
            top = jnp.maximum(before, jnp.max(scores, axis=0, keepdims=True))
            factor = jnp.exp(before - top)
            weights = jnp.exp(scores - top)
            max_ref[...] = top
        else:
            factor = None
            weights = jnp.exp2(scores * LOG2E)
        added = jnp.sum(weights.reshape(group // 8, 8, columns), axis=0)
        mixed = lax.dot_general(
            slab,
            weights.astype(jnp.bfloat16),
            (((0,), (0,)), ((), ())),
            preferred_element_type=jnp.float32,
        )[HEAD_SIZE:]
        if guarded:
            sum_ref[...] = sum_ref[...] * factor + added
            acc_ref[...] = acc_ref[...] * factor + mixed
        else:
            sum_ref[...] += added
            acc_ref[...] += mixed
        return carry

    lax.fori_loop(0, 2 * Z_RING, step, 0)

    attended = acc_ref[...] / jnp.sum(sum_ref[...], axis=0, keepdims=True)
    mean_sq = jnp.mean(attended * attended, axis=0, keepdims=True)
    unit = attended * lax.rsqrt(mean_sq + EPS)
    turned = jnp.concatenate([unit, jnp.zeros_like(unit)], axis=0).T
    low = lax.broadcasted_iota(jnp.int32, (tokens, 128), 1) < HEAD_SIZE
    for pair in range(mine_ref.shape[1] // 128):
        first = turned[(2 * pair) * tokens : (2 * pair + 1) * tokens, :]
        second = turned[(2 * pair + 1) * tokens : (2 * pair + 2) * tokens, :]
        joined = jnp.where(low, first, pltpu.roll(second, HEAD_SIZE, 1))
        lanes = slice(pair * 128, (pair + 1) * 128)
        mine_ref[:, lanes] = (joined * gain_ref[:, lanes]).astype(jnp.bfloat16)

    part = tokens // tp_count

    def rows_of(owner):
        return mine_ref.at[pl.ds(pl.multiple_of((owner % tp_count) * part, part), part)]

    def t_copy(r, source):
        return remote(
            rows_of(tp + r),
            out_ref.at[source % tp_count],
            t_send.at[r - 1],
            t_recv.at[r - 1],
            {"tp": (tp + r) % tp_count},
        )

    for r in range(1, tp_count):
        t_copy(r, tp).start()
    own = pltpu.make_async_copy(rows_of(tp), out_ref.at[tp], l_sem)
    own.start()
    own.wait()
    for r in range(1, X_RING):
        x_copy(r, x).wait_send()

    @pl.when(core == 0)
    def _():
        for way in range(2):
            for hop in range(Z_RING // 2):
                z_out(way, hop).wait_send()

    @pl.when(core == 1)
    def _():
        for k in range(1, Z_RING):
            v_copy(k, z).wait_send()
            for r in range(1, X_RING):
                u_copy(k, r, x).wait_send()

    for number in range(Z_RING):
        p_out(number).wait_send()
    for r in range(1, tp_count):
        t_copy(r, tp + tp_count - r).wait_recv()
        t_copy(r, tp).wait_send()


def layer_kernel(
    guarded,
    q_ref,
    packed_ref,
    gain_ref,
    residual_ref,
    ffn_gain_ref,
    routes_ref,
    weights_ref,
    out_proj_hbm,
    shared_gate_hbm,
    shared_up_hbm,
    shared_down_hbm,
    gate_hbm,
    up_hbm,
    down_hbm,
    out_ref,
    attention_scratch,
    heads_ref,
    out_proj_ref,
    shared_gate_ref,
    shared_up_ref,
    shared_down_ref,
    own_ref,
    hidden_ref,
    rank_ref,
    scale_ref,
    normed_ref,
    leaving_ref,
    passing_ref,
    arrived_ref,
    made_ref,
    back_passing_ref,
    back_ref,
    acc_ref,
    part_ref,
    got_ref,
    gate_ref,
    up_ref,
    down_ref,
    w_sem,
    l_sem,
    y_send,
    y_recv,
    s_send,
    s_recv,
    z_send,
    z_recv,
    i_send,
    i_recv,
    i_local,
    bz_send,
    bz_recv,
    bi_send,
    bi_recv,
    bi_local,
):
    sp, tp = lax.axis_index("sp"), lax.axis_index("tp")
    tp_count = lax.axis_size("tp")
    z, i = sp // PLANE, sp % PLANE
    part, width = hidden_ref.shape
    tokens = part * tp_count
    quarter = width // 4
    rows = PLANE * 8
    top = routes_ref.shape[0]
    experts = Z_RING * PLANE

    def at_z(z_at):
        return {"sp": (z_at % Z_RING) * PLANE + i}

    def at_i(i_at):
        return {"sp": z * PLANE + i_at % PLANE}

    def at_tp(t):
        return {"tp": t % tp_count}

    barrier = pltpu.get_barrier_semaphore()
    others = [at_z(z + k) for k in range(1, Z_RING)]
    others += [at_i(i + r) for r in range(1, PLANE)]
    others += [at_tp(tp + r) for r in range(1, tp_count)]
    for other in others:
        pl.semaphore_signal(barrier, inc=1, device_id=other, device_id_type=MESH)

    loads = [
        pltpu.make_async_copy(
            residual_ref.at[pl.ds(pl.multiple_of(tp * part, part), part)], own_ref, l_sem
        ),
    ]
    weights = (
        (out_proj_hbm, out_proj_ref),
        (shared_gate_hbm, shared_gate_ref),
        (shared_up_hbm, shared_up_ref),
        (shared_down_hbm, shared_down_ref),
        (gate_hbm, gate_ref),
        (up_hbm, up_ref),
        (down_hbm, down_ref),
    )
    for number, (source, target) in enumerate(weights):
        loads.append(pltpu.make_async_copy(source, target, w_sem.at[number]))
    for load in loads:
        load.start()

    def remote(src, dst, send_sem, recv_sem, to):
        return pltpu.make_async_remote_copy(
            src_ref=src,
            dst_ref=dst,
            send_sem=send_sem,
            recv_sem=recv_sem,
            device_id=to,
            device_id_type=MESH,
        )

    named = lax.broadcasted_iota(jnp.int32, (experts, tokens), 0) * tp_count + tp
    hot = jnp.zeros((experts, tokens), jnp.float32)
    scale = jnp.zeros((experts, tokens), jnp.float32)
    for choice in range(top):
        same = named == routes_ref[choice : choice + 1, :]
        hot += jnp.where(same, 1.0, 0.0)
        scale += jnp.where(same, weights_ref[choice : choice + 1, :], 0.0)
    earlier = lax.broadcasted_iota(jnp.int32, (tokens, tokens), 0)
    later = lax.broadcasted_iota(jnp.int32, (tokens, tokens), 1)
    before = jnp.where(earlier < later, 1.0, 0.0).astype(jnp.bfloat16)
    rank = jnp.dot(hot.astype(jnp.bfloat16), before, preferred_element_type=jnp.float32)
    rank_ref[...] = jnp.where(hot > 0.0, rank, -1.0).reshape(Z_RING, PLANE, tokens)
    scale_ref[...] = scale.reshape(Z_RING, PLANE, tokens)

    def rows_of_eight(ref, z_at):
        value = ref[z_at][:, None, :]
        return jnp.broadcast_to(value, (PLANE, 8, tokens)).reshape(rows, tokens)

    pl.semaphore_wait(barrier, len(others))
    ring_attention(guarded, q_ref, packed_ref, gain_ref, heads_ref, *attention_scratch)

    for load in loads:
        load.wait()
    size = heads_ref.shape[2]
    total = own_ref[...].astype(jnp.float32)
    for t in range(tp_count):
        total += jnp.dot(
            heads_ref[t],
            out_proj_ref[t * size : (t + 1) * size, :],
            preferred_element_type=jnp.float32,
        )
    hidden = total.astype(jnp.bfloat16).astype(jnp.float32)
    hidden_ref[...] = hidden
    normed_ref[tp] = final_norm(hidden, ffn_gain_ref[...]).astype(jnp.bfloat16)
    y_lanes = (pl.ds(0, quarter), pl.ds(quarter, width - quarter))
    z_lanes = (pl.ds(0, quarter), pl.ds(quarter, width))
    b_lanes = (pl.ds(0, width), pl.ds(width, quarter))
    whole = pl.ds(0, width + quarter)

    def y_copy(r, source, piece):
        place = normed_ref.at[source % tp_count, :, y_lanes[piece]]
        return remote(
            place, place, y_send.at[r - 1, piece], y_recv.at[r - 1, piece], at_tp(tp + r)
        )

    for piece in range(2):
        for r in (2, 1, 3):
            y_copy(r, tp, piece).start()

    def turn(n):
        odd = n % 2
        return odd * ((n + 1) // 2) + (1 - odd) * ((Z_RING - n // 2) % Z_RING)

    def z_copy(k, z_from, z_to, piece):
        return remote(
            leaving_ref.at[z_to % Z_RING, :, :, z_lanes[piece]],
            passing_ref.at[z_from % Z_RING, :, :, z_lanes[piece]],
            z_send.at[k, piece],
            z_recv.at[k, piece],
            at_z(z + k),
        )

    def bz_copy(k, z_from, z_to, piece):
        return remote(
            made_ref.at[z_to % Z_RING, :, :, b_lanes[piece]],
            back_passing_ref.at[z_from % Z_RING, :, :, b_lanes[piece]],
            bz_send.at[k, piece],
            bz_recv.at[k, piece],
            at_z(z + Z_RING - k),
        )

    out_way = (passing_ref, arrived_ref, i_send, i_recv, i_local, whole, 0)
    back_ways = [
        (back_passing_ref, back_ref, bi_send, bi_recv, bi_local, b_lanes[p], p * Z_RING)
        for p in range(2)
    ]

    def i_copy(way, k, z_at, r, tile, place):
        source_ref, target_ref, sends, recvs, _, lanes, shift = way
        return remote(
            source_ref.at[z_at % Z_RING, tile % PLANE, :, lanes],
            target_ref.at[z_at % Z_RING, place % PLANE, :, lanes],
            sends.at[k + shift, r - 1],
            recvs.at[k + shift, r - 1],
            at_i(i + r),
        )

    def own_copy(way, k, z_at):
        source_ref, target_ref, _, _, locals_, lanes, shift = way
        return pltpu.make_async_copy(
            source_ref.at[z_at % Z_RING, i, :, lanes],
            target_ref.at[z_at % Z_RING, i, :, lanes],
            locals_.at[k + shift],
        )

    def spread(way, k, z_at):
        for r in range(1, PLANE):
            i_copy(way, k, z_at, r, i + r, i).start()
        own_copy(way, k, z_at).start()

    def collected(way, k, z_at):
        for r in range(1, PLANE):
            i_copy(way, k, z_at, r, i, i + PLANE - r).wait_recv()
        own_copy(way, k, z_at).wait()

    def sent(way, k, z_at):
        for r in range(1, PLANE):
            i_copy(way, k, z_at, r, i + r, i).wait_send()

    def dispatch(piece, n, carry):
        k = turn(n)
        z_to = (z + k) % Z_RING
        row = lax.broadcasted_iota(jnp.int32, (rows, tokens), 0)
        rank = rows_of_eight(rank_ref, z_to)
        place = (row % 8).astype(jnp.float32)
        main = jnp.where(rank == place, 1.0, 0.0).astype(jnp.bfloat16)
        for q in range(1) if piece == 0 else range(1, 4):
            cols = slice(q * quarter, (q + 1) * quarter)
            normed = normed_ref[:, :, cols].reshape(tokens, quarter)
            leaving_ref[z_to, :, :, cols] = (
                jnp.dot(main, normed, preferred_element_type=jnp.float32)
                .astype(jnp.bfloat16)
                .reshape(PLANE, 8, quarter)
            )
        if piece == 1:
            extra = jnp.where(rank == 8.0 + (row % 8 // 4).astype(jnp.float32), 1.0, 0.0)
            tail = jnp.zeros((rows, quarter), jnp.float32)
            for q in range(4):
                normed = normed_ref[:, :, q * quarter : (q + 1) * quarter].reshape(tokens, quarter)
                chosen = jnp.where(row % 4 == q, extra, 0.0).astype(jnp.bfloat16)
                tail += jnp.dot(chosen, normed, preferred_element_type=jnp.float32)
            leaving_ref[z_to, :, :, width:] = tail.astype(jnp.bfloat16).reshape(PLANE, 8, quarter)

            @pl.when(n == 0)
            def _():
                spread((leaving_ref,) + out_way[1:], 0, z)

        @pl.when(n > 0)
        def _():
            z_copy(k, z, z + k, piece).start()

        return carry

    for piece in range(2):
        for r in range(1, tp_count):
            y_copy(r, tp + tp_count - r, piece).wait_recv()
        lax.fori_loop(0, Z_RING, functools.partial(dispatch, piece), 0)

    normed = normed_ref[...].reshape(tokens, width)
    gate = jnp.dot(normed, shared_gate_ref[...], preferred_element_type=jnp.float32)
    up = jnp.dot(normed, shared_up_ref[...], preferred_element_type=jnp.float32)
    inner = (gate / (1.0 + jnp.exp(-gate)) * up).astype(jnp.bfloat16)
    acc_ref[...] = jnp.dot(inner, shared_down_ref[...], preferred_element_type=jnp.float32)

    def expert(k):
        z_from = (z + Z_RING - k) % Z_RING
        tiles = arrived_ref[z_from].reshape(rows, width + quarter)
        extra_rows = rows // 4
        place = lax.broadcasted_iota(jnp.int32, (extra_rows, rows), 1)
        index = lax.broadcasted_iota(jnp.int32, (extra_rows, rows), 0)
        pieces = []
        for q in range(4):
            pick = jnp.where(place == 4 * index + q, 1.0, 0.0).astype(jnp.bfloat16)
            pieces.append(
                jnp.dot(pick, tiles[:, width:], preferred_element_type=jnp.float32).astype(
                    jnp.bfloat16
                )
            )
        every = jnp.concatenate([tiles[:, :width], jnp.concatenate(pieces, axis=1)], axis=0)
        gate = jnp.dot(every, gate_ref[...], preferred_element_type=jnp.float32)
        up = jnp.dot(every, up_ref[...], preferred_element_type=jnp.float32)
        inner = (gate / (1.0 + jnp.exp(-gate)) * up).astype(jnp.bfloat16)
        place = lax.broadcasted_iota(jnp.int32, (rows, extra_rows), 0)
        index = lax.broadcasted_iota(jnp.int32, (rows, extra_rows), 1)
        tail = jnp.zeros((rows, quarter), jnp.float32)
        for q in range(4):
            cols = slice(q * quarter, (q + 1) * quarter)
            made = jnp.dot(inner, down_ref[:, cols], preferred_element_type=jnp.float32).astype(
                jnp.bfloat16
            )
            made_ref[z_from, :, :, (q + 1) * quarter : (q + 2) * quarter] = made[:rows].reshape(
                PLANE, 8, quarter
            )
            pick = jnp.where(place == 4 * index + q, 1.0, 0.0).astype(jnp.bfloat16)
            tail += jnp.dot(pick, made[rows:], preferred_element_type=jnp.float32)
        made_ref[z_from, :, :, :quarter] = tail.astype(jnp.bfloat16).reshape(PLANE, 8, quarter)

    made_ways = [(made_ref,) + way[1:] for way in back_ways]

    def arrivals(n, carry):
        @pl.when((n > 0) & (n < Z_RING))
        def _():
            k = turn(n)
            for piece in range(2):
                z_copy(k, z + Z_RING - k, z, piece).wait_recv()
            spread(out_way, k, z + Z_RING - k)

        @pl.when(n > 0)
        def _():
            k = turn(n - 1)
            collected(out_way, k, z + Z_RING - k)
            expert(k)

            @pl.when(n > 1)
            def _():
                bz_copy(k, z, z + Z_RING - k, 0).start()

            @pl.when(n == 1)
            def _():
                spread(made_ways[0], 0, z)

        return carry

    lax.fori_loop(0, Z_RING + 1, arrivals, 0)
    spread(made_ways[1], 0, z)
    for k in (1, 7, 2, 6, 3, 5, 4):
        bz_copy(k, z, z + Z_RING - k, 1).start()

    def combine(piece, z_at):
        def twice(start):
            tiles = back_ref[z_at, :, :, start : start + quarter].reshape(rows, quarter)
            return jnp.concatenate([tiles, tiles], axis=0)

        row = lax.broadcasted_iota(jnp.int32, (rows, tokens), 0)
        rank = rows_of_eight(rank_ref, z_at)
        scale = rows_of_eight(scale_ref, z_at)
        place = (row % 8).astype(jnp.float32)
        main = jnp.where(rank == place, scale, 0.0)
        extra = jnp.where(rank == 8.0 + (row % 8 // 4).astype(jnp.float32), scale, 0.0)

        def two_terms(value):
            high = value.astype(jnp.bfloat16)
            low = (value - high.astype(jnp.float32)).astype(jnp.bfloat16)
            return jnp.concatenate([high, low], axis=0)

        def product(terms, tiles):
            return lax.dot_general(
                terms, tiles, (((0,), (0,)), ((), ())), preferred_element_type=jnp.float32
            )

        main = two_terms(main)
        for q in range(4):
            cols = slice(q * quarter, (q + 1) * quarter)
            if piece == 1:
                if q == 3:
                    acc_ref[:, cols] += product(main, twice((q + 1) * quarter))
                continue
            chosen = two_terms(jnp.where(row % 4 == q, extra, 0.0))
            added = product(chosen, twice(0))
            if q < 3:
                added += product(main, twice((q + 1) * quarter))
            acc_ref[:, cols] += added

    def returns(piece, n, carry):
        @pl.when((n > 0) & (n < Z_RING))
        def _():
            k = turn(n)
            bz_copy(k, z + k, z, piece).wait_recv()
            spread(back_ways[piece], k, z + k)

        @pl.when(n > 0)
        def _():
            k = turn(n - 1)
            collected(back_ways[piece], k, z + k)
            combine(piece, (z + k) % Z_RING)

        return carry

    s_lanes = (pl.ds(0, 3 * quarter), pl.ds(3 * quarter, quarter))

    def s_copy(r, source, piece):
        return remote(
            part_ref.at[(tp + r) % tp_count, :, s_lanes[piece]],
            got_ref.at[source % tp_count, :, s_lanes[piece]],
            s_send.at[r - 1, piece],
            s_recv.at[r - 1, piece],
            at_tp(tp + r),
        )

    for piece in range(2):
        lax.fori_loop(0, Z_RING + 1, functools.partial(returns, piece), 0)
        for r in (2, 1, 3, 0):
            owner = (tp + r) % tp_count
            own_rows = pl.ds(pl.multiple_of(owner * part, part), part)
            lanes = s_lanes[piece]
            part_ref[owner, :, lanes] = acc_ref[own_rows, lanes].astype(jnp.bfloat16)
            if r:
                s_copy(r, tp, piece).start()
            else:
                got_ref[tp, :, lanes] = part_ref[tp, :, lanes]
    for piece in range(2):
        for r in range(1, tp_count):
            s_copy(r, tp + tp_count - r, piece).wait_recv()
    total = hidden_ref[...]
    for t in range(tp_count):
        total += got_ref[t].astype(jnp.float32)
    out_ref[...] = total.astype(jnp.bfloat16)

    for piece in range(2):
        for r in range(1, tp_count):
            y_copy(r, tp, piece).wait_send()
            s_copy(r, tp, piece).wait_send()

    def drain(n, carry):
        @pl.when(n > 0)
        def _():
            for piece in range(2):
                z_copy(n, z, z + n, piece).wait_send()
                bz_copy(n, z, z + Z_RING - n, piece).wait_send()

        sent(out_way, n, z + Z_RING - n)
        for piece in range(2):
            sent(back_ways[piece], n, z + n)
        return carry

    lax.fori_loop(0, Z_RING, drain, 0)


def call(kernel, out_shape, out_specs, args):
    return pl.pallas_call(
        kernel,
        out_shape=out_shape,
        in_specs=[VM] * len(args),
        out_specs=out_specs,
    )(*args)


def shaped(dims, kind=jnp.bfloat16):
    return jax.ShapeDtypeStruct(dims, kind)


def local(
    queries,
    key_matrix,
    values,
    query_gain,
    key_norm_gain,
    head_gain,
    out_proj,
    residual,
    ffn_gain,
    routes,
    route_weights,
    expert_gate,
    expert_up,
    expert_down,
    shared_gate,
    shared_up,
    shared_down,
):
    tokens = queries.shape[0]
    heads = queries.shape[1] // HEAD_SIZE
    sp_count = lax.axis_size("sp")
    tp_count = lax.axis_size("tp")
    sequence_total = tokens * sp_count
    cosine, sine = wide_tables(lax.axis_index("sp") * tokens, tokens, sequence_total)
    columns = heads * tokens
    query_rows, packed, bound = call(
        prepare_kernel,
        (shaped((columns, 128)), shaped((tokens, 128)), shaped((1, 1), jnp.float32)),
        (VM, VM, pl.BlockSpec(memory_space=pltpu.SMEM)),
        (
            queries,
            key_matrix.T,
            values.T,
            query_gain[None],
            key_norm_gain[None],
            cosine,
            sine,
        ),
    )
    part_rows = tokens // tp_count

    width = residual.shape[1]
    hidden_units = expert_gate.shape[2]
    wide_row = width + width // 4
    tile_set = pltpu.VMEM((Z_RING, PLANE, 8, wide_row), jnp.bfloat16)
    dma = pltpu.SemaphoreType.DMA

    def like(weight):
        return pltpu.VMEM(weight.shape, weight.dtype)

    operands = (
        query_rows,
        packed,
        head_gain[None],
        residual,
        ffn_gain[None],
        routes.T,
        route_weights.T,
        out_proj,
        shared_gate,
        shared_up,
        shared_down,
        expert_gate[0],
        expert_up[0],
        expert_down[0],
    )
    attention_scratch = (
        pltpu.VMEM((Z_RING, 2, X_RING * tokens, 128), jnp.bfloat16),
        pltpu.VMEM((tokens, heads * HEAD_SIZE), jnp.bfloat16),
        pltpu.VMEM((HEAD_SIZE, columns), jnp.float32),
        pltpu.VMEM((8, columns), jnp.float32),
        pltpu.VMEM((1, columns), jnp.float32),
        dma((X_RING - 1,)),
        dma((X_RING - 1,)),
        dma((2, Z_RING // 2)),
        dma((2, Z_RING // 2)),
        dma((Z_RING - 1,)),
        dma((Z_RING - 1,)),
        dma((Z_RING - 1, X_RING - 1)),
        dma((Z_RING - 1, X_RING - 1)),
        dma((Z_RING,)),
        dma((Z_RING,)),
        dma((tp_count - 1,)),
        dma((tp_count - 1,)),
        dma,
    )

    def layer(guarded, number):
        return pl.pallas_call(
            functools.partial(layer_kernel, guarded),
            out_shape=shaped((part_rows, width)),
            in_specs=[VM] * 3 + [ANY] + [VM] * 3 + [ANY] * 7,
            out_specs=VM,
            scratch_shapes=[
                attention_scratch,
                pltpu.VMEM((tp_count, part_rows, heads * HEAD_SIZE), jnp.bfloat16),
                like(out_proj),
                like(shared_gate),
                like(shared_up),
                like(shared_down),
                pltpu.VMEM((part_rows, width), jnp.bfloat16),
                pltpu.VMEM((part_rows, width), jnp.float32),
                pltpu.VMEM((Z_RING, PLANE, tokens), jnp.float32),
                pltpu.VMEM((Z_RING, PLANE, tokens), jnp.float32),
                pltpu.VMEM((tp_count, part_rows, width), jnp.bfloat16),
                tile_set,
                tile_set,
                tile_set,
                tile_set,
                tile_set,
                tile_set,
                pltpu.VMEM((tokens, width), jnp.float32),
                pltpu.VMEM((tp_count, part_rows, width), jnp.bfloat16),
                pltpu.VMEM((tp_count, part_rows, width), jnp.bfloat16),
                like(expert_gate[0]),
                like(expert_up[0]),
                like(expert_down[0]),
                dma((7,)),
                dma,
                dma((tp_count - 1, 2)),
                dma((tp_count - 1, 2)),
                dma((tp_count - 1, 2)),
                dma((tp_count - 1, 2)),
                dma((Z_RING, 2)),
                dma((Z_RING, 2)),
                dma((Z_RING, PLANE - 1)),
                dma((Z_RING, PLANE - 1)),
                dma((Z_RING,)),
                dma((Z_RING, 2)),
                dma((Z_RING, 2)),
                dma((2 * Z_RING, PLANE - 1)),
                dma((2 * Z_RING, PLANE - 1)),
                dma((2 * Z_RING,)),
            ],
            compiler_params=pltpu.CompilerParams(
                vmem_limit_bytes=62 * 2**20, collective_id=number, has_side_effects=True
            ),
        )

    return lax.cond(bound[0, 0] > SAFE_BOUND, layer(True, 1), layer(False, 0), *operands)


def solution(mesh):
    placed = (
        P("sp", "tp"),
        P("sp", "tp"),
        P("sp", "tp"),
        P(),
        P(),
        P("tp"),
        P(),
        P("sp", None),
        P(),
        P("sp", None),
        P("sp", None),
        P(("sp", "tp"), None, None),
        P(("sp", "tp"), None, None),
        P(("sp", "tp"), None, None),
        P(None, "tp"),
        P(None, "tp"),
        P("tp", None),
    )
    return jax.shard_map(
        local, mesh=mesh, in_specs=placed, out_specs=P(("sp", "tp"), None), check_vma=False
    )
```

```python
import functools

import jax
import jax.numpy as jnp
from jax import lax
from jax.experimental import pallas as pl
from jax.experimental.pallas import tpu as pltpu
from jax.sharding import PartitionSpec as P

HEAD_SIZE = 64
GRID_W = 64
EPS = 1e-06
THETA = 10000.0
LOG2E = 1.4426950408889634
SAFE_BOUND = 70.0

VM = pl.BlockSpec(memory_space=pltpu.VMEM)
ANY = pl.BlockSpec(memory_space=pl.ANY)


def final_norm(field, gain):
    mean_sq = jnp.mean(field * field, axis=-1, keepdims=True)
    return field * lax.rsqrt(mean_sq + EPS) * gain


def wide_tables(first, tokens, sequence_total):
    grid_rows = sequence_total // GRID_W
    padded = -(-tokens // GRID_W // 8) * 8
    row_pos = first // GRID_W + jnp.arange(padded, dtype=jnp.int32) - grid_rows // 2
    col_pos = jnp.arange(GRID_W, dtype=jnp.int32) - GRID_W // 2
    place = jnp.concatenate([row_pos, col_pos]).astype(jnp.float32)
    quarter = HEAD_SIZE // 4
    inverse = THETA ** (-jnp.arange(quarter, dtype=jnp.float32) / quarter)
    lane = jnp.arange(2 * HEAD_SIZE, dtype=jnp.int32)
    angles = place[:, None] * jnp.tile(inverse, 8)
    sign = jnp.where((lane % 32) < 16, -1.0, 1.0)
    return jnp.cos(angles), jnp.sin(angles) * sign[None, :]


def spread_table(table, tokens):
    padded = table.shape[0] - GRID_W
    count = tokens // GRID_W
    by_row = jnp.concatenate(
        [jnp.broadcast_to(table[n : n + 1], (GRID_W, 128)) for n in range(count)], axis=0
    )
    by_col = jnp.concatenate([table[padded:]] * count, axis=0)
    lane = lax.broadcasted_iota(jnp.int32, (tokens, 128), 1)
    return jnp.where(lane % HEAD_SIZE < HEAD_SIZE // 2, by_row, by_col)


def normed_and_turned(field, gain, cosine, sine):
    lane = lax.broadcasted_iota(jnp.int32, field.shape, 1)
    low = lane < HEAD_SIZE
    square = field * field
    mean_low = jnp.sum(jnp.where(low, square, 0.0), axis=1, keepdims=True) / HEAD_SIZE
    mean_high = jnp.sum(jnp.where(low, 0.0, square), axis=1, keepdims=True) / HEAD_SIZE
    scale = jnp.where(low, lax.rsqrt(mean_low + EPS), lax.rsqrt(mean_high + EPS))
    unit = field * scale * gain
    partner = jnp.where(
        lane % 32 < 16, pltpu.roll(unit, 128 - 16, 1), pltpu.roll(unit, 16, 1)
    )
    return unit * cosine + partner * sine


def prepare_kernel(
    q_ref, key_ref, value_ref, qg_ref, kg_ref, cos_ref, sin_ref, rows_ref, packed_ref, bound_ref
):
    tokens = q_ref.shape[0]
    cosine = spread_table(cos_ref[...], tokens)
    sine = spread_table(sin_ref[...], tokens)
    low = lax.broadcasted_iota(jnp.int32, (tokens, 128), 1) < HEAD_SIZE
    query_gain = jnp.concatenate([qg_ref[...], qg_ref[...]], axis=1)
    key_gain = jnp.concatenate([kg_ref[...], kg_ref[...]], axis=1)
    top = jnp.max(jnp.abs(query_gain), axis=1, keepdims=True)
    top = top * jnp.max(jnp.abs(key_gain), axis=1, keepdims=True) * (HEAD_SIZE**0.5)
    bound_ref[0, 0] = jnp.max(jnp.broadcast_to(top, (8, 128)))
    both = jnp.concatenate(
        [key_ref[...].astype(jnp.float32), value_ref[...].astype(jnp.float32)], axis=0
    ).T
    turned = normed_and_turned(both, key_gain, cosine, sine)
    packed_ref[...] = jnp.where(low, turned, both).astype(jnp.bfloat16)
    for pair in range(q_ref.shape[1] // 128):
        field = q_ref[:, pair * 128 : (pair + 1) * 128].astype(jnp.float32)
        turned = normed_and_turned(field, query_gain, cosine, sine).astype(jnp.bfloat16)
        turned = turned.astype(jnp.float32) * (HEAD_SIZE**-0.5)
        first = jnp.where(low, turned, 0.0)
        second = jnp.where(low, pltpu.roll(turned, HEAD_SIZE, 1), 0.0)
        rows_ref[(2 * pair) * tokens : (2 * pair + 1) * tokens, :] = first.astype(jnp.bfloat16)
        rows_ref[(2 * pair + 1) * tokens : (2 * pair + 2) * tokens, :] = second.astype(jnp.bfloat16)


MESH = pl.DeviceIdType.MESH
Z_RING, X_RING = 8, 4
PLANE = 2 * X_RING


def ring_attention(
    guarded,
    q_ref,
    packed_ref,
    gain_ref,
    out_ref,
    kv_ref,
    mine_ref,
    acc_ref,
    sum_ref,
    max_ref,
    x_send,
    x_recv,
    z_send,
    z_recv,
    v_send,
    v_recv,
    u_send,
    u_recv,
    p_send,
    p_recv,
    t_send,
    t_recv,
    l_sem,
):
    tokens = packed_ref.shape[0]
    columns = q_ref.shape[0]
    group = X_RING * tokens
    sp, tp = lax.axis_index("sp"), lax.axis_index("tp")
    tp_count = lax.axis_size("tp")
    core = sp % 2
    x = (sp // 2) % X_RING
    z = sp // (2 * X_RING)

    def device(z_at, x_at, core_at):
        return {"sp": ((z_at % Z_RING) * X_RING + x_at % X_RING) * 2 + core_at}

    def slot(x_at, z_at=z):
        rows = pl.ds(pl.multiple_of((x_at % X_RING) * tokens, tokens), tokens)
        return kv_ref.at[z_at % Z_RING, core, rows]

    def remote(src, dst, send_sem, recv_sem, to):
        return pltpu.make_async_remote_copy(
            src_ref=src,
            dst_ref=dst,
            send_sem=send_sem,
            recv_sem=recv_sem,
            device_id=to,
            device_id_type=MESH,
        )

    def x_copy(r, source_x):
        place = slot(source_x)
        return remote(
            packed_ref, place, x_send.at[r - 1], x_recv.at[r - 1], device(z, x + r, core)
        )

    def z_copy(way, hop, z_from):
        rows = pl.ds(0, group)
        if hop == Z_RING // 2 - 1:
            rows = pl.ds(way * (group // 2), group // 2)
        place = kv_ref.at[z_from % Z_RING, core, rows]
        to = device(z + (1 if way == 0 else Z_RING - 1), x, core)
        return remote(place, place, z_send.at[way, hop], z_recv.at[way, hop], to)

    def z_out(way, hop):
        return z_copy(way, hop, z + (Z_RING - hop if way == 0 else hop))

    def z_in(way, hop):
        return z_copy(way, hop, z + (Z_RING - 1 - hop if way == 0 else 1 + hop))

    def v_copy(k, z_from):
        return remote(
            packed_ref, slot(x, z_from), v_send.at[k - 1], v_recv.at[k - 1], device(z + k, x, core)
        )

    def u_copy(k, r, x_from):
        place = slot(x_from, z + Z_RING - k)
        return remote(
            place, place, u_send.at[k - 1, r - 1], u_recv.at[k - 1, r - 1], device(z, x + r, core)
        )

    def relay(distance):
        for k in (distance, Z_RING - distance)[: 1 if 2 * distance == Z_RING else 2]:
            v_copy(k, z + Z_RING - k).wait_recv()
            for r in range(1, X_RING):
                u_copy(k, r, x).start()

    def relayed(distance):
        for k in (distance, Z_RING - distance)[: 1 if 2 * distance == Z_RING else 2]:
            for r in range(1, X_RING):
                u_copy(k, r, x + X_RING - r).wait_recv()

    def p_copy(number, z_at, core_at):
        place = kv_ref.at[z_at % Z_RING, core_at]
        return remote(
            place, place, p_send.at[number], p_recv.at[number], device(z, x, 1 - core)
        )

    def p_out(number):
        distance = (number + 1) // 2
        return p_copy(number, z + (Z_RING - distance if number % 2 else distance), core)

    own = pltpu.make_async_copy(packed_ref, slot(x), l_sem)
    own.start()
    for r in range(1, X_RING):
        x_copy(r, x).start()

    @pl.when(core == 1)
    def _():
        for k in (1, 7, 2, 6, 3, 5, 4):
            v_copy(k, z).start()

    acc_ref[...] = jnp.zeros_like(acc_ref)
    sum_ref[...] = jnp.zeros_like(sum_ref)
    if guarded:
        max_ref[...] = jnp.full_like(max_ref, -1e30)
    own.wait()
    for r in range(1, X_RING):
        x_copy(r, x + X_RING - r).wait_recv()
    p_out(0).start()

    @pl.when(core == 0)
    def _():
        z_out(0, 0).start()
        z_out(1, 0).start()

    @pl.when(core == 1)
    def _():
        relay(1)

    def step(j, carry):
        i = j + 2
        distance, member = i // 4, i % 4
        z_at = (z + Z_RING + distance * (2 * (member // 2) - 1)) % Z_RING
        core_at = (core + member % 2) % 2

        for hop in range(Z_RING // 2):

            @pl.when((j == 4 * hop + 2) & (core == 0))
            def _(hop=hop):
                z_in(0, hop).wait_recv()
                z_in(1, hop).wait_recv()
                if hop < Z_RING // 2 - 1:
                    z_out(0, hop + 1).start()
                    z_out(1, hop + 1).start()

            @pl.when((j == 4 * hop + 2) & (core == 1))
            def _(hop=hop):
                if hop < Z_RING // 2 - 1:
                    relay(hop + 2)
                relayed(hop + 1)

            @pl.when(j == 4 * hop + 2)
            def _(hop=hop):
                p_out(2 * hop + 1).start()
                if hop < Z_RING // 2 - 1:
                    p_out(2 * hop + 2).start()

        @pl.when(member % 2 == 1)
        def _():
            p_copy(j // 2, z_at, 1 - core).wait_recv()

        slab = kv_ref[z_at, core_at]
        scores = lax.dot_general(
            slab, q_ref[...], (((1,), (1,)), ((), ())), preferred_element_type=jnp.float32
        )
        if guarded:
            before = max_ref[...]
            top = jnp.maximum(before, jnp.max(scores, axis=0, keepdims=True))
            factor = jnp.exp(before - top)
            weights = jnp.exp(scores - top)
            max_ref[...] = top
        else:
            factor = None
            weights = jnp.exp2(scores * LOG2E)
        added = jnp.sum(weights.reshape(group // 8, 8, columns), axis=0)
        mixed = lax.dot_general(
            slab,
            weights.astype(jnp.bfloat16),
            (((0,), (0,)), ((), ())),
            preferred_element_type=jnp.float32,
        )[HEAD_SIZE:]
        if guarded:
            sum_ref[...] = sum_ref[...] * factor + added
            acc_ref[...] = acc_ref[...] * factor + mixed
        else:
            sum_ref[...] += added
            acc_ref[...] += mixed
        return carry

    lax.fori_loop(0, 2 * Z_RING, step, 0)

    attended = acc_ref[...] / jnp.sum(sum_ref[...], axis=0, keepdims=True)
    mean_sq = jnp.mean(attended * attended, axis=0, keepdims=True)
    unit = attended * lax.rsqrt(mean_sq + EPS)
    turned = jnp.concatenate([unit, jnp.zeros_like(unit)], axis=0).T
    low = lax.broadcasted_iota(jnp.int32, (tokens, 128), 1) < HEAD_SIZE
    for pair in range(mine_ref.shape[1] // 128):
        first = turned[(2 * pair) * tokens : (2 * pair + 1) * tokens, :]
        second = turned[(2 * pair + 1) * tokens : (2 * pair + 2) * tokens, :]
        joined = jnp.where(low, first, pltpu.roll(second, HEAD_SIZE, 1))
        lanes = slice(pair * 128, (pair + 1) * 128)
        mine_ref[:, lanes] = (joined * gain_ref[:, lanes]).astype(jnp.bfloat16)

    part = tokens // tp_count

    def rows_of(owner):
        return mine_ref.at[pl.ds(pl.multiple_of((owner % tp_count) * part, part), part)]

    def t_copy(r, source):
        return remote(
            rows_of(tp + r),
            out_ref.at[source % tp_count],
            t_send.at[r - 1],
            t_recv.at[r - 1],
            {"tp": (tp + r) % tp_count},
        )

    for r in range(1, tp_count):
        t_copy(r, tp).start()
    own = pltpu.make_async_copy(rows_of(tp), out_ref.at[tp], l_sem)
    own.start()
    own.wait()
    for r in range(1, X_RING):
        x_copy(r, x).wait_send()

    @pl.when(core == 0)
    def _():
        for way in range(2):
            for hop in range(Z_RING // 2):
                z_out(way, hop).wait_send()

    @pl.when(core == 1)
    def _():
        for k in range(1, Z_RING):
            v_copy(k, z).wait_send()
            for r in range(1, X_RING):
                u_copy(k, r, x).wait_send()

    for number in range(Z_RING):
        p_out(number).wait_send()
    for r in range(1, tp_count):
        t_copy(r, tp + tp_count - r).wait_recv()
        t_copy(r, tp).wait_send()


def layer_kernel(
    guarded,
    q_ref,
    packed_ref,
    gain_ref,
    residual_ref,
    ffn_gain_ref,
    routes_ref,
    weights_ref,
    out_proj_hbm,
    shared_gate_hbm,
    shared_up_hbm,
    shared_down_hbm,
    gate_hbm,
    up_hbm,
    down_hbm,
    out_ref,
    attention_scratch,
    heads_ref,
    out_proj_ref,
    shared_gate_ref,
    shared_up_ref,
    shared_down_ref,
    own_ref,
    hidden_ref,
    rank_ref,
    scale_ref,
    normed_ref,
    leaving_ref,
    passing_ref,
    arrived_ref,
    made_ref,
    back_passing_ref,
    back_ref,
    acc_ref,
    part_ref,
    got_ref,
    gate_ref,
    up_ref,
    down_ref,
    w_sem,
    l_sem,
    y_send,
    y_recv,
    s_send,
    s_recv,
    z_send,
    z_recv,
    i_send,
    i_recv,
    i_local,
    bz_send,
    bz_recv,
    bi_send,
    bi_recv,
    bi_local,
):
    sp, tp = lax.axis_index("sp"), lax.axis_index("tp")
    tp_count = lax.axis_size("tp")
    z, i = sp // PLANE, sp % PLANE
    part, width = hidden_ref.shape
    tokens = part * tp_count
    quarter = width // 4
    rows = PLANE * 8
    top = routes_ref.shape[0]
    experts = Z_RING * PLANE

    def at_z(z_at):
        return {"sp": (z_at % Z_RING) * PLANE + i}

    def at_i(i_at):
        return {"sp": z * PLANE + i_at % PLANE}

    def at_tp(t):
        return {"tp": t % tp_count}

    barrier = pltpu.get_barrier_semaphore()
    others = [at_z(z + k) for k in range(1, Z_RING)]
    others += [at_i(i + r) for r in range(1, PLANE)]
    others += [at_tp(tp + r) for r in range(1, tp_count)]
    for other in others:
        pl.semaphore_signal(barrier, inc=1, device_id=other, device_id_type=MESH)

    loads = [
        pltpu.make_async_copy(
            residual_ref.at[pl.ds(pl.multiple_of(tp * part, part), part)], own_ref, l_sem
        ),
    ]
    weights = (
        (out_proj_hbm, out_proj_ref),
        (shared_gate_hbm, shared_gate_ref),
        (shared_up_hbm, shared_up_ref),
        (shared_down_hbm, shared_down_ref),
        (gate_hbm, gate_ref),
        (up_hbm, up_ref),
        (down_hbm, down_ref),
    )
    for number, (source, target) in enumerate(weights):
        loads.append(pltpu.make_async_copy(source, target, w_sem.at[number]))
    for load in loads:
        load.start()

    def remote(src, dst, send_sem, recv_sem, to):
        return pltpu.make_async_remote_copy(
            src_ref=src,
            dst_ref=dst,
            send_sem=send_sem,
            recv_sem=recv_sem,
            device_id=to,
            device_id_type=MESH,
        )

    named = lax.broadcasted_iota(jnp.int32, (experts, tokens), 0) * tp_count + tp
    hot = jnp.zeros((experts, tokens), jnp.float32)
    scale = jnp.zeros((experts, tokens), jnp.float32)
    for choice in range(top):
        same = named == routes_ref[choice : choice + 1, :]
        hot += jnp.where(same, 1.0, 0.0)
        scale += jnp.where(same, weights_ref[choice : choice + 1, :], 0.0)
    earlier = lax.broadcasted_iota(jnp.int32, (tokens, tokens), 0)
    later = lax.broadcasted_iota(jnp.int32, (tokens, tokens), 1)
    before = jnp.where(earlier < later, 1.0, 0.0).astype(jnp.bfloat16)
    rank = jnp.dot(hot.astype(jnp.bfloat16), before, preferred_element_type=jnp.float32)
    rank_ref[...] = jnp.where(hot > 0.0, rank, -1.0).reshape(Z_RING, PLANE, tokens)
    scale_ref[...] = scale.reshape(Z_RING, PLANE, tokens)

    def rows_of_eight(ref, z_at):
        value = ref[z_at][:, None, :]
        return jnp.broadcast_to(value, (PLANE, 8, tokens)).reshape(rows, tokens)

    pl.semaphore_wait(barrier, len(others))
    ring_attention(guarded, q_ref, packed_ref, gain_ref, heads_ref, *attention_scratch)

    for load in loads:
        load.wait()
    size = heads_ref.shape[2]
    total = own_ref[...].astype(jnp.float32)
    for t in range(tp_count):
        total += jnp.dot(
            heads_ref[t],
            out_proj_ref[t * size : (t + 1) * size, :],
            preferred_element_type=jnp.float32,
        )
    hidden = total.astype(jnp.bfloat16).astype(jnp.float32)
    hidden_ref[...] = hidden
    normed_ref[tp] = final_norm(hidden, ffn_gain_ref[...]).astype(jnp.bfloat16)
    y_lanes = (pl.ds(0, quarter), pl.ds(quarter, width - quarter))
    z_lanes = (pl.ds(0, quarter), pl.ds(quarter, width))
    b_lanes = (pl.ds(0, width), pl.ds(width, quarter))
    whole = pl.ds(0, width + quarter)

    def y_copy(r, source, piece):
        place = normed_ref.at[source % tp_count, :, y_lanes[piece]]
        return remote(
            place, place, y_send.at[r - 1, piece], y_recv.at[r - 1, piece], at_tp(tp + r)
        )

    for piece in range(2):
        for r in (2, 1, 3):
            y_copy(r, tp, piece).start()

    def turn(n):
        odd = n % 2
        even = (Z_RING // 2 + n // 2) * ((n + Z_RING - 1) // Z_RING)
        return odd * ((Z_RING + 1 - n) // 2) + (1 - odd) * even

    def z_copy(k, z_from, z_to, piece):
        return remote(
            leaving_ref.at[z_to % Z_RING, :, :, z_lanes[piece]],
            passing_ref.at[z_from % Z_RING, :, :, z_lanes[piece]],
            z_send.at[k, piece],
            z_recv.at[k, piece],
            at_z(z + k),
        )

    def bz_copy(k, z_from, z_to, piece):
        return remote(
            made_ref.at[z_to % Z_RING, :, :, b_lanes[piece]],
            back_passing_ref.at[z_from % Z_RING, :, :, b_lanes[piece]],
            bz_send.at[k, piece],
            bz_recv.at[k, piece],
            at_z(z + Z_RING - k),
        )

    out_way = (passing_ref, arrived_ref, i_send, i_recv, i_local, whole, 0)
    back_ways = [
        (back_passing_ref, back_ref, bi_send, bi_recv, bi_local, b_lanes[p], p * Z_RING)
        for p in range(2)
    ]

    def i_copy(way, k, z_at, r, tile, place):
        source_ref, target_ref, sends, recvs, _, lanes, shift = way
        return remote(
            source_ref.at[z_at % Z_RING, tile % PLANE, :, lanes],
            target_ref.at[z_at % Z_RING, place % PLANE, :, lanes],
            sends.at[k + shift, r - 1],
            recvs.at[k + shift, r - 1],
            at_i(i + r),
        )

    def own_copy(way, k, z_at):
        source_ref, target_ref, _, _, locals_, lanes, shift = way
        return pltpu.make_async_copy(
            source_ref.at[z_at % Z_RING, i, :, lanes],
            target_ref.at[z_at % Z_RING, i, :, lanes],
            locals_.at[k + shift],
        )

    def spread(way, k, z_at):
        for r in range(1, PLANE):
            i_copy(way, k, z_at, r, i + r, i).start()
        own_copy(way, k, z_at).start()

    def collected(way, k, z_at):
        for r in range(1, PLANE):
            i_copy(way, k, z_at, r, i, i + PLANE - r).wait_recv()
        own_copy(way, k, z_at).wait()

    def sent(way, k, z_at):
        for r in range(1, PLANE):
            i_copy(way, k, z_at, r, i + r, i).wait_send()

    def dispatch(piece, n, carry):
        k = turn(n)
        z_to = (z + k) % Z_RING
        row = lax.broadcasted_iota(jnp.int32, (rows, tokens), 0)
        rank = rows_of_eight(rank_ref, z_to)
        place = (row % 8).astype(jnp.float32)
        main = jnp.where(rank == place, 1.0, 0.0).astype(jnp.bfloat16)
        for q in range(1) if piece == 0 else range(1, 4):
            cols = slice(q * quarter, (q + 1) * quarter)
            normed = normed_ref[:, :, cols].reshape(tokens, quarter)
            leaving_ref[z_to, :, :, cols] = (
                jnp.dot(main, normed, preferred_element_type=jnp.float32)
                .astype(jnp.bfloat16)
                .reshape(PLANE, 8, quarter)
            )
        if piece == 1:
            extra = jnp.where(rank == 8.0 + (row % 8 // 4).astype(jnp.float32), 1.0, 0.0)
            tail = jnp.zeros((rows, quarter), jnp.float32)
            for q in range(4):
                normed = normed_ref[:, :, q * quarter : (q + 1) * quarter].reshape(tokens, quarter)
                chosen = jnp.where(row % 4 == q, extra, 0.0).astype(jnp.bfloat16)
                tail += jnp.dot(chosen, normed, preferred_element_type=jnp.float32)
            leaving_ref[z_to, :, :, width:] = tail.astype(jnp.bfloat16).reshape(PLANE, 8, quarter)

            @pl.when(n == 0)
            def _():
                spread((leaving_ref,) + out_way[1:], 0, z)

        @pl.when(n > 0)
        def _():
            z_copy(k, z, z + k, piece).start()

        return carry

    for piece in range(2):
        for r in range(1, tp_count):
            y_copy(r, tp + tp_count - r, piece).wait_recv()
        lax.fori_loop(0, Z_RING, functools.partial(dispatch, piece), 0)

    normed = normed_ref[...].reshape(tokens, width)
    gate = jnp.dot(normed, shared_gate_ref[...], preferred_element_type=jnp.float32)
    up = jnp.dot(normed, shared_up_ref[...], preferred_element_type=jnp.float32)
    inner = (gate / (1.0 + jnp.exp(-gate)) * up).astype(jnp.bfloat16)
    acc_ref[...] = jnp.dot(inner, shared_down_ref[...], preferred_element_type=jnp.float32)

    def expert(k):
        z_from = (z + Z_RING - k) % Z_RING
        tiles = arrived_ref[z_from].reshape(rows, width + quarter)
        extra_rows = rows // 4
        place = lax.broadcasted_iota(jnp.int32, (extra_rows, rows), 1)
        index = lax.broadcasted_iota(jnp.int32, (extra_rows, rows), 0)
        pieces = []
        for q in range(4):
            pick = jnp.where(place == 4 * index + q, 1.0, 0.0).astype(jnp.bfloat16)
            pieces.append(
                jnp.dot(pick, tiles[:, width:], preferred_element_type=jnp.float32).astype(
                    jnp.bfloat16
                )
            )
        every = jnp.concatenate([tiles[:, :width], jnp.concatenate(pieces, axis=1)], axis=0)
        gate = jnp.dot(every, gate_ref[...], preferred_element_type=jnp.float32)
        up = jnp.dot(every, up_ref[...], preferred_element_type=jnp.float32)
        inner = (gate / (1.0 + jnp.exp(-gate)) * up).astype(jnp.bfloat16)
        place = lax.broadcasted_iota(jnp.int32, (rows, extra_rows), 0)
        index = lax.broadcasted_iota(jnp.int32, (rows, extra_rows), 1)
        tail = jnp.zeros((rows, quarter), jnp.float32)
        for q in range(4):
            cols = slice(q * quarter, (q + 1) * quarter)
            made = jnp.dot(inner, down_ref[:, cols], preferred_element_type=jnp.float32).astype(
                jnp.bfloat16
            )
            made_ref[z_from, :, :, (q + 1) * quarter : (q + 2) * quarter] = made[:rows].reshape(
                PLANE, 8, quarter
            )
            pick = jnp.where(place == 4 * index + q, 1.0, 0.0).astype(jnp.bfloat16)
            tail += jnp.dot(pick, made[rows:], preferred_element_type=jnp.float32)
        made_ref[z_from, :, :, :quarter] = tail.astype(jnp.bfloat16).reshape(PLANE, 8, quarter)

    made_ways = [(made_ref,) + way[1:] for way in back_ways]

    def arrivals(n, carry):
        @pl.when((n > 0) & (n < Z_RING))
        def _():
            k = turn(n)
            for piece in range(2):
                z_copy(k, z + Z_RING - k, z, piece).wait_recv()
            spread(out_way, k, z + Z_RING - k)

        @pl.when(n > 0)
        def _():
            k = turn(n - 1)
            collected(out_way, k, z + Z_RING - k)
            expert(k)

            @pl.when(n > 1)
            def _():
                bz_copy(k, z, z + Z_RING - k, 0).start()

            @pl.when(n == 1)
            def _():
                spread(made_ways[0], 0, z)

        return carry

    lax.fori_loop(0, Z_RING + 1, arrivals, 0)
    spread(made_ways[1], 0, z)
    for k in (4, 5, 3, 6, 2, 7, 1):
        bz_copy(k, z, z + Z_RING - k, 1).start()

    def combine(piece, z_at):
        def twice(start):
            tiles = back_ref[z_at, :, :, start : start + quarter].reshape(rows, quarter)
            return jnp.concatenate([tiles, tiles], axis=0)

        row = lax.broadcasted_iota(jnp.int32, (rows, tokens), 0)
        rank = rows_of_eight(rank_ref, z_at)
        scale = rows_of_eight(scale_ref, z_at)
        place = (row % 8).astype(jnp.float32)
        main = jnp.where(rank == place, scale, 0.0)
        extra = jnp.where(rank == 8.0 + (row % 8 // 4).astype(jnp.float32), scale, 0.0)

        def two_terms(value):
            high = value.astype(jnp.bfloat16)
            low = (value - high.astype(jnp.float32)).astype(jnp.bfloat16)
            return jnp.concatenate([high, low], axis=0)

        def product(terms, tiles):
            return lax.dot_general(
                terms, tiles, (((0,), (0,)), ((), ())), preferred_element_type=jnp.float32
            )

        main = two_terms(main)
        for q in range(4):
            cols = slice(q * quarter, (q + 1) * quarter)
            if piece == 1:
                if q == 3:
                    acc_ref[:, cols] += product(main, twice((q + 1) * quarter))
                continue
            chosen = two_terms(jnp.where(row % 4 == q, extra, 0.0))
            added = product(chosen, twice(0))
            if q < 3:
                added += product(main, twice((q + 1) * quarter))
            acc_ref[:, cols] += added

    def returns(piece, n, carry):
        @pl.when((n > 0) & (n < Z_RING))
        def _():
            k = turn(n)
            bz_copy(k, z + k, z, piece).wait_recv()
            spread(back_ways[piece], k, z + k)

        @pl.when(n > 0)
        def _():
            k = turn(n - 1)
            collected(back_ways[piece], k, z + k)
            combine(piece, (z + k) % Z_RING)

        return carry

    s_lanes = (pl.ds(0, 3 * quarter), pl.ds(3 * quarter, quarter))

    def s_copy(r, source, piece):
        return remote(
            part_ref.at[(tp + r) % tp_count, :, s_lanes[piece]],
            got_ref.at[source % tp_count, :, s_lanes[piece]],
            s_send.at[r - 1, piece],
            s_recv.at[r - 1, piece],
            at_tp(tp + r),
        )

    for piece in range(2):
        lax.fori_loop(0, Z_RING + 1, functools.partial(returns, piece), 0)
        for r in (2, 1, 3, 0):
            owner = (tp + r) % tp_count
            own_rows = pl.ds(pl.multiple_of(owner * part, part), part)
            lanes = s_lanes[piece]
            part_ref[owner, :, lanes] = acc_ref[own_rows, lanes].astype(jnp.bfloat16)
            if r:
                s_copy(r, tp, piece).start()
            else:
                got_ref[tp, :, lanes] = part_ref[tp, :, lanes]
    for piece in range(2):
        for r in range(1, tp_count):
            s_copy(r, tp + tp_count - r, piece).wait_recv()
    total = hidden_ref[...]
    for t in range(tp_count):
        total += got_ref[t].astype(jnp.float32)
    out_ref[...] = total.astype(jnp.bfloat16)

    for piece in range(2):
        for r in range(1, tp_count):
            y_copy(r, tp, piece).wait_send()
            s_copy(r, tp, piece).wait_send()

    def drain(n, carry):
        @pl.when(n > 0)
        def _():
            for piece in range(2):
                z_copy(n, z, z + n, piece).wait_send()
                bz_copy(n, z, z + Z_RING - n, piece).wait_send()

        sent(out_way, n, z + Z_RING - n)
        for piece in range(2):
            sent(back_ways[piece], n, z + n)
        return carry

    lax.fori_loop(0, Z_RING, drain, 0)


def call(kernel, out_shape, out_specs, args):
    return pl.pallas_call(
        kernel,
        out_shape=out_shape,
        in_specs=[VM] * len(args),
        out_specs=out_specs,
    )(*args)


def shaped(dims, kind=jnp.bfloat16):
    return jax.ShapeDtypeStruct(dims, kind)


def local(
    queries,
    key_matrix,
    values,
    query_gain,
    key_norm_gain,
    head_gain,
    out_proj,
    residual,
    ffn_gain,
    routes,
    route_weights,
    expert_gate,
    expert_up,
    expert_down,
    shared_gate,
    shared_up,
    shared_down,
):
    tokens = queries.shape[0]
    heads = queries.shape[1] // HEAD_SIZE
    sp_count = lax.axis_size("sp")
    tp_count = lax.axis_size("tp")
    sequence_total = tokens * sp_count
    cosine, sine = wide_tables(lax.axis_index("sp") * tokens, tokens, sequence_total)
    columns = heads * tokens
    query_rows, packed, bound = call(
        prepare_kernel,
        (shaped((columns, 128)), shaped((tokens, 128)), shaped((1, 1), jnp.float32)),
        (VM, VM, pl.BlockSpec(memory_space=pltpu.SMEM)),
        (
            queries,
            key_matrix.T,
            values.T,
            query_gain[None],
            key_norm_gain[None],
            cosine,
            sine,
        ),
    )
    part_rows = tokens // tp_count

    width = residual.shape[1]
    hidden_units = expert_gate.shape[2]
    wide_row = width + width // 4
    tile_set = pltpu.VMEM((Z_RING, PLANE, 8, wide_row), jnp.bfloat16)
    dma = pltpu.SemaphoreType.DMA

    def like(weight):
        return pltpu.VMEM(weight.shape, weight.dtype)

    operands = (
        query_rows,
        packed,
        head_gain[None],
        residual,
        ffn_gain[None],
        routes.T,
        route_weights.T,
        out_proj,
        shared_gate,
        shared_up,
        shared_down,
        expert_gate[0],
        expert_up[0],
        expert_down[0],
    )
    attention_scratch = (
        pltpu.VMEM((Z_RING, 2, X_RING * tokens, 128), jnp.bfloat16),
        pltpu.VMEM((tokens, heads * HEAD_SIZE), jnp.bfloat16),
        pltpu.VMEM((HEAD_SIZE, columns), jnp.float32),
        pltpu.VMEM((8, columns), jnp.float32),
        pltpu.VMEM((1, columns), jnp.float32),
        dma((X_RING - 1,)),
        dma((X_RING - 1,)),
        dma((2, Z_RING // 2)),
        dma((2, Z_RING // 2)),
        dma((Z_RING - 1,)),
        dma((Z_RING - 1,)),
        dma((Z_RING - 1, X_RING - 1)),
        dma((Z_RING - 1, X_RING - 1)),
        dma((Z_RING,)),
        dma((Z_RING,)),
        dma((tp_count - 1,)),
        dma((tp_count - 1,)),
        dma,
    )

    def layer(guarded, number):
        return pl.pallas_call(
            functools.partial(layer_kernel, guarded),
            out_shape=shaped((part_rows, width)),
            in_specs=[VM] * 3 + [ANY] + [VM] * 3 + [ANY] * 7,
            out_specs=VM,
            scratch_shapes=[
                attention_scratch,
                pltpu.VMEM((tp_count, part_rows, heads * HEAD_SIZE), jnp.bfloat16),
                like(out_proj),
                like(shared_gate),
                like(shared_up),
                like(shared_down),
                pltpu.VMEM((part_rows, width), jnp.bfloat16),
                pltpu.VMEM((part_rows, width), jnp.float32),
                pltpu.VMEM((Z_RING, PLANE, tokens), jnp.float32),
                pltpu.VMEM((Z_RING, PLANE, tokens), jnp.float32),
                pltpu.VMEM((tp_count, part_rows, width), jnp.bfloat16),
                tile_set,
                tile_set,
                tile_set,
                tile_set,
                tile_set,
                tile_set,
                pltpu.VMEM((tokens, width), jnp.float32),
                pltpu.VMEM((tp_count, part_rows, width), jnp.bfloat16),
                pltpu.VMEM((tp_count, part_rows, width), jnp.bfloat16),
                like(expert_gate[0]),
                like(expert_up[0]),
                like(expert_down[0]),
                dma((7,)),
                dma,
                dma((tp_count - 1, 2)),
                dma((tp_count - 1, 2)),
                dma((tp_count - 1, 2)),
                dma((tp_count - 1, 2)),
                dma((Z_RING, 2)),
                dma((Z_RING, 2)),
                dma((Z_RING, PLANE - 1)),
                dma((Z_RING, PLANE - 1)),
                dma((Z_RING,)),
                dma((Z_RING, 2)),
                dma((Z_RING, 2)),
                dma((2 * Z_RING, PLANE - 1)),
                dma((2 * Z_RING, PLANE - 1)),
                dma((2 * Z_RING,)),
            ],
            compiler_params=pltpu.CompilerParams(
                vmem_limit_bytes=62 * 2**20, collective_id=number, has_side_effects=True
            ),
        )

    return lax.cond(bound[0, 0] > SAFE_BOUND, layer(True, 1), layer(False, 0), *operands)


def solution(mesh):
    placed = (
        P("sp", "tp"),
        P("sp", "tp"),
        P("sp", "tp"),
        P(),
        P(),
        P("tp"),
        P(),
        P("sp", None),
        P(),
        P("sp", None),
        P("sp", None),
        P(("sp", "tp"), None, None),
        P(("sp", "tp"), None, None),
        P(("sp", "tp"), None, None),
        P(None, "tp"),
        P(None, "tp"),
        P("tp", None),
    )
    return jax.shard_map(
        local, mesh=mesh, in_specs=placed, out_specs=P(("sp", "tp"), None), check_vma=False
    )
```
